32 devices in a mesh: sp: 8 (over z, x), tp: 4 (over y, core).
Axes of the slice: x: 2, y: 2, z: 4, core: 2. Of those that a mesh axis runs over, the one named last changes fastest.
Arguments:
- query_rows: bfloat16 [2048, 2048], P('sp', 'tp'), may hold values from -6 to 6
- key_rows: bfloat16 [2048, 2048], P('sp', 'tp'), may hold values from -6 to 6
- value_rows: bfloat16 [2048, 2048], P('sp', 'tp'), may hold values from -6 to 6
- gate_rows: bfloat16 [2048, 2048], P('sp', 'tp'), may hold values from -6 to 6
- log_decay: float32 [2048, 16], P('sp', 'tp'), may hold values from -1 to 0
- head_gain: float32 [2048], P('tp'), may hold values from 0.1 to 1.9
- out_weight: bfloat16 [2048, 2048], P('tp'), may hold values from -0.125 to 0.125
- residual: bfloat16 [2048, 2048], P(('sp', 'tp')), may hold values from -6 to 6
- ffn_gain: float32 [2048], replicated, may hold values from 0.1 to 1.9
- gate_weight: bfloat16 [8, 2048, 2048], P('sp', None, 'tp'), may hold values from -0.375 to 0.375
- up_weight: bfloat16 [8, 2048, 2048], P('sp', None, 'tp'), may hold values from -0.375 to 0.375
- down_weight: bfloat16 [8, 2048, 2048], P('sp', 'tp'), may hold values from -0.01953125 to 0.01953125
- routes: int32 [2048, 4], P('sp'), may hold values from 0 to 7, all different within a row; in each aligned block of 64 rows (0 to 63, 64 to 127, ...) at most 48 rows name the same one
- route_weights: float32 [2048, 4], P(('sp', 'tp')), may hold values from 0.05 to 1
Outputs:
- layer_out: bfloat16 [2048, 2048], P(('sp', 'tp'))
The draws below stay inside these ranges and needn't reach their ends.
Inputs may be any that keep to these rules, and one draw needn't show every extreme that they name: `routes`: each row names 4 different experts. In each aligned block of 64 rows no expert is named by more than 48 rows, and in some block some expert is named by exactly 48 rows.
All inputs are finite; a program needn't handle non-finite values.
Results may differ from the reference program's by a relative error of at most 0.014.
Values may be sent and summed in bfloat16 or wider, within the bound.
A program may use at most 128 MiB of HBM per device.

```python
import math
from functools import partial
import jax
import jax.numpy as jnp
import numpy as np
from jax import lax

D = 2048
HEAD_TOTAL = 16
HEAD_DIM = 128
FF = 2048
TOPK = 4
BLOCK = 128
TOK_DEV = 256
RET_WIDTH = 2048
EXPERTS = 8
TOKEN_TOTAL = 2048
ROWS_DEV = 64
CAP = 48
N_TP = 4


def draw_log_decay(key, part):
    split_random_keys = jax.random.split(jax.random.fold_in(key, 17), 7)
    fast_share = 0.5
    is_fast = jax.random.uniform(split_random_keys[0], (HEAD_TOTAL,), jnp.float32) < fast_share
    fast_rate = jnp.exp(jax.random.uniform(split_random_keys[1], (HEAD_TOTAL,), jnp.float32, math.log(1.0 / 15.0), math.log(1.0 / 8.0)))
    slow_rate = jnp.exp(jax.random.uniform(split_random_keys[2], (HEAD_TOTAL,), jnp.float32, math.log(0.05), math.log(0.25))) / TOKEN_TOTAL
    baseline_rate = jnp.where(is_fast, fast_rate, slow_rate)
    span_count = TOKEN_TOTAL // TOK_DEV
    extent_factor = jnp.exp(jax.random.uniform(split_random_keys[3], (span_count, HEAD_TOTAL), jnp.float32, -math.log(2.0), math.log(2.0)))
    extent_factor = jnp.repeat(extent_factor, TOK_DEV, axis=0)
    coarse_factor = jax.random.uniform(split_random_keys[4], (TOKEN_TOTAL, HEAD_TOTAL), jnp.float32, 0.5, 1.5)
    spike_position = jax.random.randint(split_random_keys[5], (3,), 0, TOKEN_TOTAL)
    spike_flags = jnp.zeros((TOKEN_TOTAL,), jnp.float32).at[spike_position].set(1.0)
    spike_penalty = jnp.log(jax.random.uniform(split_random_keys[6], (HEAD_TOTAL,), jnp.float32, 0.6, 0.8))
    return (-baseline_rate[None, :] * extent_factor * coarse_factor + spike_flags[:, None] * spike_penalty[None, :]).astype(jnp.float32)


def steps_of(rng, extent, shards, low, high):
    def one(dim, shards_of):
        heights = jax.random.uniform(jax.random.fold_in(jax.random.fold_in(rng, 6), dim), (shards_of,), jnp.float32, low / len(shards), high / len(shards))
        return jnp.repeat(jnp.exp(heights), extent[dim] // shards_of).reshape((-1,) + (1,) * (len(extent) - dim - 1))

    gain = one(*shards[0])
    for cut in shards[1:]:
        gain = gain * one(*cut)
    return gain


def deal_out(key, own, number, rows, amount, top, limit, lean):
    sequence = jax.random.permutation(key, amount)
    crowded, common = shares(amount, rows * top, limit, lean, True), shares(amount, rows * top, limit, lean, False)
    places = jnp.arange(amount)

    def named(lengths, rotation):
        used = int((lengths > 0).sum())
        fixed = max(1, used // 4)
        moved = fixed + (places - fixed + rotation * (used - fixed)) % max(1, amount - fixed)
        return jnp.zeros((amount,), jnp.int32).at[sequence[jnp.where(places < fixed, places, moved)]].set(jnp.asarray(lengths, jnp.int32))

    lengths = jnp.where(number % 4 == 0, named(crowded, number // 4), named(common, number - number // 4 - 1))
    mixed = jax.random.permutation(jax.random.fold_in(own, 3), amount)
    giver, receiver = mixed[0:amount // 2 * 2:2], mixed[1:amount // 2 * 2:2]
    margin = jnp.minimum(lengths[giver] - 1, limit - lengths[receiver]) // 2
    margin = jnp.where((giver == sequence[0]) | (receiver == sequence[0]) | (lengths[receiver] == 0), 0, jnp.maximum(margin, 0))
    moved = jax.random.randint(jax.random.fold_in(own, 4), (amount // 2,), 0, 1 << 20) % (margin + 1)
    lengths = lengths.at[giver].add(-moved).at[receiver].add(moved)
    members = jnp.searchsorted(jnp.cumsum(lengths), jnp.arange(rows * top), side="right").astype(jnp.int32)
    grid = members.reshape(top, rows).T
    grid = grid[jax.random.permutation(jax.random.fold_in(own, 1), rows)]
    rotation = jax.random.randint(jax.random.fold_in(own, 2), (rows, 1), 0, top)
    return jnp.take_along_axis(grid, (jnp.arange(top)[None, :] + rotation) % top, axis=1)


def shares(number_of, total, limit, skew, full):
    weights = [(1 << 20) // math.isqrt(rank ** skew) + 1 for rank in range(1, number_of + 1)]
    largest = limit if full else min(limit, max(-(-total // number_of), total * weights[0] // sum(weights)))
    least = 1 if total - largest >= number_of - 1 else 0
    holding, rest = [largest] + [least] * (number_of - 1), total - largest - least * (number_of - 1)
    while rest > 0:
        candidates = [i for i in range(1, number_of) if holding[i] < largest] or [i for i in range(1, number_of) if holding[i] < limit]
        whole, left = sum([weights[i] for i in candidates]), rest
        for i in candidates:
            addition = min(limit - holding[i], max(1, left * weights[i] // whole), rest)
            holding[i] = holding[i] + addition
            rest = rest - addition
    return np.array(holding)


def scatter_about(own_key, shape, scale, most, cuts=(), kind=jnp.bfloat16):
    entries = jax.random.normal(own_key, shape, jnp.float32) * scale
    if len(cuts) > 0:
        entries = steps_of(own_key, shape, cuts, -0.22, 0.18) * entries
    return jnp.clip(entries, min=-most, max=most).astype(kind)


def setup_inputs(seed: int = 0) -> dict:
    key_list = jax.random.split(jax.random.key(seed), 15)
    query_rows = scatter_about(key_list[0], (TOKEN_TOTAL, RET_WIDTH), 1.0, 6.0, ((0, 8), (1, 4)))
    key_rows = scatter_about(key_list[1], (TOKEN_TOTAL, RET_WIDTH), 1.0, 6.0, ((0, 8), (1, 4)))
    value_rows = scatter_about(key_list[2], (TOKEN_TOTAL, RET_WIDTH), 1.0, 6.0, ((0, 8), (1, 4)))
    gate_rows = scatter_about(key_list[3], (TOKEN_TOTAL, RET_WIDTH), 1.0, 6.0, ((0, 8), (1, 4)))
    log_decay = draw_log_decay(jax.random.fold_in(key_list[14], 71), 0)
    head_gain = jnp.clip(1.0 + 0.18 * jax.random.normal(key_list[5], (RET_WIDTH,), jnp.float32), 0.1, 1.9)
    out_weight = scatter_about(key_list[6], (RET_WIDTH, D), RET_WIDTH ** -0.5, 0.125, ((0, 4),))
    residual = scatter_about(key_list[7], (TOKEN_TOTAL, D), 1.0, 6.0, ((0, 32),))
    ffn_gain = jnp.clip(1.0 + 0.18 * jax.random.normal(key_list[8], (D,), jnp.float32), 0.1, 1.9)
    gate_weight = scatter_about(key_list[9], (EXPERTS, D, FF), (D // 9) ** -0.5, 0.375, ((0, 8), (2, 4)))
    up_weight = scatter_about(key_list[10], (EXPERTS, D, FF), (D // 9) ** -0.5, 0.375, ((0, 8), (2, 4)))
    down_weight = scatter_about(key_list[11], (EXPERTS, FF, D), (FF * 44) ** -0.5, 0.01953125, ((0, 8), (1, 4)))
    routes_keys = jax.random.split(jax.random.fold_in(key_list[12], 1), TOKEN_TOTAL // ROWS_DEV)
    routes_turns = jax.random.permutation(jax.random.fold_in(key_list[12], 3), TOKEN_TOTAL // ROWS_DEV)
    routes = jax.vmap(lambda own, number: deal_out(jax.random.fold_in(key_list[12], 2), own, number, ROWS_DEV, EXPERTS, TOPK, CAP, 1))(routes_keys, routes_turns).reshape((TOKEN_TOTAL, TOPK))
    route_weights = jnp.clip(jnp.exp(math.log(1.0) - 2.9957323 * jax.random.uniform(key_list[13], (TOKEN_TOTAL, TOPK), jnp.float32) ** steps_of(key_list[13], (TOKEN_TOTAL, TOPK), ((0, 32),), -0.2, 0.2)), 0.05, 1.0)
    return dict(query_rows=query_rows, key_rows=key_rows, value_rows=value_rows, gate_rows=gate_rows, log_decay=log_decay, head_gain=head_gain, out_weight=out_weight, residual=residual, ffn_gain=ffn_gain, gate_weight=gate_weight, up_weight=up_weight, down_weight=down_weight, routes=routes, route_weights=route_weights)


highest = lax.Precision.HIGHEST
rope_base = 10000.0
group_eps = 1e-05
square_eps = 1e-06
clamp_limit = 7.0
swish_alpha = 1.702

def rotary_angles(positions, head_dim):
    half_dim = head_dim // 2
    inverse = rope_base ** (-jnp.arange(half_dim, dtype=jnp.float32) / half_dim)
    return positions[:, None] * inverse[None, :]

def rotate(values, angles):
    half_dim = values.shape[-1] // 2
    cosine = jnp.cos(angles)[:, None, :]
    sine_table = jnp.sin(angles)[:, None, :]
    first_half = values[..., :half_dim]
    second_half = values[..., half_dim:]
    return jnp.concatenate([first_half * cosine - second_half * sine_table, second_half * cosine + first_half * sine_table], axis=-1)

def block_pass(carry_state, queries, keys_rot, values, log_step):
    length = queries.shape[0]
    cumulative = jnp.cumsum(log_step, axis=0)
    gap_matrix = cumulative[:, None, :] - cumulative[None, :, :]
    causal = jnp.arange(length, dtype=jnp.int32)[:, None] >= jnp.arange(length, dtype=jnp.int32)[None, :]
    weights = jnp.where(causal[:, :, None], jnp.exp(jnp.minimum(gap_matrix, 0.0)), 0.0)
    scores = jnp.einsum('ihd,jhd->ijh', queries, keys_rot, precision=highest) * weights
    inner_part = jnp.einsum('ijh,jhe->ihe', scores, values, precision=highest)
    cross_part = jnp.einsum('ihd,hde->ihe', queries, carry_state, precision=highest) * jnp.exp(cumulative)[:, :, None]
    total_log = cumulative[-1]
    tail_weight = jnp.exp(total_log[None, :] - cumulative)
    carried = carry_state * jnp.exp(total_log)[:, None, None] + jnp.einsum('jhd,jh,jhe->hde', keys_rot, tail_weight, values, precision=highest)
    return (carried, inner_part + cross_part)

def head_norm(retained, gain_row, gate_rows):
    mean_part = lax.optimization_barrier(jnp.mean(retained, axis=-1, keepdims=True))
    centred = retained - mean_part
    variance = lax.optimization_barrier(jnp.mean(centred * centred, axis=-1, keepdims=True))
    scaled = (centred * lax.rsqrt(variance + group_eps)).reshape(retained.shape[0], -1)
    return (scaled * gain_row * jax.nn.silu(gate_rows.astype(jnp.float32))).astype(jnp.bfloat16)

def square_norm(updated, gain_row):
    factor = lax.rsqrt(lax.optimization_barrier(jnp.mean(updated * updated, axis=-1, keepdims=True)) + square_eps)
    return (updated * factor * gain_row).astype(jnp.bfloat16)

def expert_rows(rows, gate_part, up_part):
    gate_pre = jnp.dot(rows, gate_part, preferred_element_type=jnp.float32)
    up_pre = jnp.dot(rows, up_part, preferred_element_type=jnp.float32)
    gate_clip = jnp.minimum(gate_pre, clamp_limit)
    up_clip = jnp.clip(up_pre, -clamp_limit, clamp_limit)
    return ((up_clip + 1.0) * (gate_clip * jax.nn.sigmoid(gate_clip * swish_alpha))).astype(jnp.bfloat16)

def slot_ranks(route_block, experts):
    flat_routes = route_block.reshape(-1)
    onehot = (flat_routes[:, None] == jnp.arange(experts, dtype=jnp.int32)[None, :]).astype(jnp.int32)
    return (flat_routes, lax.optimization_barrier(jnp.sum(jnp.cumsum(onehot, axis=0) * onehot, axis=1)) - 1)

def reference(query_rows, key_rows, value_rows, gate_rows, log_decay, head_gain, out_weight, residual, ffn_gain, gate_weight, up_weight, down_weight, routes, route_weights):
    positions = jnp.arange(TOKEN_TOTAL, dtype=jnp.float32)
    angles = rotary_angles(positions, HEAD_DIM)
    head_shape = (TOKEN_TOTAL, HEAD_TOTAL, HEAD_DIM)
    queries = rotate(query_rows.astype(jnp.float32).reshape(head_shape), angles)
    keys_rot = rotate(key_rows.astype(jnp.float32).reshape(head_shape), angles) * HEAD_DIM ** (-0.5)
    values = value_rows.astype(jnp.float32).reshape(head_shape)
    block_count = TOKEN_TOTAL // BLOCK

    def advance(carry_state, pieces):
        return block_pass(carry_state, pieces[0], pieces[1], pieces[2], pieces[3])
    start_state = jnp.zeros((HEAD_TOTAL, HEAD_DIM, HEAD_DIM), jnp.float32)
    block_shape = (block_count, BLOCK, HEAD_TOTAL, HEAD_DIM)
    _, retained = lax.scan(advance, start_state, (queries.reshape(block_shape), keys_rot.reshape(block_shape), values.reshape(block_shape), log_decay.reshape(block_count, BLOCK, HEAD_TOTAL)))
    retained = retained.reshape(head_shape)
    hidden = head_norm(retained, head_gain, gate_rows)
    updated = residual.astype(jnp.float32) + jnp.dot(hidden, out_weight, preferred_element_type=jnp.float32)
    ffn_in = square_norm(updated, ffn_gain)
    block_total = TOKEN_TOTAL // ROWS_DEV
    grouped = routes.reshape(block_total, ROWS_DEV, TOPK)
    flat_experts, flat_ranks = jax.vmap(partial(slot_ranks, experts=EXPERTS))(grouped)
    block_index = jnp.arange(block_total, dtype=jnp.int32)[:, None]
    slot_index = flat_experts * (block_total * CAP) + block_index * CAP + flat_ranks
    row_index = block_index * ROWS_DEV + jnp.arange(ROWS_DEV * TOPK, dtype=jnp.int32)[None, :] // TOPK
    source_row = jnp.full((EXPERTS * block_total * CAP,), TOKEN_TOTAL, jnp.int32).at[slot_index.reshape(-1)].set(row_index.reshape(-1))
    slot_weight = jnp.zeros((EXPERTS * block_total * CAP,), jnp.float32).at[slot_index.reshape(-1)].set(route_weights.reshape(-1))
    padded = jnp.concatenate([ffn_in, jnp.zeros((1, D), jnp.bfloat16)], axis=0)
    quarter = FF // N_TP

    def expert_step(accumulated, pieces):
        sources, weight_col, gate_part, up_part, down_part = pieces
        activity = expert_rows(padded[sources], gate_part, up_part)
        partials = jnp.einsum('mqf,qfd->qmd', activity.reshape(-1, N_TP, quarter).astype(jnp.float32), down_part.reshape(N_TP, quarter, D).astype(jnp.float32))
        rounded = lax.optimization_barrier(partials.astype(jnp.bfloat16)).astype(jnp.float32)
        expert_out = lax.optimization_barrier(jnp.sum(rounded, axis=0)).astype(jnp.bfloat16)
        return (accumulated.at[sources].add(weight_col[:, None] * expert_out.astype(jnp.float32)), None)
    start_sum = jnp.zeros((TOKEN_TOTAL + 1, D), jnp.float32)
    accumulated, _ = lax.scan(expert_step, start_sum, (source_row.reshape(EXPERTS, -1), slot_weight.reshape(EXPERTS, -1), gate_weight, up_weight, down_weight))
    return (updated + accumulated[:TOKEN_TOTAL]).astype(jnp.bfloat16)
```

```python
import functools

import jax
import jax.numpy as jnp
from jax import lax
from jax.experimental import pallas as pl
from jax.experimental.pallas import tpu as pltpu
from jax.sharding import PartitionSpec as P

HEAD_DIM = 128
TOPK = 4
BLOCK = 128


highest = lax.Precision.HIGHEST
rope_base = 10000.0
group_eps = 1e-05
square_eps = 1e-06
clamp_limit = 7.0
swish_alpha = 1.702


def rotary_angles(positions, head_dim):
    half_dim = head_dim // 2
    inverse = rope_base ** (-jnp.arange(half_dim, dtype=jnp.float32) / half_dim)
    return positions[:, None] * inverse[None, :]


def square_norm(updated, gain_row):
    factor = lax.rsqrt(jnp.mean(updated * updated, axis=-1, keepdims=True) + square_eps)
    return (updated * factor * gain_row).astype(jnp.bfloat16)


def expert_rows(rows, gate_part, up_part):
    gate_pre = jnp.dot(rows, gate_part, preferred_element_type=jnp.float32)
    up_pre = jnp.dot(rows, up_part, preferred_element_type=jnp.float32)
    gate_clip = jnp.minimum(gate_pre, clamp_limit)
    up_clip = jnp.clip(up_pre, -clamp_limit, clamp_limit)
    return ((up_clip + 1.0) * (gate_clip * jax.nn.sigmoid(gate_clip * swish_alpha))).astype(
        jnp.bfloat16
    )


def slot_ranks(route_block, experts):
    flat_routes = route_block.reshape(-1)
    onehot = (flat_routes[:, None] == jnp.arange(experts, dtype=jnp.int32)[None, :]).astype(
        jnp.int32
    )
    return (flat_routes, jnp.sum(jnp.cumsum(onehot, axis=0) * onehot, axis=1) - 1)


def retention_kernel(q_ref, k_ref, v_ref, cos_ref, sin_ref, cum_ref, cum_row_ref, ret_ref, qdec_ref, state_ref):
    head = pl.program_id(0)
    length = q_ref.shape[0]
    cosine, sine = cos_ref[...], sin_ref[...]
    half = HEAD_DIM // 2

    def turned(ref):
        rows = ref[...].astype(jnp.float32)
        return rows * cosine + pltpu.roll(rows, half, 1) * sine

    lanes = lax.broadcasted_iota(jnp.int32, cum_ref.shape, 1)
    column = jnp.sum(jnp.where(lanes == head, cum_ref[...], 0.0), axis=1, keepdims=True)
    row = cum_row_ref[0]
    queries = turned(q_ref)
    keys = turned(k_ref) * HEAD_DIM ** (-0.5)
    values = v_ref[...]
    scores = lax.dot_general(
        queries.astype(jnp.bfloat16),
        keys.astype(jnp.bfloat16),
        (((1,), (1,)), ((), ())),
        preferred_element_type=jnp.float32,
    )
    causal = lax.broadcasted_iota(jnp.int32, (length, length), 0) >= lax.broadcasted_iota(
        jnp.int32, (length, length), 1
    )
    weights = jnp.where(causal, jnp.exp(jnp.minimum(column - row, 0.0)), 0.0)
    ret_ref[...] = jnp.dot(
        (scores * weights).astype(jnp.bfloat16), values, preferred_element_type=jnp.float32
    )
    qdec_ref[...] = (queries * jnp.exp(column)).astype(jnp.bfloat16)
    total = column[length - 1 :, :]
    tailed = (keys * jnp.exp(total - column)).astype(jnp.bfloat16)
    state_ref[0, :HEAD_DIM, :] = lax.dot_general(
        tailed, values, (((0,), (0,)), ((), ())), preferred_element_type=jnp.float32
    )
    state_ref[0, HEAD_DIM:, :] = jnp.broadcast_to(total, (8, HEAD_DIM))


def norm_kernel(ret_ref, qdec_ref, enter_ref, gain_ref, gate_ref, hidden_ref):
    retained = ret_ref[...] + jnp.dot(
        qdec_ref[...], enter_ref[0].astype(jnp.bfloat16), preferred_element_type=jnp.float32
    )
    centred = retained - jnp.mean(retained, axis=-1, keepdims=True)
    variance = jnp.mean(centred * centred, axis=-1, keepdims=True)
    gate = gate_ref[...].astype(jnp.float32)
    scaled = centred * lax.rsqrt(variance + group_eps) * gain_ref[...]
    hidden_ref[...] = (scaled * (gate / (1.0 + jnp.exp(-gate)))).astype(jnp.bfloat16)


def greet(devices):
    barrier = pltpu.get_barrier_semaphore()
    for device in devices:
        pl.semaphore_signal(barrier, inc=1, device_id=device, device_id_type=pl.DeviceIdType.MESH)
    pl.semaphore_wait(barrier, len(devices))


def state_kernel(planes, state, totals, entering, gs, gt, ssem, rsem, lsem):
    sp, tp = lax.axis_index("sp"), lax.axis_index("tp")
    z, x = sp // 2, sp % 2
    heads = state.shape[0]
    to_x = {"sp": z * 2 + (1 - x), "tp": tp}

    def later(i):
        return {"sp": ((z + i) % planes) * 2 + x, "tp": tp}

    def plane_of(i):
        return (z + planes - i) % planes

    def move(kind, i, ref, device):
        return pltpu.make_async_remote_copy(
            src_ref=ref, dst_ref=ref, send_sem=ssem.at[kind, i], recv_sem=rsem.at[kind, i],
            device_id=device, device_id_type=pl.DeviceIdType.MESH,
        )

    own = [
        pltpu.make_async_copy(state, gs.at[z, x], lsem.at[0]),
        pltpu.make_async_copy(totals, gt.at[z, x], lsem.at[1]),
    ]
    for copy in own:
        copy.start()
    greet([to_x] + [later(i) for i in range(1, planes)])
    for copy in own:
        copy.wait()
    for i in range(1, planes):
        move(0, i, gs.at[z, x], later(i)).start()
        move(1, i, gt.at[z, x], later(i)).start()
    for i in range(planes):
        p = plane_of(i)
        if i > 0:
            move(0, i, gs.at[p, x], to_x).wait_recv()
            move(1, i, gt.at[p, x], to_x).wait_recv()
        move(2, i, gs.at[p, x], to_x).start()
        move(3, i, gt.at[p, x], to_x).start()
    for i in range(planes):
        p = plane_of(i)
        move(2, i, gs.at[p, 1 - x], to_x).wait_recv()
        move(3, i, gt.at[p, 1 - x], to_x).wait_recv()
    running = jnp.zeros((8, HEAD_DIM), jnp.float32)
    sums = [jnp.zeros((HEAD_DIM, HEAD_DIM), jnp.float32) for _ in range(heads)]
    for s in reversed(range(2 * planes)):
        earlier = s < sp
        factor = jnp.where(earlier, jnp.exp(running), 0.0)
        running = running + jnp.where(earlier, gt[s // 2, s % 2], 0.0)
        for h in range(heads):
            sums[h] = sums[h] + factor[h : h + 1, :] * gs[s // 2, s % 2, h].astype(jnp.float32)
    for h in range(heads):
        entering[h] = sums[h].astype(jnp.bfloat16)
    for i in range(planes):
        p = plane_of(i)
        if i > 0:
            move(0, i, gs.at[z, x], to_x).wait_send()
            move(1, i, gt.at[z, x], to_x).wait_send()
        move(2, i, gs.at[p, x], to_x).wait_send()
        move(3, i, gt.at[p, x], to_x).wait_send()


def mix_kernel(part, out, from_core, held, from_y, ssem, rsem):
    sp, tp = lax.axis_index("sp"), lax.axis_index("tp")
    y, c = tp // 2, tp % 2
    to_core = {"sp": sp, "tp": y * 2 + (1 - c)}
    to_y = {"sp": sp, "tp": (1 - y) * 2 + c}

    def move(i, src, dst, device):
        return pltpu.make_async_remote_copy(
            src_ref=src, dst_ref=dst, send_sem=ssem.at[i], recv_sem=rsem.at[i],
            device_id=device, device_id_type=pl.DeviceIdType.MESH,
        )

    greet([to_core, to_y])
    far = move(0, part.at[1 - y, 1 - c], from_core.at[0], to_core)
    near = move(1, part.at[y, 1 - c], from_core.at[1], to_core)
    far.start()
    near.start()
    far.wait_recv()
    held[0] = (
        part[1 - y, c].astype(jnp.float32) + from_core[0].astype(jnp.float32)
    ).astype(jnp.bfloat16)
    across = move(2, held.at[0], from_y, to_y)
    across.start()
    near.wait_recv()
    mine = part[y, c].astype(jnp.float32) + from_core[1].astype(jnp.float32)
    across.wait_recv()
    out[...] = mine + from_y[...].astype(jnp.float32)
    far.wait_send()
    near.wait_send()
    across.wait_send()


def retention(query_rows, key_rows, value_rows, gate_rows, log_decay, head_gain):
    length, local_heads = log_decay.shape
    width = query_rows.shape[1]
    sp_count, mine = lax.axis_size("sp"), lax.axis_index("sp")
    positions = (mine * length + jnp.arange(length, dtype=jnp.int32)).astype(jnp.float32)
    angles = rotary_angles(positions, HEAD_DIM)
    cosine, sine = jnp.cos(angles), jnp.sin(angles)
    cosine = jnp.concatenate([cosine, cosine], axis=1)
    sine = jnp.concatenate([-sine, sine], axis=1)
    cumulative = jnp.cumsum(log_decay, axis=0)
    rows_spec = pl.BlockSpec((length, HEAD_DIM), lambda h: (0, h))
    table_spec = pl.BlockSpec((length, HEAD_DIM), lambda h: (0, 0))
    retained, qdec, state = pl.pallas_call(
        retention_kernel,
        grid=(local_heads,),
        out_shape=(
            jax.ShapeDtypeStruct((length, width), jnp.float32),
            jax.ShapeDtypeStruct((length, width), jnp.bfloat16),
            jax.ShapeDtypeStruct((local_heads, HEAD_DIM + 8, HEAD_DIM), jnp.float32),
        ),
        in_specs=[
            rows_spec,
            rows_spec,
            rows_spec,
            table_spec,
            table_spec,
            pl.BlockSpec((length, local_heads), lambda h: (0, 0)),
            pl.BlockSpec((1, 1, length), lambda h: (h, 0, 0)),
        ],
        out_specs=(
            rows_spec,
            rows_spec,
            pl.BlockSpec((1, HEAD_DIM + 8, HEAD_DIM), lambda h: (h, 0, 0)),
        ),
    )(query_rows, key_rows, value_rows, cosine, sine, cumulative, cumulative.T[:, None, :])
    if sp_count % 2 == 0 and local_heads <= 8 and sp_count <= 16:
        totals = jnp.broadcast_to(state[:, HEAD_DIM, :1], (local_heads, HEAD_DIM))
        totals = jnp.pad(totals, ((0, 8 - local_heads), (0, 0)))
        planes = sp_count // 2
        block = (local_heads, HEAD_DIM, HEAD_DIM)
        entering = pl.pallas_call(
            functools.partial(state_kernel, planes),
            out_shape=jax.ShapeDtypeStruct(block, jnp.bfloat16),
            in_specs=[pl.BlockSpec(memory_space=pltpu.VMEM)] * 2,
            out_specs=pl.BlockSpec(memory_space=pltpu.VMEM),
            scratch_shapes=[
                pltpu.VMEM((planes, 2) + block, jnp.bfloat16),
                pltpu.VMEM((planes, 2, 8, HEAD_DIM), jnp.float32),
                pltpu.SemaphoreType.DMA((4, planes)),
                pltpu.SemaphoreType.DMA((4, planes)),
                pltpu.SemaphoreType.DMA((2,)),
            ],
            compiler_params=pltpu.CompilerParams(collective_id=1, has_side_effects=True),
        )(state[:, :HEAD_DIM, :].astype(jnp.bfloat16), totals)
    else:
        pieces = lax.all_gather(state, "sp")
        totals = pieces[:, :, HEAD_DIM, 0]
        index = jnp.arange(sp_count, dtype=jnp.int32)
        between = (index[None, :] > index[:, None]) & (index[None, :] < mine)
        gap = jnp.sum(jnp.where(between[:, :, None], totals[None], 0.0), axis=1)
        factor = jnp.where((index < mine)[:, None], jnp.exp(gap), 0.0)
        entering = jnp.sum(factor[:, :, None, None] * pieces[:, :, :HEAD_DIM, :], axis=0)
    return pl.pallas_call(
        norm_kernel,
        grid=(local_heads,),
        out_shape=jax.ShapeDtypeStruct((length, width), jnp.bfloat16),
        in_specs=[
            rows_spec,
            rows_spec,
            pl.BlockSpec((1, HEAD_DIM, HEAD_DIM), lambda h: (h, 0, 0)),
            pl.BlockSpec((1, HEAD_DIM), lambda h: (0, h)),
            rows_spec,
        ],
        out_specs=rows_spec,
    )(retained, qdec, entering, head_gain[None, :], gate_rows)


Z_A, Z_B, X_A2, Y_B2, Y_A3, Y_A4, X_B3, X_B4, C_A, C_B, C_P, Y_A, X_B, X_A, Y_B, RZ_A, RZ_B = range(17)


def experts_kernel(
    planes, x0, x1, upd, wg_hbm, wu_hbm, wd_hbm, out,
    wg, wu, wd, g0, g1, pm, pr, a0, a1, r10, r11, b0, b1, r20, r21, d0, d1, z0, z1,
    ssem, rsem, lsem, wsem,
):
    sp, tp = lax.axis_index("sp"), lax.axis_index("tp")
    sp_count = 2 * planes
    z, x = sp // 2, sp % 2
    y, c = tp // 2, tp % 2
    half = x1.shape[1]
    rows = x1.shape[0] // 2
    items = 2 * planes
    f32, bf16 = jnp.float32, jnp.bfloat16
    to_core = {"sp": sp, "tp": y * 2 + (1 - c)}
    to_y = {"sp": sp, "tp": (1 - y) * 2 + c}
    to_x = {"sp": z * 2 + (1 - x), "tp": tp}

    def item_of(i, r):
        return (items - 1) * r if i == 0 else 2 * i - 1 + r

    def turn_of(n):
        return ((n + 1) // 2) % planes

    def to_z(i):
        return {"sp": ((z + planes - i) % planes) * 2 + x, "tp": tp}

    def from_z(i):
        return {"sp": ((z + i) % planes) * 2 + x, "tp": tp}

    def move(kind, n, src, dst, device):
        return pltpu.make_async_remote_copy(
            src_ref=src, dst_ref=dst, send_sem=ssem.at[kind, n], recv_sem=rsem.at[kind, n],
            device_id=device, device_id_type=pl.DeviceIdType.MESH,
        )

    def send(kind, n, src, dst, device):
        move(kind, n, src, dst, device).start()

    def arrived(kind, n, dst):
        move(kind, n, dst, dst, to_core).wait_recv()

    def left(kind, n, src):
        move(kind, n, src, src, to_core).wait_send()

    barrier = pltpu.get_barrier_semaphore()
    for device in [to_core, to_y, to_x] + [to_z(i) for i in range(1, planes)]:
        pl.semaphore_signal(barrier, inc=1, device_id=device, device_id_type=pl.DeviceIdType.MESH)

    here = x * 2 + y
    other_x = (1 - x) * 2 + y
    other_y = x * 2 + (1 - y)
    other_xy = (1 - x) * 2 + (1 - y)
    own = []
    for r in range(2):
        n, part = item_of(0, r), pl.ds(r * rows, rows)
        own.append(pltpu.make_async_copy(x0.at[part], g0.at[c, n, here], lsem.at[2 * r]))
        own.append(pltpu.make_async_copy(x1.at[part], g1.at[c, n, here], lsem.at[2 * r + 1]))
    for copy in own:
        copy.start()
    weights = [
        pltpu.make_async_copy(wg_hbm, wg, wsem.at[0]),
        pltpu.make_async_copy(wu_hbm, wu, wsem.at[1]),
        pltpu.make_async_copy(wd_hbm, wd, wsem.at[2]),
    ]
    for copy in weights:
        copy.start()
    for copy in own:
        copy.wait()
    pl.semaphore_wait(barrier, 2 + planes)

    def spread(n):
        send(X_A2, n, g0.at[c, n, here], g0.at[c, n, here], to_x)
        send(Y_B2, n, g1.at[c, n, here], g1.at[c, n, here], to_y)
        send(Y_A3, n, g0.at[c, n, here], g0.at[c, n, here], to_y)
        send(X_B3, n, g1.at[c, n, here], g1.at[c, n, here], to_x)

    spread(0)
    for i in range(1, planes):
        for r in range(2):
            n, m = item_of(i, r), item_of(0, r)
            send(Z_A, n, g0.at[c, m, here], g0.at[c, n, here], from_z(i))
            send(Z_B, n, g1.at[c, m, here], g1.at[c, n, here], from_z(i))

    def tick(t, carry):
        @pl.when(t < items)
        def _():
            arrived(X_A2, t, g0.at[c, t, other_x])
            send(Y_A4, t, g0.at[c, t, other_x], g0.at[c, t, other_x], to_y)
            arrived(Y_B2, t, g1.at[c, t, other_y])
            send(X_B4, t, g1.at[c, t, other_y], g1.at[c, t, other_y], to_x)

        @pl.when(t + 1 < items)
        def _():
            n = t + 1

            @pl.when(n < items - 1)
            def _():
                arrived(Z_A, n, g0.at[c, n, here])
                arrived(Z_B, n, g1.at[c, n, here])

            spread(n)

        @pl.when(t == 2)
        def _():
            for copy in weights:
                copy.wait()

        @pl.when((t >= 2) & (t < items + 2))
        def _():
            n = t - 2
            arrived(C_A, n, g0.at[1 - c, n])
            arrived(C_B, n, g1.at[1 - c, n])
            lead = g0[:, n].reshape(8 * rows, half + 128)
            tail = lead[:, half:].astype(f32)
            lead = lead[:, :half]
            rest = g1[:, n].reshape(8 * rows, half)
            lane = lax.broadcasted_iota(jnp.int32, tail.shape, 1)
            weight = jnp.sum(
                jnp.where((lane == sp) | (lane == sp + sp_count), tail, 0.0), axis=1, keepdims=True
            )

            def product(w):
                return jnp.dot(lead, w[:half, :], preferred_element_type=f32) + jnp.dot(
                    rest, w[half:, :], preferred_element_type=f32
                )

            gate = jnp.minimum(product(wg), clamp_limit)
            up = jnp.clip(product(wu), -clamp_limit, clamp_limit)
            act = ((up + 1.0) * (gate / (1.0 + jnp.exp(-swish_alpha * gate)))).astype(bf16)
            made = (jnp.dot(act, wd[...], preferred_element_type=f32) * weight).astype(bf16)
            pm[n] = made.reshape(2, 4 * rows, 2 * half)
            send(C_P, n, pm.at[n, 1 - c], pr.at[n], to_core)

        @pl.when((t >= 1) & (t < items + 1))
        def _():
            n = t - 1
            arrived(Y_A3, n, g0.at[c, n, other_y])
            arrived(Y_A4, n, g0.at[c, n, other_xy])
            arrived(X_B3, n, g1.at[c, n, other_x])
            arrived(X_B4, n, g1.at[c, n, other_xy])
            send(C_A, n, g0.at[c, n], g0.at[c, n], to_core)
            send(C_B, n, g1.at[c, n], g1.at[c, n], to_core)

        @pl.when((t >= 3) & (t < items + 3))
        def _():
            n = t - 3
            arrived(C_P, n, pr.at[n])
            for q in range(4):
                part = pl.ds(q * rows, rows)
                total = (pm[n, c, part, :].astype(f32) + pr[n, part, :].astype(f32)).astype(bf16)
                a0[n, q % 2, q // 2] = total[:, :half]
                a1[n, q // 2, q % 2] = total[:, half:]
            send(Y_A, n, a0.at[n, 1 - y], r10.at[n], to_y)
            send(X_B, n, a1.at[n, 1 - x], r11.at[n], to_x)

        @pl.when((t >= 4) & (t < items + 4))
        def _():
            n = t - 4
            arrived(Y_A, n, r10.at[n])
            b0[n] = (a0[n, y].astype(f32) + r10[n].astype(f32)).astype(bf16)
            send(X_A, n, b0.at[n, 1 - x], r20.at[n], to_x)
            arrived(X_B, n, r11.at[n])
            b1[n] = (a1[n, x].astype(f32) + r11[n].astype(f32)).astype(bf16)
            send(Y_B, n, b1.at[n, 1 - y], r21.at[n], to_y)

        @pl.when(t >= 5)
        def _():
            n = t - 5
            arrived(X_A, n, r20.at[n])
            d0[n] = (b0[n, x].astype(f32) + r20[n].astype(f32)).astype(bf16)
            arrived(Y_B, n, r21.at[n])
            d1[n] = (b1[n, y].astype(f32) + r21[n].astype(f32)).astype(bf16)

            @pl.when((n > 0) & (n < items - 1))
            def _():
                send(RZ_A, n, d0.at[n], z0.at[n], to_z(turn_of(n)))
                send(RZ_B, n, d1.at[n], z1.at[n], to_z(turn_of(n)))

        return carry

    lax.fori_loop(0, items + 5, tick, 0)
    for r in range(2):
        n, part = item_of(0, r), pl.ds(r * rows, rows)
        low = upd[part, :half] + d0[n].astype(f32)
        high = upd[part, half:] + d1[n].astype(f32)
        for i in range(1, planes):
            n = item_of(i, r)
            arrived(RZ_A, n, z0.at[n])
            low = low + z0[n].astype(f32)
            arrived(RZ_B, n, z1.at[n])
            high = high + z1[n].astype(f32)
        out[part, :half] = low.astype(bf16)
        out[part, half:] = high.astype(bf16)

    def drain(n, carry):
        @pl.when((n > 0) & (n < items - 1))
        def _():
            left(Z_A, n, g0.at[c, n, here])
            left(Z_B, n, g1.at[c, n, here])
            left(RZ_A, n, d0.at[n])
            left(RZ_B, n, d1.at[n])

        left(X_A2, n, g0.at[c, n, here])
        left(Y_B2, n, g1.at[c, n, here])
        left(Y_A3, n, g0.at[c, n, here])
        left(X_B3, n, g1.at[c, n, here])
        left(Y_A4, n, g0.at[c, n, other_x])
        left(X_B4, n, g1.at[c, n, other_y])
        left(C_A, n, g0.at[c, n])
        left(C_B, n, g1.at[c, n])
        left(C_P, n, pm.at[n, 1 - c])
        left(Y_A, n, a0.at[n, 1 - y])
        left(X_B, n, a1.at[n, 1 - x])
        left(X_A, n, b0.at[n, 1 - x])
        left(Y_B, n, b1.at[n, 1 - y])
        return carry

    lax.fori_loop(0, items, drain, 0)


def dense_experts(updated, ffn_in, own_routes, route_weights, gate_part, up_part, down_part):
    sp_count, mine = lax.axis_size("sp"), lax.axis_index("sp")
    width = ffn_in.shape[1]
    chosen = own_routes[:, :, None] == jnp.arange(sp_count, dtype=jnp.int32)[None, None, :]
    shares = jnp.sum(jnp.where(chosen, route_weights[:, :, None], 0.0), axis=1)
    coarse = shares.astype(jnp.bfloat16)
    fine = (shares - coarse.astype(jnp.float32)).astype(jnp.bfloat16)
    spare = jnp.zeros((ffn_in.shape[0], 128 - 2 * sp_count), jnp.bfloat16)
    half = width // 2
    first = jnp.concatenate([ffn_in[:, :half], coarse, fine, spare], axis=1)
    second = ffn_in[:, half:]
    planes = sp_count // 2
    items = 2 * planes
    rows = ffn_in.shape[0] // 2
    bf16 = jnp.bfloat16
    whole = pl.BlockSpec(memory_space=pltpu.VMEM)
    far = pl.BlockSpec(memory_space=pl.ANY)
    return pl.pallas_call(
        functools.partial(experts_kernel, planes),
        out_shape=jax.ShapeDtypeStruct((2 * rows, width), bf16),
        in_specs=[whole] * 3 + [far] * 3,
        out_specs=whole,
        scratch_shapes=[
            pltpu.VMEM(gate_part.shape, bf16),
            pltpu.VMEM(up_part.shape, bf16),
            pltpu.VMEM(down_part.shape, bf16),
            pltpu.VMEM((2, items, 4, rows, half + 128), bf16),
            pltpu.VMEM((2, items, 4, rows, half), bf16),
            pltpu.VMEM((items, 2, 4 * rows, width), bf16),
            pltpu.VMEM((items, 4 * rows, width), bf16),
            pltpu.VMEM((items, 2, 2, rows, half), bf16),
            pltpu.VMEM((items, 2, 2, rows, half), bf16),
            pltpu.VMEM((items, 2, rows, half), bf16),
            pltpu.VMEM((items, 2, rows, half), bf16),
            pltpu.VMEM((items, 2, rows, half), bf16),
            pltpu.VMEM((items, 2, rows, half), bf16),
            pltpu.VMEM((items, rows, half), bf16),
            pltpu.VMEM((items, rows, half), bf16),
            pltpu.VMEM((items, rows, half), bf16),
            pltpu.VMEM((items, rows, half), bf16),
            pltpu.VMEM((items, rows, half), bf16),
            pltpu.VMEM((items, rows, half), bf16),
            pltpu.SemaphoreType.DMA((17, items)),
            pltpu.SemaphoreType.DMA((17, items)),
            pltpu.SemaphoreType.DMA((4,)),
            pltpu.SemaphoreType.DMA((3,)),
        ],
        compiler_params=pltpu.CompilerParams(
            collective_id=0, has_side_effects=True, vmem_limit_bytes=63 * 1024 * 1024
        ),
    )(first, second, updated, gate_part, up_part, down_part)


def body(
    query_rows,
    key_rows,
    value_rows,
    gate_rows,
    log_decay,
    head_gain,
    out_weight,
    residual,
    ffn_gain,
    gate_weight,
    up_weight,
    down_weight,
    routes,
    route_weights,
):
    tok_count = query_rows.shape[0]
    local_heads = log_decay.shape[1]
    sp_count = lax.axis_size("sp")
    tp_count = lax.axis_size("tp")
    model_width = residual.shape[1]
    rows_own = tok_count // tp_count
    capacity = max(2, 3 * rows_own * TOPK // (2 * sp_count))
    hidden = retention(query_rows, key_rows, value_rows, gate_rows, log_decay, head_gain)
    mixed = jnp.dot(hidden, out_weight, preferred_element_type=jnp.float32).astype(jnp.bfloat16)
    if tp_count == 4 and sp_count <= 16:
        mixed_sum = pl.pallas_call(
            mix_kernel,
            out_shape=jax.ShapeDtypeStruct((rows_own, model_width), jnp.float32),
            in_specs=[pl.BlockSpec(memory_space=pltpu.VMEM)],
            out_specs=pl.BlockSpec(memory_space=pltpu.VMEM),
            scratch_shapes=[
                pltpu.VMEM((2, rows_own, model_width), jnp.bfloat16),
                pltpu.VMEM((2, rows_own, model_width), jnp.bfloat16),
                pltpu.VMEM((rows_own, model_width), jnp.bfloat16),
                pltpu.SemaphoreType.DMA((3,)),
                pltpu.SemaphoreType.DMA((3,)),
            ],
            compiler_params=pltpu.CompilerParams(collective_id=2, has_side_effects=True),
        )(mixed.reshape(2, 2, rows_own, model_width))
    else:
        mixed_sum = lax.psum_scatter(mixed, "tp", scatter_dimension=0, tiled=True).astype(
            jnp.float32
        )
    updated = residual.astype(jnp.float32) + mixed_sum
    ffn_in = square_norm(updated, ffn_gain)
    tp_index = lax.axis_index("tp")
    own_routes = lax.dynamic_slice_in_dim(routes, tp_index * rows_own, rows_own, 0)
    if rows_own < 2 * capacity and 2 * sp_count <= 128 and sp_count % 2 == 0 and tp_count == 4:
        return dense_experts(
            updated, ffn_in, own_routes, route_weights, gate_weight[0], up_weight[0], down_weight[0]
        )
    own_experts, own_ranks = slot_ranks(own_routes, sp_count)
    home_slot = own_experts * capacity + own_ranks
    gate_part = gate_weight[0]
    up_part = up_weight[0]
    down_part = down_weight[0]
    empty_row = jnp.zeros((1, model_width), jnp.bfloat16)
    source_row = (
        jnp.full((sp_count * capacity,), rows_own, jnp.int32)
        .at[home_slot]
        .set(jnp.arange(rows_own * TOPK, dtype=jnp.int32) // TOPK)
    )
    padded = jnp.concatenate([ffn_in, empty_row], axis=0)
    outgoing = padded[source_row].reshape(sp_count, capacity, model_width)
    arrived = lax.all_to_all(outgoing, "sp", split_axis=0, concat_axis=0, tiled=True)
    fanned = lax.all_gather(arrived[None], "tp", axis=0, tiled=True)
    activity = expert_rows(fanned.reshape(-1, model_width), gate_part, up_part)
    partial_out = jnp.dot(activity, down_part, preferred_element_type=jnp.float32).reshape(
        tp_count, sp_count, capacity, model_width
    )
    summed = (
        lax.psum_scatter(partial_out.astype(jnp.bfloat16), "tp", scatter_dimension=0, tiled=True)
        .astype(jnp.float32)
        .reshape(sp_count, capacity, model_width)
    )
    returned = lax.all_to_all(
        summed.astype(jnp.bfloat16), "sp", split_axis=0, concat_axis=0, tiled=True
    )
    picked = returned.reshape(sp_count * capacity, model_width)[home_slot].reshape(
        rows_own, TOPK, model_width
    )
    expert_sum = jnp.sum(route_weights[:, :, None] * picked.astype(jnp.float32), axis=1)
    return (updated + expert_sum).astype(jnp.bfloat16)


def solution(mesh):
    return jax.shard_map(
        body,
        mesh=mesh,
        in_specs=(
            P("sp", "tp"),
            P("sp", "tp"),
            P("sp", "tp"),
            P("sp", "tp"),
            P("sp", "tp"),
            P("tp"),
            P("tp", None),
            P(("sp", "tp"), None),
            P(),
            P("sp", None, "tp"),
            P("sp", None, "tp"),
            P("sp", "tp", None),
            P("sp", None),
            P(("sp", "tp"), None),
        ),
        out_specs=P(("sp", "tp"), None),
        check_vma=False,
    )
```

```python
import functools

import jax
import jax.numpy as jnp
import numpy as np
from jax import lax
from jax.experimental import pallas as pl
from jax.experimental.pallas import tpu as pltpu
from jax.sharding import PartitionSpec as P

HEAD_DIM = 128
TOPK = 4
BLOCK = 128


highest = lax.Precision.HIGHEST
rope_base = 10000.0
group_eps = 1e-05
square_eps = 1e-06
clamp_limit = 7.0
swish_alpha = 1.702


def rotary_angles(positions, head_dim):
    half_dim = head_dim // 2
    inverse = rope_base ** (-jnp.arange(half_dim, dtype=jnp.float32) / half_dim)
    return positions[:, None] * inverse[None, :]


def square_norm(updated, gain_row):
    factor = lax.rsqrt(jnp.mean(updated * updated, axis=-1, keepdims=True) + square_eps)
    return (updated * factor * gain_row).astype(jnp.bfloat16)


def expert_rows(rows, gate_part, up_part):
    gate_pre = jnp.dot(rows, gate_part, preferred_element_type=jnp.float32)
    up_pre = jnp.dot(rows, up_part, preferred_element_type=jnp.float32)
    gate_clip = jnp.minimum(gate_pre, clamp_limit)
    up_clip = jnp.clip(up_pre, -clamp_limit, clamp_limit)
    return ((up_clip + 1.0) * (gate_clip * jax.nn.sigmoid(gate_clip * swish_alpha))).astype(
        jnp.bfloat16
    )


def slot_ranks(route_block, experts):
    flat_routes = route_block.reshape(-1)
    onehot = (flat_routes[:, None] == jnp.arange(experts, dtype=jnp.int32)[None, :]).astype(
        jnp.int32
    )
    return (flat_routes, jnp.sum(jnp.cumsum(onehot, axis=0) * onehot, axis=1) - 1)


def retention_kernel(q_ref, k_ref, v_ref, cos_ref, sin_ref, cum_ref, cum_row_ref, ret_ref, qdec_ref, state_ref):
    head = pl.program_id(0)
    length = q_ref.shape[0]
    cosine, sine = cos_ref[...], sin_ref[...]
    half = HEAD_DIM // 2

    def turned(ref):
        rows = ref[...].astype(jnp.float32)
        return rows * cosine + pltpu.roll(rows, half, 1) * sine

    lanes = lax.broadcasted_iota(jnp.int32, cum_ref.shape, 1)
    column = jnp.sum(jnp.where(lanes == head, cum_ref[...], 0.0), axis=1, keepdims=True)
    row = cum_row_ref[0]
    queries = turned(q_ref)
    keys = turned(k_ref) * HEAD_DIM ** (-0.5)
    values = v_ref[...]
    scores = lax.dot_general(
        queries.astype(jnp.bfloat16),
        keys.astype(jnp.bfloat16),
        (((1,), (1,)), ((), ())),
        preferred_element_type=jnp.float32,
    )
    causal = lax.broadcasted_iota(jnp.int32, (length, length), 0) >= lax.broadcasted_iota(
        jnp.int32, (length, length), 1
    )
    weights = jnp.where(causal, jnp.exp(jnp.minimum(column - row, 0.0)), 0.0)
    ret_ref[...] = jnp.dot(
        (scores * weights).astype(jnp.bfloat16), values, preferred_element_type=jnp.float32
    )
    qdec_ref[...] = (queries * jnp.exp(column)).astype(jnp.bfloat16)
    total = column[length - 1 :, :]
    tailed = (keys * jnp.exp(total - column)).astype(jnp.bfloat16)
    state_ref[0, :HEAD_DIM, :] = lax.dot_general(
        tailed, values, (((0,), (0,)), ((), ())), preferred_element_type=jnp.float32
    )
    state_ref[0, HEAD_DIM:, :] = jnp.broadcast_to(total, (8, HEAD_DIM))


def norm_kernel(ret_ref, qdec_ref, enter_ref, gain_ref, gate_ref, hidden_ref):
    retained = ret_ref[...] + jnp.dot(
        qdec_ref[...], enter_ref[0].astype(jnp.bfloat16), preferred_element_type=jnp.float32
    )
    centred = retained - jnp.mean(retained, axis=-1, keepdims=True)
    variance = jnp.mean(centred * centred, axis=-1, keepdims=True)
    gate = gate_ref[...].astype(jnp.float32)
    scaled = centred * lax.rsqrt(variance + group_eps) * gain_ref[...]
    hidden_ref[...] = (scaled * (gate / (1.0 + jnp.exp(-gate)))).astype(jnp.bfloat16)


def retention(query_rows, key_rows, value_rows, gate_rows, log_decay, head_gain):
    length, local_heads = log_decay.shape
    width = query_rows.shape[1]
    sp_count, mine = lax.axis_size("sp"), lax.axis_index("sp")
    positions = (mine * length + jnp.arange(length, dtype=jnp.int32)).astype(jnp.float32)
    angles = rotary_angles(positions, HEAD_DIM)
    cosine, sine = jnp.cos(angles), jnp.sin(angles)
    cosine = jnp.concatenate([cosine, cosine], axis=1)
    sine = jnp.concatenate([-sine, sine], axis=1)
    cumulative = jnp.cumsum(log_decay, axis=0)
    rows_spec = pl.BlockSpec((length, HEAD_DIM), lambda h: (0, h))
    table_spec = pl.BlockSpec((length, HEAD_DIM), lambda h: (0, 0))
    retained, qdec, state = pl.pallas_call(
        retention_kernel,
        grid=(local_heads,),
        out_shape=(
            jax.ShapeDtypeStruct((length, width), jnp.float32),
            jax.ShapeDtypeStruct((length, width), jnp.bfloat16),
            jax.ShapeDtypeStruct((local_heads, HEAD_DIM + 8, HEAD_DIM), jnp.float32),
        ),
        in_specs=[
            rows_spec,
            rows_spec,
            rows_spec,
            table_spec,
            table_spec,
            pl.BlockSpec((length, local_heads), lambda h: (0, 0)),
            pl.BlockSpec((1, 1, length), lambda h: (h, 0, 0)),
        ],
        out_specs=(
            rows_spec,
            rows_spec,
            pl.BlockSpec((1, HEAD_DIM + 8, HEAD_DIM), lambda h: (h, 0, 0)),
        ),
    )(query_rows, key_rows, value_rows, cosine, sine, cumulative, cumulative.T[:, None, :])
    pieces = lax.all_gather(state, "sp")
    totals = pieces[:, :, HEAD_DIM, 0]
    index = jnp.arange(sp_count, dtype=jnp.int32)
    between = (index[None, :] > index[:, None]) & (index[None, :] < mine)
    gap = jnp.sum(jnp.where(between[:, :, None], totals[None], 0.0), axis=1)
    factor = jnp.where((index < mine)[:, None], jnp.exp(gap), 0.0)
    entering = jnp.sum(factor[:, :, None, None] * pieces[:, :, :HEAD_DIM, :], axis=0)
    return pl.pallas_call(
        norm_kernel,
        grid=(local_heads,),
        out_shape=jax.ShapeDtypeStruct((length, width), jnp.bfloat16),
        in_specs=[
            rows_spec,
            rows_spec,
            pl.BlockSpec((1, HEAD_DIM, HEAD_DIM), lambda h: (h, 0, 0)),
            pl.BlockSpec((1, HEAD_DIM), lambda h: (0, h)),
            rows_spec,
        ],
        out_specs=rows_spec,
    )(retained, qdec, entering, head_gain[None, :], gate_rows)


(
    UP_A, UP_B, DOWN_A, DOWN_B, X_A2, Y_B2, Y_A3, Y_A4, X_B3, X_B4, C_A, C_B, C_P, Y_A, X_B, X_A, Y_B, RZ_A, RZ_B,
    TOTAL, CHAIN, ACROSS, MIX_C, MIX_Y,
) = range(24)


def layer_kernel(
    planes, q_ref, k_ref, v_ref, gate_ref, logs, head_gain, near_table, base_table, residual, ffn_gain, shares,
    wo_hbm, wg_hbm, wu_hbm, wd_hbm, out,
    wo, wg, wu, wd, rotary, turned_k, ret, qdec, state, cum_col, cum_row, total_own, total_x, carry_in, carry_out,
    side_out, side_in, hidden, blend, from_core, held, from_y, upd,
    g0, g1, pm, pr, a0, a1, r10, r11, b0, b1, r20, r21, d0, d1, z0, z1,
    ssem, rsem, wsem,
):
    sp, tp = lax.axis_index("sp"), lax.axis_index("tp")
    sp_count = 2 * planes
    z, x = sp // 2, sp % 2
    y, c = tp // 2, tp % 2
    own_rows, width = out.shape
    half = width // 2
    rows = own_rows // 2
    items = 2 * planes
    lag = items - 3
    f32, bf16 = jnp.float32, jnp.bfloat16
    to_core = {"sp": sp, "tp": y * 2 + (1 - c)}
    to_y = {"sp": sp, "tp": (1 - y) * 2 + c}
    to_x = {"sp": z * 2 + (1 - x), "tp": tp}

    def half_of(n):
        return jnp.where(n == items - 1, 1, jnp.where(n == 0, 0, (n + 1) % 2))

    def plane_at(k):
        low = z < planes // 2
        mirrored = jnp.where(low, z, planes - 1 - z)
        q = jnp.where(k <= mirrored, mirrored - k, k)
        return jnp.where(low, q, planes - 1 - q)

    def plane_of(n):
        return plane_at(((n + 1) // 2) % planes)

    def item_of(n):
        return 2 * plane_of(n) + half_of(n)

    def step_of(turn):
        back = items - 3 - 2 * ((turn - 1) // 2) + (turn - 1) % 2
        return jnp.where((turn == 0) | (turn == items - 1), turn, back)

    def turn_at(u):
        return jnp.where(u == 0, 0, u - 1)

    def has_turn(u):
        return (u == 0) | ((u >= 2) & (u <= items))

    def at_plane(p):
        return {"sp": p * 2 + x, "tp": tp}

    def to_z(i):
        return at_plane((z + planes - i) % planes)

    def move(kind, n, src, dst, device, m=None):
        return pltpu.make_async_remote_copy(
            src_ref=src, dst_ref=dst, send_sem=ssem.at[kind, n],
            recv_sem=rsem.at[kind, n if m is None else m],
            device_id=device, device_id_type=pl.DeviceIdType.MESH,
        )

    def send(kind, n, src, dst, device, m=None):
        move(kind, n, src, dst, device, m).start()

    def arrived(kind, n, dst):
        move(kind, n, dst, dst, to_core).wait_recv()

    def left(kind, n, src):
        move(kind, n, src, src, to_core).wait_send()

    barrier = pltpu.get_barrier_semaphore()
    for device in [to_core, to_y, to_x] + [to_z(i) for i in range(1, planes)]:
        pl.semaphore_signal(barrier, inc=1, device_id=device, device_id_type=pl.DeviceIdType.MESH)

    weights = [
        pltpu.make_async_copy(wo_hbm, wo, wsem.at[0]),
        pltpu.make_async_copy(wg_hbm, wg, wsem.at[1]),
        pltpu.make_async_copy(wu_hbm, wu, wsem.at[2]),
        pltpu.make_async_copy(wd_hbm, wd, wsem.at[3]),
    ]
    for copy in weights:
        copy.start()

    length = q_ref.shape[0]
    heads = state.shape[0]
    dim = HEAD_DIM
    after = lax.broadcasted_iota(jnp.int32, (length, length), 0) >= lax.broadcasted_iota(
        jnp.int32, (length, length), 1
    )
    ones = jnp.where(after, 1.0, 0.0).astype(f32)
    log_rows = jnp.concatenate([logs[...], jnp.zeros((8 - heads, length), f32)], axis=0)
    cum_row[...] = lax.dot_general(
        log_rows, ones, (((1,), (1,)), ((), ())), precision=highest, preferred_element_type=f32
    )
    cum_col[...] = lax.dot_general(
        ones, log_rows, (((1,), (1,)), ((), ())), precision=highest, preferred_element_type=f32
    )
    total_own[...] = jnp.broadcast_to(cum_row[:, length - 1 :], (8, dim))
    pl.semaphore_wait(barrier, 2 + planes)
    send(TOTAL, 0, total_own, total_x, to_x)

    base = base_table[pl.ds(sp * 8, 8), :]
    cosine = base[0:1] * near_table[0] - base[1:2] * near_table[1]
    sine = base[2:3] * near_table[0] + base[3:4] * near_table[1]
    rotary[0] = cosine
    rotary[1] = sine

    def turned(rows_in):
        wide = rows_in.astype(f32)
        return wide * rotary[0] + pltpu.roll(wide, dim // 2, 1) * rotary[1]

    def column_of(h):
        lanes = lax.broadcasted_iota(jnp.int32, cum_col.shape, 1)
        return jnp.sum(jnp.where(lanes == h, cum_col[...], 0.0), axis=1, keepdims=True)

    for h in range(heads):
        lanes = pl.ds(h * dim, dim)
        keys = turned(k_ref[:, lanes]) * dim ** (-0.5)
        turned_k[:, lanes] = keys.astype(bf16)
        column = column_of(h)
        tailed = (keys * jnp.exp(column[length - 1 :, :] - column)).astype(bf16)
        state[h] = lax.dot_general(
            tailed, v_ref[:, lanes], (((0,), (0,)), ((), ())), preferred_element_type=f32
        )

    def attend(h, carry):
        lanes = pl.ds(pl.multiple_of(h * dim, dim), dim)
        queries = turned(q_ref[:, lanes])
        column = column_of(h)
        scores = lax.dot_general(
            queries.astype(bf16), turned_k[:, lanes], (((1,), (1,)), ((), ())), preferred_element_type=f32
        )
        gap = jnp.minimum(column - cum_row[pl.ds(h, 1), :], 0.0)
        decays = jnp.where(after, jnp.exp(gap), 0.0)
        ret[:, lanes] = jnp.dot((scores * decays).astype(bf16), v_ref[:, lanes], preferred_element_type=f32)
        qdec[:, lanes] = (queries * jnp.exp(column)).astype(bf16)
        return carry

    early = jnp.where(z >= planes // 2, heads, 0)
    lax.fori_loop(0, early, attend, 0)

    arrived(TOTAL, 0, total_x)
    left_side = x == 0
    for h in range(heads):
        own_total, x_total = total_own[h : h + 1, :], total_x[h : h + 1, :]

        @pl.when(z > 0)
        def _():
            arrived(CHAIN, h, carry_in.at[h])

        @pl.when(z == 0)
        def _():
            carry_in[h] = jnp.zeros((dim, dim), bf16)

        before = carry_in[h].astype(f32)

        @pl.when(z + 1 < planes)
        def _():
            fresh = jnp.where(left_side, jnp.exp(x_total), 1.0) * state[h]
            carry_out[h] = (jnp.exp(own_total + x_total) * before + fresh).astype(bf16)
            send(CHAIN, h, carry_out.at[h], carry_in.at[h], at_plane(z + 1))

        side_out[h] = jnp.where(left_side, jnp.exp(own_total) * before + state[h], before).astype(bf16)
        send(ACROSS, h, side_out.at[h], side_in.at[h], to_x)

    lax.fori_loop(early, heads, attend, 0)

    for h in range(heads):
        lanes = pl.ds(h * dim, dim)
        arrived(ACROSS, h, side_in.at[h])
        factor = jnp.where(left_side, 1.0, jnp.exp(total_x[h : h + 1, :]))
        entering = (factor * carry_in[h].astype(f32) + side_in[h].astype(f32)).astype(bf16)
        retained = ret[:, lanes] + jnp.dot(qdec[:, lanes], entering, preferred_element_type=f32)
        centred = retained - jnp.mean(retained, axis=-1, keepdims=True)
        variance = jnp.mean(centred * centred, axis=-1, keepdims=True)
        gate_in = gate_ref[:, lanes].astype(f32)
        scaled = centred * lax.rsqrt(variance + group_eps) * head_gain[:, lanes]
        hidden[:, lanes] = (scaled * (gate_in / (1.0 + jnp.exp(-gate_in)))).astype(bf16)

    weights[0].wait()
    pieces = blend.shape[0]
    span = width // pieces

    def cross(j):
        arrived(MIX_C, j, from_core.at[j])
        held[j] = (blend[j, c, 1 - y].astype(f32) + from_core[j, 1 - y].astype(f32)).astype(bf16)
        send(MIX_Y, j, held.at[j], from_y.at[j], to_y)

    for j in range(pieces):
        mixed = jnp.dot(hidden[...], wo[:, pl.ds(j * span, span)], preferred_element_type=f32).astype(bf16)
        for q in range(4):
            blend[j, q % 2, q // 2] = mixed[q * own_rows : (q + 1) * own_rows, :]
        send(MIX_C, j, blend.at[j, 1 - c], from_core.at[j], to_core)
        if j > 0:
            cross(j - 1)
    cross(pieces - 1)
    square = jnp.zeros((own_rows, 1), f32)
    for j in range(pieces):
        cols = pl.ds(j * span, span)
        base_rows = residual[:, cols].astype(f32) + blend[j, c, y].astype(f32) + from_core[j, y].astype(f32)
        arrived(MIX_Y, j, from_y.at[j])
        total = base_rows + from_y[j].astype(f32)
        upd[:, cols] = total
        square = square + jnp.sum(total * total, axis=-1, keepdims=True)
    scale = lax.rsqrt(square * (1.0 / width) + square_eps)

    here = x * 2 + y
    other_x = (1 - x) * 2 + y
    other_y = x * 2 + (1 - y)
    other_xy = (1 - x) * 2 + (1 - y)
    share = jnp.transpose(shares[...])[:own_rows, :]
    coarse = share.astype(bf16).astype(f32)
    tail_rows = (coarse + pltpu.roll(share - coarse, sp_count, 1)).astype(bf16)
    for r in range(2):
        mine, n = slice(r * rows, (r + 1) * rows), 2 * z + r
        ready = (upd[mine, :] * scale[mine] * ffn_gain[...]).astype(bf16)
        g0[c, n, here, :, :half] = ready[:, :half]
        g0[c, n, here, :, half:] = tail_rows[mine]
        g1[c, n, here] = ready[:, half:]

    def spread(n):
        send(X_A2, n, g0.at[c, n, here], g0.at[c, n, here], to_x)
        send(Y_B2, n, g1.at[c, n, here], g1.at[c, n, here], to_y)
        send(Y_A3, n, g0.at[c, n, here], g0.at[c, n, here], to_y)
        send(X_B3, n, g1.at[c, n, here], g1.at[c, n, here], to_x)

    def raise_up(n):
        @pl.when(z + 1 < planes)
        def _():
            send(UP_A, n, g0.at[c, n, here], g0.at[c, n, here], at_plane(z + 1))
            send(UP_B, n, g1.at[c, n, here], g1.at[c, n, here], at_plane(z + 1))

    def hand_down(n):
        @pl.when(z > 0)
        def _():
            send(DOWN_A, n, g0.at[c, n, here], g0.at[c, n, here], at_plane(z - 1))
            send(DOWN_B, n, g1.at[c, n, here], g1.at[c, n, here], at_plane(z - 1))

    spread(2 * z)
    for r in range(2):
        raise_up(2 * z + r)
        hand_down(2 * z + r)

    def tick(t, carry):
        def relay():
            n = item_of(t)
            arrived(X_A2, n, g0.at[c, n, other_x])
            send(Y_A4, n, g0.at[c, n, other_x], g0.at[c, n, other_x], to_y)
            arrived(Y_B2, n, g1.at[c, n, other_y])
            send(X_B4, n, g1.at[c, n, other_y], g1.at[c, n, other_y], to_x)

        pl.when(t == 0)(relay)

        @pl.when(t + 1 < items)
        def _():
            k, r = (t + 2) // 2, t % 2

            @pl.when((t + 1 < items - 1) & (z - k >= 0))
            def _():
                n = 2 * (z - k) + r
                arrived(UP_A, n, g0.at[c, n, here])
                arrived(UP_B, n, g1.at[c, n, here])
                raise_up(n)

            @pl.when((t + 1 < items - 1) & (z + k < planes))
            def _():
                n = 2 * (z + k) + r
                arrived(DOWN_A, n, g0.at[c, n, here])
                arrived(DOWN_B, n, g1.at[c, n, here])
                hand_down(n)

            spread(item_of(t + 1))

        pl.when((t > 0) & (t < items))(relay)

        @pl.when(t == 2)
        def _():
            for copy in weights[1:]:
                copy.wait()

        @pl.when((t >= 2) & (t < items + 2))
        def _():
            n = item_of(t - 2)
            arrived(C_A, n, g0.at[1 - c, n])
            arrived(C_B, n, g1.at[1 - c, n])
            lead = g0[:, n].reshape(8 * rows, half + 128)
            tail = lead[:, half:].astype(f32)
            lead = lead[:, :half]
            rest = g1[:, n].reshape(8 * rows, half)
            lane = lax.broadcasted_iota(jnp.int32, tail.shape, 1)
            weight = jnp.sum(
                jnp.where((lane == sp) | (lane == sp + sp_count), tail, 0.0), axis=1, keepdims=True
            )

            def product(w):
                return jnp.dot(lead, w[:half, :], preferred_element_type=f32) + jnp.dot(
                    rest, w[half:, :], preferred_element_type=f32
                )

            gate = jnp.minimum(product(wg), clamp_limit)
            up = jnp.clip(product(wu), -clamp_limit, clamp_limit)
            act = ((up + 1.0) * (gate / (1.0 + jnp.exp(-swish_alpha * gate)))).astype(bf16)
            made = (jnp.dot(act, wd[...], preferred_element_type=f32) * weight).astype(bf16)
            pm[n] = made.reshape(2, 4 * rows, 2 * half)
            send(C_P, n, pm.at[n, 1 - c], pr.at[n], to_core)

        @pl.when((t >= 1) & (t < items + 1))
        def _():
            n = item_of(t - 1)
            arrived(Y_A3, n, g0.at[c, n, other_y])
            arrived(Y_A4, n, g0.at[c, n, other_xy])
            arrived(X_B3, n, g1.at[c, n, other_x])
            arrived(X_B4, n, g1.at[c, n, other_xy])
            send(C_A, n, g0.at[c, n], g0.at[c, n], to_core)
            send(C_B, n, g1.at[c, n], g1.at[c, n], to_core)

        @pl.when(has_turn(t - lag))
        def _():
            n = item_of(step_of(turn_at(t - lag)))
            arrived(C_P, n, pr.at[n])
            for q in range(4):
                part = pl.ds(q * rows, rows)
                total = (pm[n, c, part, :].astype(f32) + pr[n, part, :].astype(f32)).astype(bf16)
                a0[n, q % 2, q // 2] = total[:, :half]
                a1[n, q // 2, q % 2] = total[:, half:]
            send(Y_A, n, a0.at[n, 1 - y], r10.at[n], to_y)
            send(X_B, n, a1.at[n, 1 - x], r11.at[n], to_x)

        @pl.when(has_turn(t - lag - 1))
        def _():
            n = item_of(step_of(turn_at(t - lag - 1)))
            arrived(Y_A, n, r10.at[n])
            b0[n] = (a0[n, y].astype(f32) + r10[n].astype(f32)).astype(bf16)
            send(X_A, n, b0.at[n, 1 - x], r20.at[n], to_x)
            arrived(X_B, n, r11.at[n])
            b1[n] = (a1[n, x].astype(f32) + r11[n].astype(f32)).astype(bf16)
            send(Y_B, n, b1.at[n, 1 - y], r21.at[n], to_y)

        @pl.when(has_turn(t - lag - 2))
        def _():
            turn = step_of(turn_at(t - lag - 2))
            n = item_of(turn)
            arrived(X_A, n, r20.at[n])
            d0[n] = (b0[n, x].astype(f32) + r20[n].astype(f32)).astype(bf16)
            arrived(Y_B, n, r21.at[n])
            d1[n] = (b1[n, y].astype(f32) + r21[n].astype(f32)).astype(bf16)

            @pl.when((turn > 0) & (turn < items - 1))
            def _():
                m = 2 * z + half_of(turn)
                send(RZ_A, n, d0.at[n], z0.at[m], at_plane(plane_of(turn)), m)
                send(RZ_B, n, d1.at[n], z1.at[m], at_plane(plane_of(turn)), m)

        return carry

    lax.fori_loop(0, items + lag + 3, tick, 0)
    for r in range(2):
        n, part = 2 * z + r, pl.ds(r * rows, rows)
        low = upd[part, :half] + d0[n].astype(f32)
        high = upd[part, half:] + d1[n].astype(f32)
        for i in range(1, planes):
            n = 2 * ((z + i) % planes) + r
            arrived(RZ_A, n, z0.at[n])
            low = low + z0[n].astype(f32)
            arrived(RZ_B, n, z1.at[n])
            high = high + z1[n].astype(f32)
        out[part, :half] = low.astype(bf16)
        out[part, half:] = high.astype(bf16)

    def drain(n, carry):
        p = n // 2

        @pl.when((p <= z) & (z + 1 < planes))
        def _():
            left(UP_A, n, g0.at[c, n, here])
            left(UP_B, n, g1.at[c, n, here])

        @pl.when((p >= z) & (z > 0))
        def _():
            left(DOWN_A, n, g0.at[c, n, here])
            left(DOWN_B, n, g1.at[c, n, here])

        @pl.when((p < z) | (p > z))
        def _():
            left(RZ_A, n, d0.at[n])
            left(RZ_B, n, d1.at[n])

        left(X_A2, n, g0.at[c, n, here])
        left(Y_B2, n, g1.at[c, n, here])
        left(Y_A3, n, g0.at[c, n, here])
        left(X_B3, n, g1.at[c, n, here])
        left(Y_A4, n, g0.at[c, n, other_x])
        left(X_B4, n, g1.at[c, n, other_y])
        left(C_A, n, g0.at[c, n])
        left(C_B, n, g1.at[c, n])
        left(C_P, n, pm.at[n, 1 - c])
        left(Y_A, n, a0.at[n, 1 - y])
        left(X_B, n, a1.at[n, 1 - x])
        left(X_A, n, b0.at[n, 1 - x])
        left(Y_B, n, b1.at[n, 1 - y])
        return carry

    lax.fori_loop(0, items, drain, 0)
    left(TOTAL, 0, total_own)
    for h in range(heads):
        left(ACROSS, h, side_out.at[h])

        @pl.when(z + 1 < planes)
        def _():
            left(CHAIN, h, carry_out.at[h])

    for j in range(pieces):
        left(MIX_C, j, blend.at[j, 1 - c])
        left(MIX_Y, j, held.at[j])


def rope_tables(length, spans):
    half_dim = HEAD_DIM // 2
    rates = rope_base ** (-np.arange(half_dim, dtype=np.float64) / half_dim)
    rates = np.concatenate([rates, rates])[None, :]
    near = np.arange(length, dtype=np.float64)[:, None] * rates
    starts = (np.arange(spans, dtype=np.float64) * length)[:, None] * rates
    sign = np.concatenate([-np.ones(half_dim), np.ones(half_dim)])[None, :]
    base = np.zeros((spans, 8, HEAD_DIM))
    base[:, 0], base[:, 1] = np.cos(starts), np.sin(starts)
    base[:, 2], base[:, 3] = sign * np.sin(starts), sign * np.cos(starts)
    near_table = np.stack([np.cos(near), np.sin(near)]).astype(np.float32)
    return jnp.asarray(near_table), jnp.asarray(base.reshape(spans * 8, HEAD_DIM).astype(np.float32))


def fused_layer(
    query_rows, key_rows, value_rows, gate_rows, log_decay, head_gain, out_weight, residual, ffn_gain,
    gate_part, up_part, down_part, own_routes, route_weights,
):
    sp_count = lax.axis_size("sp")
    length, heads = log_decay.shape
    rows_all, width = residual.shape
    inner = query_rows.shape[1]
    chosen = own_routes.T[:, None, :] == jnp.arange(128, dtype=jnp.int32)[None, :, None]
    shares = jnp.sum(jnp.where(chosen, route_weights.T[:, None, :], 0.0), axis=0)
    shares = jnp.pad(shares, ((0, 0), (0, 128 - rows_all)))
    near_table, base_table = rope_tables(length, sp_count)
    half = width // 2
    planes = sp_count // 2
    items = 2 * planes
    rows = rows_all // 2
    pieces = 4
    span = width // pieces
    bf16, f32 = jnp.bfloat16, jnp.float32
    whole = pl.BlockSpec(memory_space=pltpu.VMEM)
    far = pl.BlockSpec(memory_space=pl.ANY)
    square = (heads, HEAD_DIM, HEAD_DIM)
    return pl.pallas_call(
        functools.partial(layer_kernel, planes),
        out_shape=jax.ShapeDtypeStruct((rows_all, width), bf16),
        in_specs=[whole] * 11 + [far] * 4,
        out_specs=whole,
        scratch_shapes=[
            pltpu.VMEM(out_weight.shape, bf16),
            pltpu.VMEM(gate_part.shape, bf16),
            pltpu.VMEM(up_part.shape, bf16),
            pltpu.VMEM(down_part.shape, bf16),
            pltpu.VMEM((2, length, HEAD_DIM), f32),
            pltpu.VMEM((length, inner), bf16),
            pltpu.VMEM((length, inner), f32),
            pltpu.VMEM((length, inner), bf16),
            pltpu.VMEM(square, f32),
            pltpu.VMEM((length, 8), f32),
            pltpu.VMEM((8, length), f32),
            pltpu.VMEM((8, HEAD_DIM), f32),
            pltpu.VMEM((8, HEAD_DIM), f32),
            pltpu.VMEM(square, bf16),
            pltpu.VMEM(square, bf16),
            pltpu.VMEM(square, bf16),
            pltpu.VMEM(square, bf16),
            pltpu.VMEM((length, inner), bf16),
            pltpu.VMEM((pieces, 2, 2, rows_all, span), bf16),
            pltpu.VMEM((pieces, 2, rows_all, span), bf16),
            pltpu.VMEM((pieces, rows_all, span), bf16),
            pltpu.VMEM((pieces, rows_all, span), bf16),
            pltpu.VMEM((rows_all, width), f32),
            pltpu.VMEM((2, items, 4, rows, half + 128), bf16),
            pltpu.VMEM((2, items, 4, rows, half), bf16),
            pltpu.VMEM((items, 2, 4 * rows, width), bf16),
            pltpu.VMEM((items, 4 * rows, width), bf16),
            pltpu.VMEM((items, 2, 2, rows, half), bf16),
            pltpu.VMEM((items, 2, 2, rows, half), bf16),
            pltpu.VMEM((items, 2, rows, half), bf16),
            pltpu.VMEM((items, 2, rows, half), bf16),
            pltpu.VMEM((items, 2, rows, half), bf16),
            pltpu.VMEM((items, 2, rows, half), bf16),
            pltpu.VMEM((items, rows, half), bf16),
            pltpu.VMEM((items, rows, half), bf16),
            pltpu.VMEM((items, rows, half), bf16),
            pltpu.VMEM((items, rows, half), bf16),
            pltpu.VMEM((items, rows, half), bf16),
            pltpu.VMEM((items, rows, half), bf16),
            pltpu.SemaphoreType.DMA((24, max(items, heads))),
            pltpu.SemaphoreType.DMA((24, max(items, heads))),
            pltpu.SemaphoreType.DMA((4,)),
        ],
        compiler_params=pltpu.CompilerParams(
            collective_id=0, has_side_effects=True, vmem_limit_bytes=63 * 1024 * 1024
        ),
    )(
        query_rows, key_rows, value_rows, gate_rows, log_decay.T, head_gain[None, :], near_table, base_table,
        residual, ffn_gain[None, :], shares, out_weight, gate_part, up_part, down_part,
    )


def body(
    query_rows,
    key_rows,
    value_rows,
    gate_rows,
    log_decay,
    head_gain,
    out_weight,
    residual,
    ffn_gain,
    gate_weight,
    up_weight,
    down_weight,
    routes,
    route_weights,
):
    tok_count = query_rows.shape[0]
    local_heads = log_decay.shape[1]
    sp_count = lax.axis_size("sp")
    tp_count = lax.axis_size("tp")
    model_width = residual.shape[1]
    rows_own = tok_count // tp_count
    capacity = max(2, 3 * rows_own * TOPK // (2 * sp_count))
    tp_index = lax.axis_index("tp")
    own_routes = lax.dynamic_slice_in_dim(routes, tp_index * rows_own, rows_own, 0)
    if (
        tp_count == 4 and sp_count % 2 == 0 and sp_count <= 16 and local_heads <= 8
        and rows_own <= 128 and rows_own < 2 * capacity
    ):
        return fused_layer(
            query_rows, key_rows, value_rows, gate_rows, log_decay, head_gain, out_weight, residual, ffn_gain,
            gate_weight[0], up_weight[0], down_weight[0], own_routes, route_weights,
        )
    hidden = retention(query_rows, key_rows, value_rows, gate_rows, log_decay, head_gain)
    mixed = jnp.dot(hidden, out_weight, preferred_element_type=jnp.float32).astype(jnp.bfloat16)
    mixed_sum = lax.psum_scatter(mixed, "tp", scatter_dimension=0, tiled=True).astype(jnp.float32)
    updated = residual.astype(jnp.float32) + mixed_sum
    ffn_in = square_norm(updated, ffn_gain)
    own_experts, own_ranks = slot_ranks(own_routes, sp_count)
    home_slot = own_experts * capacity + own_ranks
    gate_part = gate_weight[0]
    up_part = up_weight[0]
    down_part = down_weight[0]
    empty_row = jnp.zeros((1, model_width), jnp.bfloat16)
    source_row = (
        jnp.full((sp_count * capacity,), rows_own, jnp.int32)
        .at[home_slot]
        .set(jnp.arange(rows_own * TOPK, dtype=jnp.int32) // TOPK)
    )
    padded = jnp.concatenate([ffn_in, empty_row], axis=0)
    outgoing = padded[source_row].reshape(sp_count, capacity, model_width)
    arrived = lax.all_to_all(outgoing, "sp", split_axis=0, concat_axis=0, tiled=True)
    fanned = lax.all_gather(arrived[None], "tp", axis=0, tiled=True)
    activity = expert_rows(fanned.reshape(-1, model_width), gate_part, up_part)
    partial_out = jnp.dot(activity, down_part, preferred_element_type=jnp.float32).reshape(
        tp_count, sp_count, capacity, model_width
    )
    summed = (
        lax.psum_scatter(partial_out.astype(jnp.bfloat16), "tp", scatter_dimension=0, tiled=True)
        .astype(jnp.float32)
        .reshape(sp_count, capacity, model_width)
    )
    returned = lax.all_to_all(
        summed.astype(jnp.bfloat16), "sp", split_axis=0, concat_axis=0, tiled=True
    )
    picked = returned.reshape(sp_count * capacity, model_width)[home_slot].reshape(
        rows_own, TOPK, model_width
    )
    expert_sum = jnp.sum(route_weights[:, :, None] * picked.astype(jnp.float32), axis=1)
    return (updated + expert_sum).astype(jnp.bfloat16)


def solution(mesh):
    return jax.shard_map(
        body,
        mesh=mesh,
        in_specs=(
            P("sp", "tp"),
            P("sp", "tp"),
            P("sp", "tp"),
            P("sp", "tp"),
            P("sp", "tp"),
            P("tp"),
            P("tp", None),
            P(("sp", "tp"), None),
            P(),
            P("sp", None, "tp"),
            P("sp", None, "tp"),
            P("sp", "tp", None),
            P("sp", None),
            P(("sp", "tp"), None),
        ),
        out_specs=P(("sp", "tp"), None),
        check_vma=False,
    )
```

```python
import functools

import jax
import jax.numpy as jnp
import numpy as np
from jax import lax
from jax.experimental import pallas as pl
from jax.experimental.pallas import tpu as pltpu
from jax.sharding import PartitionSpec as P

HEAD_DIM = 128
TOPK = 4
BLOCK = 128


highest = lax.Precision.HIGHEST
rope_base = 10000.0
group_eps = 1e-05
square_eps = 1e-06
clamp_limit = 7.0
swish_alpha = 1.702


def rotary_angles(positions, head_dim):
    half_dim = head_dim // 2
    inverse = rope_base ** (-jnp.arange(half_dim, dtype=jnp.float32) / half_dim)
    return positions[:, None] * inverse[None, :]


def square_norm(updated, gain_row):
    factor = lax.rsqrt(jnp.mean(updated * updated, axis=-1, keepdims=True) + square_eps)
    return (updated * factor * gain_row).astype(jnp.bfloat16)


def expert_rows(rows, gate_part, up_part):
    gate_pre = jnp.dot(rows, gate_part, preferred_element_type=jnp.float32)
    up_pre = jnp.dot(rows, up_part, preferred_element_type=jnp.float32)
    gate_clip = jnp.minimum(gate_pre, clamp_limit)
    up_clip = jnp.clip(up_pre, -clamp_limit, clamp_limit)
    return ((up_clip + 1.0) * (gate_clip * jax.nn.sigmoid(gate_clip * swish_alpha))).astype(
        jnp.bfloat16
    )


def slot_ranks(route_block, experts):
    flat_routes = route_block.reshape(-1)
    onehot = (flat_routes[:, None] == jnp.arange(experts, dtype=jnp.int32)[None, :]).astype(
        jnp.int32
    )
    return (flat_routes, jnp.sum(jnp.cumsum(onehot, axis=0) * onehot, axis=1) - 1)


def retention_kernel(q_ref, k_ref, v_ref, cos_ref, sin_ref, cum_ref, cum_row_ref, ret_ref, qdec_ref, state_ref):
    head = pl.program_id(0)
    length = q_ref.shape[0]
    cosine, sine = cos_ref[...], sin_ref[...]
    half = HEAD_DIM // 2

    def turned(ref):
        rows = ref[...].astype(jnp.float32)
        return rows * cosine + pltpu.roll(rows, half, 1) * sine

    lanes = lax.broadcasted_iota(jnp.int32, cum_ref.shape, 1)
    column = jnp.sum(jnp.where(lanes == head, cum_ref[...], 0.0), axis=1, keepdims=True)
    row = cum_row_ref[0]
    queries = turned(q_ref)
    keys = turned(k_ref) * HEAD_DIM ** (-0.5)
    values = v_ref[...]
    scores = lax.dot_general(
        queries.astype(jnp.bfloat16),
        keys.astype(jnp.bfloat16),
        (((1,), (1,)), ((), ())),
        preferred_element_type=jnp.float32,
    )
    causal = lax.broadcasted_iota(jnp.int32, (length, length), 0) >= lax.broadcasted_iota(
        jnp.int32, (length, length), 1
    )
    weights = jnp.where(causal, jnp.exp(jnp.minimum(column - row, 0.0)), 0.0)
    ret_ref[...] = jnp.dot(
        (scores * weights).astype(jnp.bfloat16), values, preferred_element_type=jnp.float32
    )
    qdec_ref[...] = (queries * jnp.exp(column)).astype(jnp.bfloat16)
    total = column[length - 1 :, :]
    tailed = (keys * jnp.exp(total - column)).astype(jnp.bfloat16)
    state_ref[0, :HEAD_DIM, :] = lax.dot_general(
        tailed, values, (((0,), (0,)), ((), ())), preferred_element_type=jnp.float32
    )
    state_ref[0, HEAD_DIM:, :] = jnp.broadcast_to(total, (8, HEAD_DIM))


def norm_kernel(ret_ref, qdec_ref, enter_ref, gain_ref, gate_ref, hidden_ref):
    retained = ret_ref[...] + jnp.dot(
        qdec_ref[...], enter_ref[0].astype(jnp.bfloat16), preferred_element_type=jnp.float32
    )
    centred = retained - jnp.mean(retained, axis=-1, keepdims=True)
    variance = jnp.mean(centred * centred, axis=-1, keepdims=True)
    gate = gate_ref[...].astype(jnp.float32)
    scaled = centred * lax.rsqrt(variance + group_eps) * gain_ref[...]
    hidden_ref[...] = (scaled * (gate / (1.0 + jnp.exp(-gate)))).astype(jnp.bfloat16)


def retention(query_rows, key_rows, value_rows, gate_rows, log_decay, head_gain):
    length, local_heads = log_decay.shape
    width = query_rows.shape[1]
    sp_count, mine = lax.axis_size("sp"), lax.axis_index("sp")
    positions = (mine * length + jnp.arange(length, dtype=jnp.int32)).astype(jnp.float32)
    angles = rotary_angles(positions, HEAD_DIM)
    cosine, sine = jnp.cos(angles), jnp.sin(angles)
    cosine = jnp.concatenate([cosine, cosine], axis=1)
    sine = jnp.concatenate([-sine, sine], axis=1)
    cumulative = jnp.cumsum(log_decay, axis=0)
    rows_spec = pl.BlockSpec((length, HEAD_DIM), lambda h: (0, h))
    table_spec = pl.BlockSpec((length, HEAD_DIM), lambda h: (0, 0))
    retained, qdec, state = pl.pallas_call(
        retention_kernel,
        grid=(local_heads,),
        out_shape=(
            jax.ShapeDtypeStruct((length, width), jnp.float32),
            jax.ShapeDtypeStruct((length, width), jnp.bfloat16),
            jax.ShapeDtypeStruct((local_heads, HEAD_DIM + 8, HEAD_DIM), jnp.float32),
        ),
        in_specs=[
            rows_spec,
            rows_spec,
            rows_spec,
            table_spec,
            table_spec,
            pl.BlockSpec((length, local_heads), lambda h: (0, 0)),
            pl.BlockSpec((1, 1, length), lambda h: (h, 0, 0)),
        ],
        out_specs=(
            rows_spec,
            rows_spec,
            pl.BlockSpec((1, HEAD_DIM + 8, HEAD_DIM), lambda h: (h, 0, 0)),
        ),
    )(query_rows, key_rows, value_rows, cosine, sine, cumulative, cumulative.T[:, None, :])
    pieces = lax.all_gather(state, "sp")
    totals = pieces[:, :, HEAD_DIM, 0]
    index = jnp.arange(sp_count, dtype=jnp.int32)
    between = (index[None, :] > index[:, None]) & (index[None, :] < mine)
    gap = jnp.sum(jnp.where(between[:, :, None], totals[None], 0.0), axis=1)
    factor = jnp.where((index < mine)[:, None], jnp.exp(gap), 0.0)
    entering = jnp.sum(factor[:, :, None, None] * pieces[:, :, :HEAD_DIM, :], axis=0)
    return pl.pallas_call(
        norm_kernel,
        grid=(local_heads,),
        out_shape=jax.ShapeDtypeStruct((length, width), jnp.bfloat16),
        in_specs=[
            rows_spec,
            rows_spec,
            pl.BlockSpec((1, HEAD_DIM, HEAD_DIM), lambda h: (h, 0, 0)),
            pl.BlockSpec((1, HEAD_DIM), lambda h: (0, h)),
            rows_spec,
        ],
        out_specs=rows_spec,
    )(retained, qdec, entering, head_gain[None, :], gate_rows)


(
    UP_A, UP_B, DOWN_A, DOWN_B, X_A2, Y_B2, Y_A3, Y_A4, X_B3, X_B4, C_A, C_B, C_P, Y_A, X_B, X_A, Y_B, RZ_A, RZ_B,
    TOTAL, CHAIN, ACROSS, MIX_C, MIX_Y, S_X2, S_Y2, S_Y3, S_X3, S_Y4, S_X4, S_UP, S_DOWN, S_CORE,
) = range(33)


def layer_kernel(
    planes, q_ref, k_ref, v_ref, gate_ref, logs, head_gain, near_table, base_table, residual, ffn_gain,
    routes, route_weights,
    wo_hbm, wg_hbm, wu_hbm, wd_hbm, out,
    wo, wg, wu, wd, rotary, turned_k, ret, qdec, state, cum_col, cum_row, total_own, total_x, carry_in, carry_out,
    side_out, side_in, hidden, blend, from_core, held, from_y, upd,
    share_in, g0, g1, gs, pm, pr, a0, a1, r10, r11, b0, b1, r20, r21, d0, d1, z0, z1,
    ssem, rsem, wsem,
):
    sp, tp = lax.axis_index("sp"), lax.axis_index("tp")
    sp_count = 2 * planes
    z, x = sp // 2, sp % 2
    y, c = tp // 2, tp % 2
    own_rows, width = out.shape
    half = width // 2
    wide_a, wide_b = g0.shape[-1] - 128, g1.shape[-1]
    wide_ab = wide_a + wide_b
    rows = own_rows // 2
    items = 2 * planes
    lag = items - 3
    f32, bf16 = jnp.float32, jnp.bfloat16
    to_core = {"sp": sp, "tp": y * 2 + (1 - c)}
    to_y = {"sp": sp, "tp": (1 - y) * 2 + c}
    to_x = {"sp": z * 2 + (1 - x), "tp": tp}

    def half_of(n):
        return jnp.where(n == items - 1, 1, jnp.where(n == 0, 0, (n + 1) % 2))

    def plane_at(k):
        low = z < planes // 2
        mirrored = jnp.where(low, z, planes - 1 - z)
        q = jnp.where(k <= mirrored, mirrored - k, k)
        return jnp.where(low, q, planes - 1 - q)

    def plane_of(n):
        return plane_at(((n + 1) // 2) % planes)

    def item_of(n):
        return 2 * plane_of(n) + half_of(n)

    def step_of(turn):
        back = items - 3 - 2 * ((turn - 1) // 2) + (turn - 1) % 2
        return jnp.where((turn == 0) | (turn == items - 1), turn, back)

    def turn_at(u):
        return jnp.where(u == 0, 0, u - 1)

    def has_turn(u):
        return (u == 0) | ((u >= 2) & (u <= items))

    def at_plane(p):
        return {"sp": p * 2 + x, "tp": tp}

    def to_z(i):
        return at_plane((z + planes - i) % planes)

    def move(kind, n, src, dst, device, m=None):
        return pltpu.make_async_remote_copy(
            src_ref=src, dst_ref=dst, send_sem=ssem.at[kind, n],
            recv_sem=rsem.at[kind, n if m is None else m],
            device_id=device, device_id_type=pl.DeviceIdType.MESH,
        )

    def send(kind, n, src, dst, device, m=None):
        move(kind, n, src, dst, device, m).start()

    def arrived(kind, n, dst):
        move(kind, n, dst, dst, to_core).wait_recv()

    def left(kind, n, src):
        move(kind, n, src, src, to_core).wait_send()

    barrier = pltpu.get_barrier_semaphore()
    for device in [to_core, to_y, to_x] + [to_z(i) for i in range(1, planes)]:
        pl.semaphore_signal(barrier, inc=1, device_id=device, device_id_type=pl.DeviceIdType.MESH)

    weights = [
        pltpu.make_async_copy(wo_hbm, wo, wsem.at[0]),
        pltpu.make_async_copy(wg_hbm, wg, wsem.at[1]),
        pltpu.make_async_copy(wu_hbm, wu, wsem.at[2]),
        pltpu.make_async_copy(wd_hbm, wd, wsem.at[3]),
    ]
    for copy in weights:
        copy.start()

    length = q_ref.shape[0]
    heads = state.shape[0]
    dim = HEAD_DIM
    after = lax.broadcasted_iota(jnp.int32, (length, length), 0) >= lax.broadcasted_iota(
        jnp.int32, (length, length), 1
    )
    ones = jnp.where(after, 1.0, 0.0).astype(f32)
    log_rows = jnp.concatenate([logs[...], jnp.zeros((8 - heads, length), f32)], axis=0)
    cum_row[...] = lax.dot_general(
        log_rows, ones, (((1,), (1,)), ((), ())), precision=highest, preferred_element_type=f32
    )
    cum_col[...] = lax.dot_general(
        ones, log_rows, (((1,), (1,)), ((), ())), precision=highest, preferred_element_type=f32
    )
    total_own[...] = jnp.broadcast_to(cum_row[:, length - 1 :], (8, dim))
    pl.semaphore_wait(barrier, 2 + planes)
    send(TOTAL, 0, total_own, total_x, to_x)

    base = base_table[pl.ds(sp * 8, 8), :]
    cosine = base[0:1] * near_table[0] - base[1:2] * near_table[1]
    sine = base[2:3] * near_table[0] + base[3:4] * near_table[1]
    rotary[0] = cosine
    rotary[1] = sine

    def turned(rows_in):
        wide = rows_in.astype(f32)
        return wide * rotary[0] + pltpu.roll(wide, dim // 2, 1) * rotary[1]

    def column_of(h):
        lanes = lax.broadcasted_iota(jnp.int32, cum_col.shape, 1)
        return jnp.sum(jnp.where(lanes == h, cum_col[...], 0.0), axis=1, keepdims=True)

    for h in range(heads):
        lanes = pl.ds(h * dim, dim)
        keys = turned(k_ref[:, lanes]) * dim ** (-0.5)
        turned_k[:, lanes] = keys.astype(bf16)
        column = column_of(h)
        tailed = (keys * jnp.exp(column[length - 1 :, :] - column)).astype(bf16)
        state[h] = lax.dot_general(
            tailed, v_ref[:, lanes], (((0,), (0,)), ((), ())), preferred_element_type=f32
        )

    def attend(h, carry):
        lanes = pl.ds(pl.multiple_of(h * dim, dim), dim)
        queries = turned(q_ref[:, lanes])
        column = column_of(h)
        scores = lax.dot_general(
            queries.astype(bf16), turned_k[:, lanes], (((1,), (1,)), ((), ())), preferred_element_type=f32
        )
        gap = jnp.minimum(column - cum_row[pl.ds(h, 1), :], 0.0)
        decays = jnp.where(after, jnp.exp(gap), 0.0)
        ret[:, lanes] = jnp.dot((scores * decays).astype(bf16), v_ref[:, lanes], preferred_element_type=f32)
        qdec[:, lanes] = (queries * jnp.exp(column)).astype(bf16)
        return carry

    early = jnp.where(z >= planes // 2, heads, 0)
    lax.fori_loop(0, early, attend, 0)

    arrived(TOTAL, 0, total_x)
    left_side = x == 0
    for h in range(heads):
        own_total, x_total = total_own[h : h + 1, :], total_x[h : h + 1, :]

        @pl.when(z > 0)
        def _():
            arrived(CHAIN, h, carry_in.at[h])

        @pl.when(z == 0)
        def _():
            carry_in[h] = jnp.zeros((dim, dim), bf16)

        before = carry_in[h].astype(f32)

        @pl.when(z + 1 < planes)
        def _():
            fresh = jnp.where(left_side, jnp.exp(x_total), 1.0) * state[h]
            carry_out[h] = (jnp.exp(own_total + x_total) * before + fresh).astype(bf16)
            send(CHAIN, h, carry_out.at[h], carry_in.at[h], at_plane(z + 1))

        side_out[h] = jnp.where(left_side, jnp.exp(own_total) * before + state[h], before).astype(bf16)
        send(ACROSS, h, side_out.at[h], side_in.at[h], to_x)

    lax.fori_loop(early, heads, attend, 0)

    for h in range(heads):
        lanes = pl.ds(h * dim, dim)
        arrived(ACROSS, h, side_in.at[h])
        factor = jnp.where(left_side, 1.0, jnp.exp(total_x[h : h + 1, :]))
        entering = (factor * carry_in[h].astype(f32) + side_in[h].astype(f32)).astype(bf16)
        retained = ret[:, lanes] + jnp.dot(qdec[:, lanes], entering, preferred_element_type=f32)
        centred = retained - jnp.mean(retained, axis=-1, keepdims=True)
        variance = jnp.mean(centred * centred, axis=-1, keepdims=True)
        gate_in = gate_ref[:, lanes].astype(f32)
        scaled = centred * lax.rsqrt(variance + group_eps) * head_gain[:, lanes]
        hidden[:, lanes] = (scaled * (gate_in / (1.0 + jnp.exp(-gate_in)))).astype(bf16)

    weights[0].wait()
    pieces = blend.shape[0]
    span = width // pieces

    def cross(j):
        arrived(MIX_C, j, from_core.at[j])
        held[j] = (blend[j, c, 1 - y].astype(f32) + from_core[j, 1 - y].astype(f32)).astype(bf16)
        send(MIX_Y, j, held.at[j], from_y.at[j], to_y)

    for j in range(pieces):
        mixed = jnp.dot(hidden[...], wo[:, pl.ds(j * span, span)], preferred_element_type=f32).astype(bf16)
        for q in range(4):
            blend[j, q % 2, q // 2] = mixed[q * own_rows : (q + 1) * own_rows, :]
        send(MIX_C, j, blend.at[j, 1 - c], from_core.at[j], to_core)
        if j > 0:
            cross(j - 1)
    cross(pieces - 1)
    square = jnp.zeros((own_rows, 1), f32)
    for j in range(pieces):
        cols = pl.ds(j * span, span)
        base_rows = residual[:, cols].astype(f32) + blend[j, c, y].astype(f32) + from_core[j, y].astype(f32)
        arrived(MIX_Y, j, from_y.at[j])
        total = base_rows + from_y[j].astype(f32)
        upd[:, cols] = total
        square = square + jnp.sum(total * total, axis=-1, keepdims=True)
    scale = lax.rsqrt(square * (1.0 / width) + square_eps)

    here = x * 2 + y
    other_x = (1 - x) * 2 + y
    other_y = x * 2 + (1 - y)
    other_xy = (1 - x) * 2 + (1 - y)
    count = routes.shape[0]
    share_in[...] = jnp.zeros_like(share_in)
    share_in[:count, :own_rows] = route_weights[...]
    all_routes = jnp.concatenate([routes[...]] * (8 // count), axis=0)
    own_routes = jnp.zeros((8, 128), jnp.int32)
    for q in range(4):
        turned_routes = pltpu.roll(all_routes, (length - q * own_rows) % length, 1)
        own_routes = own_routes + jnp.where(tp == q, turned_routes[:, :128], 0)
    expert = lax.broadcasted_iota(jnp.int32, (128, 128), 0)
    shares = jnp.zeros((128, 128), f32)
    for k in range(count):
        shares = shares + jnp.where(own_routes[k : k + 1, :] == expert, share_in[k : k + 1, :], 0.0)
    share = jnp.transpose(shares)[:own_rows, :]
    coarse = share.astype(bf16).astype(f32)
    tail_rows = (coarse + pltpu.roll(share - coarse, sp_count, 1)).astype(bf16)
    first_rows, last_rows = pl.ds(0, rows), pl.ds(rows, rows)
    for r in range(2):
        mine, n = slice(r * rows, (r + 1) * rows), 2 * z + r
        ready = (upd[mine, :] * scale[mine] * ffn_gain[...]).astype(bf16)
        g0[c, n, here, :, :wide_a] = ready[:, :wide_a]
        g0[c, n, here, :, wide_a:] = tail_rows[mine]
        g1[c, n, here] = ready[:, wide_a:wide_ab]
        gs[c, z, here, mine, :] = ready[:, wide_ab:]

    def side(p, chip, part):
        return gs.at[c, p, chip, part]

    def pass_side(kind, n, chip, part, device):
        send(kind, n, side(z, chip, part), side(z, chip, part), device)

    def spread_side():
        pass_side(S_X2, 0, here, first_rows, to_x)
        pass_side(S_Y2, 0, here, last_rows, to_y)
        pass_side(S_Y3, 0, here, first_rows, to_y)
        pass_side(S_X3, 0, here, last_rows, to_x)

    def relay_side():
        arrived(S_X2, 0, side(z, other_x, first_rows))
        pass_side(S_Y4, 0, other_x, first_rows, to_y)
        arrived(S_Y2, 0, side(z, other_y, last_rows))
        pass_side(S_X4, 0, other_y, last_rows, to_x)

    def side_up(p):
        @pl.when(z + 1 < planes)
        def _():
            send(S_UP, p, gs.at[c, p], gs.at[c, p], at_plane(z + 1))

    def side_down(p):
        @pl.when(z > 0)
        def _():
            send(S_DOWN, p, gs.at[c, p], gs.at[c, p], at_plane(z - 1))

    def side_core(p):
        send(S_CORE, p, gs.at[c, p], gs.at[c, p], to_core)

    def close_side():
        arrived(S_Y3, 0, side(z, other_y, first_rows))
        arrived(S_Y4, 0, side(z, other_xy, first_rows))
        arrived(S_X3, 0, side(z, other_x, last_rows))
        arrived(S_X4, 0, side(z, other_xy, last_rows))
        side_up(z)
        side_down(z)
        side_core(z)

    def spread(n):
        send(X_A2, n, g0.at[c, n, here], g0.at[c, n, here], to_x)
        send(Y_B2, n, g1.at[c, n, here], g1.at[c, n, here], to_y)
        send(Y_A3, n, g0.at[c, n, here], g0.at[c, n, here], to_y)
        send(X_B3, n, g1.at[c, n, here], g1.at[c, n, here], to_x)

    def raise_up(n):
        @pl.when(z + 1 < planes)
        def _():
            send(UP_A, n, g0.at[c, n, here], g0.at[c, n, here], at_plane(z + 1))
            send(UP_B, n, g1.at[c, n, here], g1.at[c, n, here], at_plane(z + 1))

    def hand_down(n):
        @pl.when(z > 0)
        def _():
            send(DOWN_A, n, g0.at[c, n, here], g0.at[c, n, here], at_plane(z - 1))
            send(DOWN_B, n, g1.at[c, n, here], g1.at[c, n, here], at_plane(z - 1))

    spread_side()
    spread(2 * z)
    for r in range(2):
        raise_up(2 * z + r)
        hand_down(2 * z + r)

    def tick(t, carry):
        def relay():
            n = item_of(t)
            arrived(X_A2, n, g0.at[c, n, other_x])
            send(Y_A4, n, g0.at[c, n, other_x], g0.at[c, n, other_x], to_y)
            arrived(Y_B2, n, g1.at[c, n, other_y])
            send(X_B4, n, g1.at[c, n, other_y], g1.at[c, n, other_y], to_x)

        pl.when(t == 0)(relay_side)
        pl.when(t == 0)(relay)
        pl.when(t == 1)(close_side)

        @pl.when(t + 1 < items)
        def _():
            k, r = (t + 2) // 2, t % 2

            @pl.when((t + 1 < items - 1) & (z - k >= 0))
            def _():
                n = 2 * (z - k) + r
                arrived(UP_A, n, g0.at[c, n, here])
                arrived(UP_B, n, g1.at[c, n, here])
                raise_up(n)

            @pl.when((t + 1 < items - 1) & (z + k < planes))
            def _():
                n = 2 * (z + k) + r
                arrived(DOWN_A, n, g0.at[c, n, here])
                arrived(DOWN_B, n, g1.at[c, n, here])
                hand_down(n)

            spread(item_of(t + 1))

        pl.when((t > 0) & (t < items))(relay)

        @pl.when((t >= 2) & (t < items) & (t % 2 == 0))
        def _():
            below, above = z - t // 2, z + t // 2

            @pl.when(below >= 0)
            def _():
                arrived(S_UP, below, gs.at[c, below])
                side_up(below)
                side_core(below)

            @pl.when(above < planes)
            def _():
                arrived(S_DOWN, above, gs.at[c, above])
                side_down(above)
                side_core(above)

        @pl.when(t == 2)
        def _():
            for copy in weights[1:]:
                copy.wait()

        @pl.when((t >= 2) & (t < items + 2))
        def _():
            n = item_of(t - 2)
            arrived(C_A, n, g0.at[1 - c, n])
            arrived(C_B, n, g1.at[1 - c, n])
            p, r = plane_of(t - 2), half_of(t - 2)

            @pl.when(r == 0)
            def _():
                arrived(S_CORE, p, gs.at[1 - c, p])

            lead = g0[:, n].reshape(8 * rows, wide_a + 128)
            tail = lead[:, wide_a:].astype(f32)
            rest = g1[:, n].reshape(8 * rows, wide_b)
            last = gs[:, p, :, pl.ds(pl.multiple_of(r * rows, rows), rows), :].reshape(8 * rows, width - wide_ab)
            rows_in = jnp.concatenate([lead[:, :wide_a], rest, last], axis=1)
            lane = lax.broadcasted_iota(jnp.int32, tail.shape, 1)
            weight = jnp.sum(
                jnp.where((lane == sp) | (lane == sp + sp_count), tail, 0.0), axis=1, keepdims=True
            )

            def product(w):
                return jnp.dot(rows_in, w[...], preferred_element_type=f32)

            gate = jnp.minimum(product(wg), clamp_limit)
            up = jnp.clip(product(wu), -clamp_limit, clamp_limit)
            act = ((up + 1.0) * (gate / (1.0 + jnp.exp(-swish_alpha * gate)))).astype(bf16)
            made = (jnp.dot(act, wd[...], preferred_element_type=f32) * weight).astype(bf16)
            pm[n] = made.reshape(2, 4 * rows, 2 * half)
            send(C_P, n, pm.at[n, 1 - c], pr.at[n], to_core)

        @pl.when((t >= 1) & (t < items + 1))
        def _():
            n = item_of(t - 1)
            arrived(Y_A3, n, g0.at[c, n, other_y])
            arrived(Y_A4, n, g0.at[c, n, other_xy])
            arrived(X_B3, n, g1.at[c, n, other_x])
            arrived(X_B4, n, g1.at[c, n, other_xy])
            send(C_A, n, g0.at[c, n], g0.at[c, n], to_core)
            send(C_B, n, g1.at[c, n], g1.at[c, n], to_core)

        @pl.when(has_turn(t - lag))
        def _():
            n = item_of(step_of(turn_at(t - lag)))
            arrived(C_P, n, pr.at[n])
            for q in range(4):
                part = pl.ds(q * rows, rows)
                total = (pm[n, c, part, :].astype(f32) + pr[n, part, :].astype(f32)).astype(bf16)
                a0[n, q % 2, q // 2] = total[:, :half]
                a1[n, q // 2, q % 2] = total[:, half:]
            send(Y_A, n, a0.at[n, 1 - y], r10.at[n], to_y)
            send(X_B, n, a1.at[n, 1 - x], r11.at[n], to_x)

        @pl.when(has_turn(t - lag - 1))
        def _():
            n = item_of(step_of(turn_at(t - lag - 1)))
            arrived(Y_A, n, r10.at[n])
            b0[n] = (a0[n, y].astype(f32) + r10[n].astype(f32)).astype(bf16)
            send(X_A, n, b0.at[n, 1 - x], r20.at[n], to_x)
            arrived(X_B, n, r11.at[n])
            b1[n] = (a1[n, x].astype(f32) + r11[n].astype(f32)).astype(bf16)
            send(Y_B, n, b1.at[n, 1 - y], r21.at[n], to_y)

        @pl.when(has_turn(t - lag - 2))
        def _():
            turn = step_of(turn_at(t - lag - 2))
            n = item_of(turn)
            arrived(X_A, n, r20.at[n])
            d0[n] = (b0[n, x].astype(f32) + r20[n].astype(f32)).astype(bf16)
            arrived(Y_B, n, r21.at[n])
            d1[n] = (b1[n, y].astype(f32) + r21[n].astype(f32)).astype(bf16)

            @pl.when((turn > 0) & (turn < items - 1))
            def _():
                m = 2 * z + half_of(turn)
                send(RZ_A, n, d0.at[n], z0.at[m], at_plane(plane_of(turn)), m)
                send(RZ_B, n, d1.at[n], z1.at[m], at_plane(plane_of(turn)), m)

        return carry

    lax.fori_loop(0, items + lag + 3, tick, 0)
    for r in range(2):
        n, part = 2 * z + r, pl.ds(r * rows, rows)
        low = upd[part, :half] + d0[n].astype(f32)
        high = upd[part, half:] + d1[n].astype(f32)
        for i in range(1, planes):
            n = 2 * ((z + i) % planes) + r
            arrived(RZ_A, n, z0.at[n])
            low = low + z0[n].astype(f32)
            arrived(RZ_B, n, z1.at[n])
            high = high + z1[n].astype(f32)
        out[part, :half] = low.astype(bf16)
        out[part, half:] = high.astype(bf16)

    def drain(n, carry):
        p = n // 2

        @pl.when((p <= z) & (z + 1 < planes))
        def _():
            left(UP_A, n, g0.at[c, n, here])
            left(UP_B, n, g1.at[c, n, here])

        @pl.when((p >= z) & (z > 0))
        def _():
            left(DOWN_A, n, g0.at[c, n, here])
            left(DOWN_B, n, g1.at[c, n, here])

        @pl.when((p < z) | (p > z))
        def _():
            left(RZ_A, n, d0.at[n])
            left(RZ_B, n, d1.at[n])

        left(X_A2, n, g0.at[c, n, here])
        left(Y_B2, n, g1.at[c, n, here])
        left(Y_A3, n, g0.at[c, n, here])
        left(X_B3, n, g1.at[c, n, here])
        left(Y_A4, n, g0.at[c, n, other_x])
        left(X_B4, n, g1.at[c, n, other_y])
        left(C_A, n, g0.at[c, n])
        left(C_B, n, g1.at[c, n])
        left(C_P, n, pm.at[n, 1 - c])
        left(Y_A, n, a0.at[n, 1 - y])
        left(X_B, n, a1.at[n, 1 - x])
        left(X_A, n, b0.at[n, 1 - x])
        left(Y_B, n, b1.at[n, 1 - y])
        return carry

    lax.fori_loop(0, items, drain, 0)
    left(S_X2, 0, side(z, here, first_rows))
    left(S_Y2, 0, side(z, here, last_rows))
    left(S_Y3, 0, side(z, here, first_rows))
    left(S_X3, 0, side(z, here, last_rows))
    left(S_Y4, 0, side(z, other_x, first_rows))
    left(S_X4, 0, side(z, other_y, last_rows))

    def drain_side(p, carry):
        @pl.when((p <= z) & (z + 1 < planes))
        def _():
            left(S_UP, p, gs.at[c, p])

        @pl.when((p >= z) & (z > 0))
        def _():
            left(S_DOWN, p, gs.at[c, p])

        left(S_CORE, p, gs.at[c, p])
        return carry

    lax.fori_loop(0, planes, drain_side, 0)
    left(TOTAL, 0, total_own)
    for h in range(heads):
        left(ACROSS, h, side_out.at[h])

        @pl.when(z + 1 < planes)
        def _():
            left(CHAIN, h, carry_out.at[h])

    for j in range(pieces):
        left(MIX_C, j, blend.at[j, 1 - c])
        left(MIX_Y, j, held.at[j])


def rope_tables(length, spans):
    half_dim = HEAD_DIM // 2
    rates = rope_base ** (-np.arange(half_dim, dtype=np.float64) / half_dim)
    rates = np.concatenate([rates, rates])[None, :]
    near = np.arange(length, dtype=np.float64)[:, None] * rates
    starts = (np.arange(spans, dtype=np.float64) * length)[:, None] * rates
    sign = np.concatenate([-np.ones(half_dim), np.ones(half_dim)])[None, :]
    base = np.zeros((spans, 8, HEAD_DIM))
    base[:, 0], base[:, 1] = np.cos(starts), np.sin(starts)
    base[:, 2], base[:, 3] = sign * np.sin(starts), sign * np.cos(starts)
    near_table = np.stack([np.cos(near), np.sin(near)]).astype(np.float32)
    return jnp.asarray(near_table), jnp.asarray(base.reshape(spans * 8, HEAD_DIM).astype(np.float32))


def fused_layer(
    query_rows, key_rows, value_rows, gate_rows, log_decay, head_gain, out_weight, residual, ffn_gain,
    gate_part, up_part, down_part, routes, route_weights,
):
    sp_count = lax.axis_size("sp")
    length, heads = log_decay.shape
    rows_all, width = residual.shape
    inner = query_rows.shape[1]
    near_table, base_table = rope_tables(length, sp_count)
    half = width // 2
    planes = sp_count // 2
    items = 2 * planes
    rows = rows_all // 2
    pieces = 4
    span = width // pieces
    wide_s = 128 * (3 * width // 2048)
    wide_a = (width - wide_s - 128) // 256 * 128
    wide_b = width - wide_s - wide_a
    bf16, f32 = jnp.bfloat16, jnp.float32
    whole = pl.BlockSpec(memory_space=pltpu.VMEM)
    far = pl.BlockSpec(memory_space=pl.ANY)
    square = (heads, HEAD_DIM, HEAD_DIM)
    return pl.pallas_call(
        functools.partial(layer_kernel, planes),
        out_shape=jax.ShapeDtypeStruct((rows_all, width), bf16),
        in_specs=[whole] * 12 + [far] * 4,
        out_specs=whole,
        scratch_shapes=[
            pltpu.VMEM(out_weight.shape, bf16),
            pltpu.VMEM(gate_part.shape, bf16),
            pltpu.VMEM(up_part.shape, bf16),
            pltpu.VMEM(down_part.shape, bf16),
            pltpu.VMEM((2, length, HEAD_DIM), f32),
            pltpu.VMEM((length, inner), bf16),
            pltpu.VMEM((length, inner), f32),
            pltpu.VMEM((length, inner), bf16),
            pltpu.VMEM(square, f32),
            pltpu.VMEM((length, 8), f32),
            pltpu.VMEM((8, length), f32),
            pltpu.VMEM((8, HEAD_DIM), f32),
            pltpu.VMEM((8, HEAD_DIM), f32),
            pltpu.VMEM(square, bf16),
            pltpu.VMEM(square, bf16),
            pltpu.VMEM(square, bf16),
            pltpu.VMEM(square, bf16),
            pltpu.VMEM((length, inner), bf16),
            pltpu.VMEM((pieces, 2, 2, rows_all, span), bf16),
            pltpu.VMEM((pieces, 2, rows_all, span), bf16),
            pltpu.VMEM((pieces, rows_all, span), bf16),
            pltpu.VMEM((pieces, rows_all, span), bf16),
            pltpu.VMEM((rows_all, width), f32),
            pltpu.VMEM((8, 128), f32),
            pltpu.VMEM((2, items, 4, rows, wide_a + 128), bf16),
            pltpu.VMEM((2, items, 4, rows, wide_b), bf16),
            pltpu.VMEM((2, planes, 4, rows_all, wide_s), bf16),
            pltpu.VMEM((items, 2, 4 * rows, width), bf16),
            pltpu.VMEM((items, 4 * rows, width), bf16),
            pltpu.VMEM((items, 2, 2, rows, half), bf16),
            pltpu.VMEM((items, 2, 2, rows, half), bf16),
            pltpu.VMEM((items, 2, rows, half), bf16),
            pltpu.VMEM((items, 2, rows, half), bf16),
            pltpu.VMEM((items, 2, rows, half), bf16),
            pltpu.VMEM((items, 2, rows, half), bf16),
            pltpu.VMEM((items, rows, half), bf16),
            pltpu.VMEM((items, rows, half), bf16),
            pltpu.VMEM((items, rows, half), bf16),
            pltpu.VMEM((items, rows, half), bf16),
            pltpu.VMEM((items, rows, half), bf16),
            pltpu.VMEM((items, rows, half), bf16),
            pltpu.SemaphoreType.DMA((33, max(items, heads))),
            pltpu.SemaphoreType.DMA((33, max(items, heads))),
            pltpu.SemaphoreType.DMA((4,)),
        ],
        compiler_params=pltpu.CompilerParams(
            collective_id=0, has_side_effects=True, vmem_limit_bytes=63 * 1024 * 1024
        ),
    )(
        query_rows, key_rows, value_rows, gate_rows, log_decay.T, head_gain[None, :], near_table, base_table,
        residual, ffn_gain[None, :], routes.T, route_weights.T, out_weight, gate_part, up_part, down_part,
    )


def body(
    query_rows,
    key_rows,
    value_rows,
    gate_rows,
    log_decay,
    head_gain,
    out_weight,
    residual,
    ffn_gain,
    gate_weight,
    up_weight,
    down_weight,
    routes,
    route_weights,
):
    tok_count = query_rows.shape[0]
    local_heads = log_decay.shape[1]
    sp_count = lax.axis_size("sp")
    tp_count = lax.axis_size("tp")
    model_width = residual.shape[1]
    rows_own = tok_count // tp_count
    capacity = max(2, 3 * rows_own * TOPK // (2 * sp_count))
    tp_index = lax.axis_index("tp")
    if (
        tp_count == 4 and sp_count % 2 == 0 and sp_count <= 16 and local_heads <= 8
        and rows_own <= 128 and rows_own < 2 * capacity and model_width % 2048 == 0
    ):
        return fused_layer(
            query_rows, key_rows, value_rows, gate_rows, log_decay, head_gain, out_weight, residual, ffn_gain,
            gate_weight[0], up_weight[0], down_weight[0], routes, route_weights,
        )
    own_routes = lax.dynamic_slice_in_dim(routes, tp_index * rows_own, rows_own, 0)
    hidden = retention(query_rows, key_rows, value_rows, gate_rows, log_decay, head_gain)
    mixed = jnp.dot(hidden, out_weight, preferred_element_type=jnp.float32).astype(jnp.bfloat16)
    mixed_sum = lax.psum_scatter(mixed, "tp", scatter_dimension=0, tiled=True).astype(jnp.float32)
    updated = residual.astype(jnp.float32) + mixed_sum
    ffn_in = square_norm(updated, ffn_gain)
    own_experts, own_ranks = slot_ranks(own_routes, sp_count)
    home_slot = own_experts * capacity + own_ranks
    gate_part = gate_weight[0]
    up_part = up_weight[0]
    down_part = down_weight[0]
    empty_row = jnp.zeros((1, model_width), jnp.bfloat16)
    source_row = (
        jnp.full((sp_count * capacity,), rows_own, jnp.int32)
        .at[home_slot]
        .set(jnp.arange(rows_own * TOPK, dtype=jnp.int32) // TOPK)
    )
    padded = jnp.concatenate([ffn_in, empty_row], axis=0)
    outgoing = padded[source_row].reshape(sp_count, capacity, model_width)
    arrived = lax.all_to_all(outgoing, "sp", split_axis=0, concat_axis=0, tiled=True)
    fanned = lax.all_gather(arrived[None], "tp", axis=0, tiled=True)
    activity = expert_rows(fanned.reshape(-1, model_width), gate_part, up_part)
    partial_out = jnp.dot(activity, down_part, preferred_element_type=jnp.float32).reshape(
        tp_count, sp_count, capacity, model_width
    )
    summed = (
        lax.psum_scatter(partial_out.astype(jnp.bfloat16), "tp", scatter_dimension=0, tiled=True)
        .astype(jnp.float32)
        .reshape(sp_count, capacity, model_width)
    )
    returned = lax.all_to_all(
        summed.astype(jnp.bfloat16), "sp", split_axis=0, concat_axis=0, tiled=True
    )
    picked = returned.reshape(sp_count * capacity, model_width)[home_slot].reshape(
        rows_own, TOPK, model_width
    )
    expert_sum = jnp.sum(route_weights[:, :, None] * picked.astype(jnp.float32), axis=1)
    return (updated + expert_sum).astype(jnp.bfloat16)


def solution(mesh):
    return jax.shard_map(
        body,
        mesh=mesh,
        in_specs=(
            P("sp", "tp"),
            P("sp", "tp"),
            P("sp", "tp"),
            P("sp", "tp"),
            P("sp", "tp"),
            P("tp"),
            P("tp", None),
            P(("sp", "tp"), None),
            P(),
            P("sp", None, "tp"),
            P("sp", None, "tp"),
            P("sp", "tp", None),
            P("sp", None),
            P(("sp", "tp"), None),
        ),
        out_specs=P(("sp", "tp"), None),
        check_vma=False,
    )
```

```python
import functools

import jax
import jax.numpy as jnp
import numpy as np
from jax import lax
from jax.experimental import pallas as pl
from jax.experimental.pallas import tpu as pltpu
from jax.sharding import PartitionSpec as P

HEAD_DIM = 128
TOPK = 4
BLOCK = 128


highest = lax.Precision.HIGHEST
rope_base = 10000.0
group_eps = 1e-05
square_eps = 1e-06
clamp_limit = 7.0
swish_alpha = 1.702


def rotary_angles(positions, head_dim):
    half_dim = head_dim // 2
    inverse = rope_base ** (-jnp.arange(half_dim, dtype=jnp.float32) / half_dim)
    return positions[:, None] * inverse[None, :]


def square_norm(updated, gain_row):
    factor = lax.rsqrt(jnp.mean(updated * updated, axis=-1, keepdims=True) + square_eps)
    return (updated * factor * gain_row).astype(jnp.bfloat16)


def expert_rows(rows, gate_part, up_part):
    gate_pre = jnp.dot(rows, gate_part, preferred_element_type=jnp.float32)
    up_pre = jnp.dot(rows, up_part, preferred_element_type=jnp.float32)
    gate_clip = jnp.minimum(gate_pre, clamp_limit)
    up_clip = jnp.clip(up_pre, -clamp_limit, clamp_limit)
    return ((up_clip + 1.0) * (gate_clip * jax.nn.sigmoid(gate_clip * swish_alpha))).astype(
        jnp.bfloat16
    )


def slot_ranks(route_block, experts):
    flat_routes = route_block.reshape(-1)
    onehot = (flat_routes[:, None] == jnp.arange(experts, dtype=jnp.int32)[None, :]).astype(
        jnp.int32
    )
    return (flat_routes, jnp.sum(jnp.cumsum(onehot, axis=0) * onehot, axis=1) - 1)


def retention_kernel(q_ref, k_ref, v_ref, cos_ref, sin_ref, cum_ref, cum_row_ref, ret_ref, qdec_ref, state_ref):
    head = pl.program_id(0)
    length = q_ref.shape[0]
    cosine, sine = cos_ref[...], sin_ref[...]
    half = HEAD_DIM // 2

    def turned(ref):
        rows = ref[...].astype(jnp.float32)
        return rows * cosine + pltpu.roll(rows, half, 1) * sine

    lanes = lax.broadcasted_iota(jnp.int32, cum_ref.shape, 1)
    column = jnp.sum(jnp.where(lanes == head, cum_ref[...], 0.0), axis=1, keepdims=True)
    row = cum_row_ref[0]
    queries = turned(q_ref)
    keys = turned(k_ref) * HEAD_DIM ** (-0.5)
    values = v_ref[...]
    scores = lax.dot_general(
        queries.astype(jnp.bfloat16),
        keys.astype(jnp.bfloat16),
        (((1,), (1,)), ((), ())),
        preferred_element_type=jnp.float32,
    )
    causal = lax.broadcasted_iota(jnp.int32, (length, length), 0) >= lax.broadcasted_iota(
        jnp.int32, (length, length), 1
    )
    weights = jnp.where(causal, jnp.exp(jnp.minimum(column - row, 0.0)), 0.0)
    ret_ref[...] = jnp.dot(
        (scores * weights).astype(jnp.bfloat16), values, preferred_element_type=jnp.float32
    )
    qdec_ref[...] = (queries * jnp.exp(column)).astype(jnp.bfloat16)
    total = column[length - 1 :, :]
    tailed = (keys * jnp.exp(total - column)).astype(jnp.bfloat16)
    state_ref[0, :HEAD_DIM, :] = lax.dot_general(
        tailed, values, (((0,), (0,)), ((), ())), preferred_element_type=jnp.float32
    )
    state_ref[0, HEAD_DIM:, :] = jnp.broadcast_to(total, (8, HEAD_DIM))


def norm_kernel(ret_ref, qdec_ref, enter_ref, gain_ref, gate_ref, hidden_ref):
    retained = ret_ref[...] + jnp.dot(
        qdec_ref[...], enter_ref[0].astype(jnp.bfloat16), preferred_element_type=jnp.float32
    )
    centred = retained - jnp.mean(retained, axis=-1, keepdims=True)
    variance = jnp.mean(centred * centred, axis=-1, keepdims=True)
    gate = gate_ref[...].astype(jnp.float32)
    scaled = centred * lax.rsqrt(variance + group_eps) * gain_ref[...]
    hidden_ref[...] = (scaled * (gate / (1.0 + jnp.exp(-gate)))).astype(jnp.bfloat16)


def retention(query_rows, key_rows, value_rows, gate_rows, log_decay, head_gain):
    length, local_heads = log_decay.shape
    width = query_rows.shape[1]
    sp_count, mine = lax.axis_size("sp"), lax.axis_index("sp")
    positions = (mine * length + jnp.arange(length, dtype=jnp.int32)).astype(jnp.float32)
    angles = rotary_angles(positions, HEAD_DIM)
    cosine, sine = jnp.cos(angles), jnp.sin(angles)
    cosine = jnp.concatenate([cosine, cosine], axis=1)
    sine = jnp.concatenate([-sine, sine], axis=1)
    cumulative = jnp.cumsum(log_decay, axis=0)
    rows_spec = pl.BlockSpec((length, HEAD_DIM), lambda h: (0, h))
    table_spec = pl.BlockSpec((length, HEAD_DIM), lambda h: (0, 0))
    retained, qdec, state = pl.pallas_call(
        retention_kernel,
        grid=(local_heads,),
        out_shape=(
            jax.ShapeDtypeStruct((length, width), jnp.float32),
            jax.ShapeDtypeStruct((length, width), jnp.bfloat16),
            jax.ShapeDtypeStruct((local_heads, HEAD_DIM + 8, HEAD_DIM), jnp.float32),
        ),
        in_specs=[
            rows_spec,
            rows_spec,
            rows_spec,
            table_spec,
            table_spec,
            pl.BlockSpec((length, local_heads), lambda h: (0, 0)),
            pl.BlockSpec((1, 1, length), lambda h: (h, 0, 0)),
        ],
        out_specs=(
            rows_spec,
            rows_spec,
            pl.BlockSpec((1, HEAD_DIM + 8, HEAD_DIM), lambda h: (h, 0, 0)),
        ),
    )(query_rows, key_rows, value_rows, cosine, sine, cumulative, cumulative.T[:, None, :])
    pieces = lax.all_gather(state, "sp")
    totals = pieces[:, :, HEAD_DIM, 0]
    index = jnp.arange(sp_count, dtype=jnp.int32)
    between = (index[None, :] > index[:, None]) & (index[None, :] < mine)
    gap = jnp.sum(jnp.where(between[:, :, None], totals[None], 0.0), axis=1)
    factor = jnp.where((index < mine)[:, None], jnp.exp(gap), 0.0)
    entering = jnp.sum(factor[:, :, None, None] * pieces[:, :, :HEAD_DIM, :], axis=0)
    return pl.pallas_call(
        norm_kernel,
        grid=(local_heads,),
        out_shape=jax.ShapeDtypeStruct((length, width), jnp.bfloat16),
        in_specs=[
            rows_spec,
            rows_spec,
            pl.BlockSpec((1, HEAD_DIM, HEAD_DIM), lambda h: (h, 0, 0)),
            pl.BlockSpec((1, HEAD_DIM), lambda h: (0, h)),
            rows_spec,
        ],
        out_specs=rows_spec,
    )(retained, qdec, entering, head_gain[None, :], gate_rows)


(
    UP_A, UP_B, DOWN_A, DOWN_B, X_A2, Y_B2, Y_A3, Y_A4, X_B3, X_B4, C_A, C_B, C_P, Y_A, X_B, X_A, Y_B, RZ_A, RZ_B,
    TOTAL, CHAIN, ACROSS, MIX_C, MIX_Y, S_X2, S_Y2, S_Y3, S_X3, S_Y4, S_X4, S_UP, S_DOWN, S_CORE,
) = range(33)


def layer_kernel(
    planes, logs_hbm, k_hbm, near_hbm, base_hbm, v_hbm, q_hbm, gate_hbm, gain_hbm, routes_hbm, shares_hbm,
    residual_hbm, ffn_gain_hbm, wo_hbm, wg_hbm, wu_hbm, wd_hbm, out,
    logs, k_ref, near_table, base_table, v_ref, q_ref, gate_ref, head_gain, routes, route_weights,
    residual, ffn_gain, wo, wg, wu, wd, rotary, turned_k, ret, qdec, state, cum_col, cum_row, total_own, total_x, carry_in, carry_out,
    side_out, side_in, hidden, blend, from_core, held, from_y, upd,
    share_in, g0, g1, gs, pm, pr, a0, a1, r10, r11, b0, b1, r20, r21, d0, d1, z0, z1,
    ssem, rsem, wsem,
):
    sp, tp = lax.axis_index("sp"), lax.axis_index("tp")
    sp_count = 2 * planes
    z, x = sp // 2, sp % 2
    y, c = tp // 2, tp % 2
    own_rows, width = out.shape
    half = width // 2
    wide_a, wide_b = g0.shape[-1] - 128, g1.shape[-1]
    wide_ab = wide_a + wide_b
    rows = own_rows // 2
    items = 2 * planes
    lag = items - 3
    f32, bf16 = jnp.float32, jnp.bfloat16
    to_core = {"sp": sp, "tp": y * 2 + (1 - c)}
    to_y = {"sp": sp, "tp": (1 - y) * 2 + c}
    to_x = {"sp": z * 2 + (1 - x), "tp": tp}

    def half_of(n):
        return jnp.where(n == items - 1, 1, jnp.where(n == 0, 0, (n + 1) % 2))

    def plane_at(k):
        low = z < planes // 2
        mirrored = jnp.where(low, z, planes - 1 - z)
        q = jnp.where(k <= mirrored, mirrored - k, k)
        return jnp.where(low, q, planes - 1 - q)

    def plane_of(n):
        return plane_at(((n + 1) // 2) % planes)

    def item_of(n):
        return 2 * plane_of(n) + half_of(n)

    def step_of(turn):
        back = items - 3 - 2 * ((turn - 2) // 2) + turn % 2
        kept = (turn <= 1) | (turn == items - 1)
        return jnp.where(kept, turn, jnp.where(turn == items - 2, 2, back))

    def has_turn(u):
        return (u >= 0) & (u < items)

    def at_plane(p):
        return {"sp": p * 2 + x, "tp": tp}

    def to_z(i):
        return at_plane((z + planes - i) % planes)

    def move(kind, n, src, dst, device, m=None):
        return pltpu.make_async_remote_copy(
            src_ref=src, dst_ref=dst, send_sem=ssem.at[kind, n],
            recv_sem=rsem.at[kind, n if m is None else m],
            device_id=device, device_id_type=pl.DeviceIdType.MESH,
        )

    def send(kind, n, src, dst, device, m=None):
        move(kind, n, src, dst, device, m).start()

    def arrived(kind, n, dst):
        move(kind, n, dst, dst, to_core).wait_recv()

    def left(kind, n, src):
        move(kind, n, src, src, to_core).wait_send()

    loads = [
        pltpu.make_async_copy(far, near, wsem.at[i])
        for i, (far, near) in enumerate(
            [
                (logs_hbm, logs), (k_hbm, k_ref), (near_hbm, near_table), (base_hbm, base_table), (v_hbm, v_ref),
                (q_hbm, q_ref), (gate_hbm, gate_ref), (gain_hbm, head_gain), (routes_hbm, routes),
                (shares_hbm, route_weights), (residual_hbm, residual), (ffn_gain_hbm, ffn_gain),
                (wo_hbm, wo), (wg_hbm, wg), (wu_hbm, wu), (wd_hbm, wd),
            ]
        )
    ]
    for copy in loads:
        copy.start()
    barrier = pltpu.get_barrier_semaphore()
    for device in [to_core, to_y, to_x] + [to_z(i) for i in range(1, planes)]:
        pl.semaphore_signal(barrier, inc=1, device_id=device, device_id_type=pl.DeviceIdType.MESH)

    length = q_ref.shape[0]
    dim = HEAD_DIM
    heads = q_ref.shape[1] // dim
    depth = state.shape[1]
    cuts = dim // depth
    after = lax.broadcasted_iota(jnp.int32, (length, length), 0) >= lax.broadcasted_iota(
        jnp.int32, (length, length), 1
    )
    ones = jnp.where(after, 1.0, 0.0).astype(f32)
    loads[0].wait()
    log_rows = jnp.concatenate([logs[...], jnp.zeros((8 - heads, length), f32)], axis=0)
    cum_row[...] = lax.dot_general(
        log_rows, ones, (((1,), (1,)), ((), ())), precision=highest, preferred_element_type=f32
    )
    cum_col[...] = lax.dot_general(
        ones, log_rows, (((1,), (1,)), ((), ())), precision=highest, preferred_element_type=f32
    )
    total_own[...] = jnp.broadcast_to(cum_row[:, length - 1 :], (8, dim))
    pl.semaphore_wait(barrier, 2 + planes)
    send(TOTAL, 0, total_own, total_x, to_x)

    loads[2].wait()
    loads[3].wait()
    base = base_table[pl.ds(sp * 8, 8), :]
    cosine = base[0:1] * near_table[0] - base[1:2] * near_table[1]
    sine = base[2:3] * near_table[0] + base[3:4] * near_table[1]
    rotary[0] = cosine
    rotary[1] = sine

    def turned(rows_in):
        wide = rows_in.astype(f32)
        return wide * rotary[0] + pltpu.roll(wide, dim // 2, 1) * rotary[1]

    def column_of(h):
        lanes = lax.broadcasted_iota(jnp.int32, cum_col.shape, 1)
        return jnp.sum(jnp.where(lanes == h, cum_col[...], 0.0), axis=1, keepdims=True)

    left_side = x == 0

    def pass_state(e):
        h = e // cuts
        own_total, x_total = total_own[h : h + 1, :], total_x[h : h + 1, :]
        before = carry_in[e].astype(f32)

        @pl.when(z + 1 < planes)
        def _():
            fresh = jnp.where(left_side, jnp.exp(x_total), 1.0) * state[e]
            carry_out[e] = (jnp.exp(own_total + x_total) * before + fresh).astype(bf16)
            send(CHAIN, e, carry_out.at[e], carry_in.at[e], at_plane(z + 1))

        side_out[e] = jnp.where(left_side, jnp.exp(own_total) * before + state[e], before).astype(bf16)
        send(ACROSS, e, side_out.at[e], side_in.at[e], to_x)

    @pl.when(z == 0)
    def _():
        carry_in[...] = jnp.zeros_like(carry_in)

    loads[1].wait()
    loads[4].wait()
    for h in range(heads):
        lanes = pl.ds(h * dim, dim)
        keys = turned(k_ref[:, lanes]) * dim ** (-0.5)
        turned_k[:, lanes] = keys.astype(bf16)
        column = column_of(h)
        tailed = (keys * jnp.exp(column[length - 1 :, :] - column)).astype(bf16)
        state[cuts * h : cuts * (h + 1)] = lax.dot_general(
            tailed, v_ref[:, lanes], (((0,), (0,)), ((), ())), preferred_element_type=f32
        ).reshape(cuts, depth, dim)

        @pl.when(z == 0)
        def _():
            if h == 0:
                arrived(TOTAL, 0, total_x)
            for e in range(cuts * h, cuts * (h + 1)):
                pass_state(e)

    def attend(h, carry):
        lanes = pl.ds(pl.multiple_of(h * dim, dim), dim)
        queries = turned(q_ref[:, lanes])
        column = column_of(h)
        scores = lax.dot_general(
            queries.astype(bf16), turned_k[:, lanes], (((1,), (1,)), ((), ())), preferred_element_type=f32
        )
        gap = jnp.minimum(column - cum_row[pl.ds(h, 1), :], 0.0)
        decays = jnp.where(after, jnp.exp(gap), 0.0)
        ret[:, lanes] = jnp.dot((scores * decays).astype(bf16), v_ref[:, lanes], preferred_element_type=f32)
        qdec[:, lanes] = (queries * jnp.exp(column)).astype(bf16)
        return carry

    early = jnp.where(z >= planes // 2, heads, 0)
    loads[5].wait()
    lax.fori_loop(0, early, attend, 0)

    @pl.when(z > 0)
    def _():
        arrived(TOTAL, 0, total_x)

    for e in range(cuts * heads):

        @pl.when(z > 0)
        def _():
            arrived(CHAIN, e, carry_in.at[e])
            pass_state(e)

    lax.fori_loop(early, heads, attend, 0)

    for h in range(heads):
        lanes = pl.ds(h * dim, dim)
        if h == 0:
            loads[6].wait()
            loads[7].wait()
        blocks = slice(cuts * h, cuts * (h + 1))
        for e in range(cuts * h, cuts * (h + 1)):
            arrived(ACROSS, e, side_in.at[e])
        factor = jnp.where(left_side, 1.0, jnp.exp(total_x[h : h + 1, :]))
        before = carry_in[blocks].reshape(dim, dim).astype(f32)
        entering = (factor * before + side_in[blocks].reshape(dim, dim).astype(f32)).astype(bf16)
        retained = ret[:, lanes] + jnp.dot(qdec[:, lanes], entering, preferred_element_type=f32)
        centred = retained - jnp.mean(retained, axis=-1, keepdims=True)
        variance = jnp.mean(centred * centred, axis=-1, keepdims=True)
        gate_in = gate_ref[:, lanes].astype(f32)
        scaled = centred * lax.rsqrt(variance + group_eps) * head_gain[:, lanes]
        made = (scaled * (gate_in / (1.0 + jnp.exp(-gate_in)))).astype(bf16)
        hidden[:, :, lanes] = made.reshape(4, own_rows, dim)

    loads[12].wait()
    pieces = blend.shape[0]
    spans = pieces // 2
    span = width // spans

    def cross(j):
        arrived(MIX_C, j, from_core.at[j])
        held[j] = (blend[j, c, 1 - y].astype(f32) + from_core[j, 1 - y].astype(f32)).astype(bf16)
        send(MIX_Y, j, held.at[j], from_y.at[j], to_y)

    for j in range(pieces):
        picked = hidden[:, j // spans * rows : (j // spans + 1) * rows, :].reshape(4 * rows, heads * dim)
        mixed = jnp.dot(picked, wo[:, pl.ds(j % spans * span, span)], preferred_element_type=f32).astype(bf16)
        for q in range(4):
            blend[j, q % 2, q // 2] = mixed[q * rows : (q + 1) * rows, :]
        send(MIX_C, j, blend.at[j, 1 - c], from_core.at[j], to_core)
        if j > 0:
            cross(j - 1)
    cross(pieces - 1)

    here = x * 2 + y
    other_x = (1 - x) * 2 + y
    other_y = x * 2 + (1 - y)
    other_xy = (1 - x) * 2 + (1 - y)
    for copy in loads[8:12]:
        copy.wait()
    count = routes.shape[0]
    share_in[...] = jnp.zeros_like(share_in)
    share_in[:count, :own_rows] = route_weights[...]
    all_routes = jnp.concatenate([routes[...]] * (8 // count), axis=0)
    own_routes = jnp.zeros((8, 128), jnp.int32)
    for q in range(4):
        turned_routes = pltpu.roll(all_routes, (length - q * own_rows) % length, 1)
        own_routes = own_routes + jnp.where(tp == q, turned_routes[:, :128], 0)
    expert = lax.broadcasted_iota(jnp.int32, (128, 128), 0)
    shares = jnp.zeros((128, 128), f32)
    for k in range(count):
        shares = shares + jnp.where(own_routes[k : k + 1, :] == expert, share_in[k : k + 1, :], 0.0)
    share = jnp.transpose(shares)[:own_rows, :]
    coarse = share.astype(bf16).astype(f32)
    tail_rows = (coarse + pltpu.roll(share - coarse, sp_count, 1)).astype(bf16)
    first_rows, last_rows = pl.ds(0, rows), pl.ds(rows, rows)
    def side(p, chip, part):
        return gs.at[c, p, chip, part]

    def pass_side(kind, n, chip, part, device):
        send(kind, n, side(z, chip, part), side(z, chip, part), device)

    def spread_side(r):
        if r == 0:
            pass_side(S_X2, 0, here, first_rows, to_x)
            pass_side(S_Y3, 0, here, first_rows, to_y)
        else:
            pass_side(S_Y2, 0, here, last_rows, to_y)
            pass_side(S_X3, 0, here, last_rows, to_x)

    def relay_side():
        arrived(S_X2, 0, side(z, other_x, first_rows))
        pass_side(S_Y4, 0, other_x, first_rows, to_y)
        arrived(S_Y2, 0, side(z, other_y, last_rows))
        pass_side(S_X4, 0, other_y, last_rows, to_x)

    def side_up(p):
        @pl.when(z + 1 < planes)
        def _():
            send(S_UP, p, gs.at[c, p], gs.at[c, p], at_plane(z + 1))

    def side_down(p):
        @pl.when(z > 0)
        def _():
            send(S_DOWN, p, gs.at[c, p], gs.at[c, p], at_plane(z - 1))

    def side_core(p):
        send(S_CORE, p, gs.at[c, p], gs.at[c, p], to_core)

    def close_side():
        arrived(S_Y3, 0, side(z, other_y, first_rows))
        arrived(S_Y4, 0, side(z, other_xy, first_rows))
        arrived(S_X3, 0, side(z, other_x, last_rows))
        arrived(S_X4, 0, side(z, other_xy, last_rows))
        side_up(z)
        side_down(z)
        side_core(z)

    def spread(n):
        send(X_A2, n, g0.at[c, n, here], g0.at[c, n, here], to_x)
        send(Y_B2, n, g1.at[c, n, here], g1.at[c, n, here], to_y)
        send(Y_A3, n, g0.at[c, n, here], g0.at[c, n, here], to_y)
        send(X_B3, n, g1.at[c, n, here], g1.at[c, n, here], to_x)

    def raise_up(n):
        @pl.when(z + 1 < planes)
        def _():
            send(UP_A, n, g0.at[c, n, here], g0.at[c, n, here], at_plane(z + 1))
            send(UP_B, n, g1.at[c, n, here], g1.at[c, n, here], at_plane(z + 1))

    def hand_down(n):
        @pl.when(z > 0)
        def _():
            send(DOWN_A, n, g0.at[c, n, here], g0.at[c, n, here], at_plane(z - 1))
            send(DOWN_B, n, g1.at[c, n, here], g1.at[c, n, here], at_plane(z - 1))

    for r in range(2):
        mine, n = slice(r * rows, (r + 1) * rows), 2 * z + r
        square = jnp.zeros((rows, 1), f32)
        for j in range(r * spans, (r + 1) * spans):
            cols = pl.ds(j % spans * span, span)
            near = residual[mine, cols].astype(f32) + blend[j, c, y].astype(f32) + from_core[j, y].astype(f32)
            arrived(MIX_Y, j, from_y.at[j])
            total = near + from_y[j].astype(f32)
            upd[mine, cols] = total
            square = square + jnp.sum(total * total, axis=-1, keepdims=True)
        scale = lax.rsqrt(square * (1.0 / width) + square_eps)
        ready = (upd[mine, :] * scale * ffn_gain[...]).astype(bf16)
        g0[c, n, here, :, :wide_a] = ready[:, :wide_a]
        g0[c, n, here, :, wide_a:] = tail_rows[mine]
        g1[c, n, here] = ready[:, wide_a:wide_ab]
        gs[c, z, here, mine, :] = ready[:, wide_ab:]
        raise_up(n)
        hand_down(n)
        spread_side(r)
        if r == 0:
            spread(n)

    def tick(t, carry):
        def relay():
            n = item_of(t)
            arrived(X_A2, n, g0.at[c, n, other_x])
            send(Y_A4, n, g0.at[c, n, other_x], g0.at[c, n, other_x], to_y)
            arrived(Y_B2, n, g1.at[c, n, other_y])
            send(X_B4, n, g1.at[c, n, other_y], g1.at[c, n, other_y], to_x)

        pl.when(t == 0)(relay_side)
        pl.when(t == 0)(relay)
        pl.when(t == 1)(close_side)

        @pl.when(t + 1 < items)
        def _():
            k, r = (t + 2) // 2, t % 2

            @pl.when((t + 1 < items - 1) & (z - k >= 0))
            def _():
                n = 2 * (z - k) + r
                arrived(UP_A, n, g0.at[c, n, here])
                arrived(UP_B, n, g1.at[c, n, here])
                raise_up(n)

            @pl.when((t + 1 < items - 1) & (z + k < planes))
            def _():
                n = 2 * (z + k) + r
                arrived(DOWN_A, n, g0.at[c, n, here])
                arrived(DOWN_B, n, g1.at[c, n, here])
                hand_down(n)

            spread(item_of(t + 1))

        pl.when((t > 0) & (t < items))(relay)

        @pl.when((t >= 2) & (t < items) & (t % 2 == 0))
        def _():
            below, above = z - t // 2, z + t // 2

            @pl.when(below >= 0)
            def _():
                arrived(S_UP, below, gs.at[c, below])
                side_up(below)
                side_core(below)

            @pl.when(above < planes)
            def _():
                arrived(S_DOWN, above, gs.at[c, above])
                side_down(above)
                side_core(above)

        @pl.when(t == 2)
        def _():
            for copy in loads[13:]:
                copy.wait()

        @pl.when((t >= 2) & (t < items + 2))
        def _():
            n = item_of(t - 2)
            arrived(C_A, n, g0.at[1 - c, n])
            arrived(C_B, n, g1.at[1 - c, n])
            p, r = plane_of(t - 2), half_of(t - 2)

            @pl.when(r == 0)
            def _():
                arrived(S_CORE, p, gs.at[1 - c, p])

            lead = g0[:, n].reshape(8 * rows, wide_a + 128)
            tail = lead[:, wide_a:].astype(f32)
            rest = g1[:, n].reshape(8 * rows, wide_b)
            last = gs[:, p, :, pl.ds(pl.multiple_of(r * rows, rows), rows), :].reshape(8 * rows, width - wide_ab)
            rows_in = jnp.concatenate([lead[:, :wide_a], rest, last], axis=1)
            lane = lax.broadcasted_iota(jnp.int32, tail.shape, 1)
            weight = jnp.sum(
                jnp.where((lane == sp) | (lane == sp + sp_count), tail, 0.0), axis=1, keepdims=True
            )

            def product(w):
                return jnp.dot(rows_in, w[...], preferred_element_type=f32)

            gate = jnp.minimum(product(wg), clamp_limit)
            up = jnp.clip(product(wu), -clamp_limit, clamp_limit)
            act = ((up + 1.0) * (gate / (1.0 + jnp.exp(-swish_alpha * gate)))).astype(bf16)
            made = (jnp.dot(act, wd[...], preferred_element_type=f32) * weight).astype(bf16)
            pm[n] = made.reshape(2, 4 * rows, 2 * half)
            send(C_P, n, pm.at[n, 1 - c], pr.at[n], to_core)

        @pl.when((t >= 1) & (t < items + 1))
        def _():
            n = item_of(t - 1)
            arrived(Y_A3, n, g0.at[c, n, other_y])
            arrived(Y_A4, n, g0.at[c, n, other_xy])
            arrived(X_B3, n, g1.at[c, n, other_x])
            arrived(X_B4, n, g1.at[c, n, other_xy])
            send(C_A, n, g0.at[c, n], g0.at[c, n], to_core)
            send(C_B, n, g1.at[c, n], g1.at[c, n], to_core)

        @pl.when(has_turn(t - lag))
        def _():
            n = item_of(step_of(t - lag))
            arrived(C_P, n, pr.at[n])
            for q in range(4):
                part = pl.ds(q * rows, rows)
                total = (pm[n, c, part, :].astype(f32) + pr[n, part, :].astype(f32)).astype(bf16)
                a0[n, q % 2, q // 2] = total[:, :half]
                a1[n, q // 2, q % 2] = total[:, half:]
            send(Y_A, n, a0.at[n, 1 - y], r10.at[n], to_y)
            send(X_B, n, a1.at[n, 1 - x], r11.at[n], to_x)

        @pl.when(has_turn(t - lag - 1))
        def _():
            n = item_of(step_of(t - lag - 1))
            arrived(Y_A, n, r10.at[n])
            b0[n] = (a0[n, y].astype(f32) + r10[n].astype(f32)).astype(bf16)
            send(X_A, n, b0.at[n, 1 - x], r20.at[n], to_x)
            arrived(X_B, n, r11.at[n])
            b1[n] = (a1[n, x].astype(f32) + r11[n].astype(f32)).astype(bf16)
            send(Y_B, n, b1.at[n, 1 - y], r21.at[n], to_y)

        @pl.when(has_turn(t - lag - 2))
        def _():
            turn = step_of(t - lag - 2)
            n = item_of(turn)
            arrived(X_A, n, r20.at[n])
            d0[n] = (b0[n, x].astype(f32) + r20[n].astype(f32)).astype(bf16)
            arrived(Y_B, n, r21.at[n])
            d1[n] = (b1[n, y].astype(f32) + r21[n].astype(f32)).astype(bf16)

            @pl.when((turn > 0) & (turn < items - 1))
            def _():
                m = 2 * z + half_of(turn)
                send(RZ_A, n, d0.at[n], z0.at[m], at_plane(plane_of(turn)), m)
                send(RZ_B, n, d1.at[n], z1.at[m], at_plane(plane_of(turn)), m)

        return carry

    lax.fori_loop(0, items + lag + 2, tick, 0)
    for r in range(2):
        n, part = 2 * z + r, pl.ds(r * rows, rows)
        low = upd[part, :half] + d0[n].astype(f32)
        high = upd[part, half:] + d1[n].astype(f32)
        for i in range(1, planes):
            n = 2 * ((z + i) % planes) + r
            arrived(RZ_A, n, z0.at[n])
            low = low + z0[n].astype(f32)
            arrived(RZ_B, n, z1.at[n])
            high = high + z1[n].astype(f32)
        out[part, :half] = low.astype(bf16)
        out[part, half:] = high.astype(bf16)

    def drain(n, carry):
        p = n // 2

        @pl.when((p <= z) & (z + 1 < planes))
        def _():
            left(UP_A, n, g0.at[c, n, here])
            left(UP_B, n, g1.at[c, n, here])

        @pl.when((p >= z) & (z > 0))
        def _():
            left(DOWN_A, n, g0.at[c, n, here])
            left(DOWN_B, n, g1.at[c, n, here])

        @pl.when((p < z) | (p > z))
        def _():
            left(RZ_A, n, d0.at[n])
            left(RZ_B, n, d1.at[n])

        left(X_A2, n, g0.at[c, n, here])
        left(Y_B2, n, g1.at[c, n, here])
        left(Y_A3, n, g0.at[c, n, here])
        left(X_B3, n, g1.at[c, n, here])
        left(Y_A4, n, g0.at[c, n, other_x])
        left(X_B4, n, g1.at[c, n, other_y])
        left(C_A, n, g0.at[c, n])
        left(C_B, n, g1.at[c, n])
        left(C_P, n, pm.at[n, 1 - c])
        left(Y_A, n, a0.at[n, 1 - y])
        left(X_B, n, a1.at[n, 1 - x])
        left(X_A, n, b0.at[n, 1 - x])
        left(Y_B, n, b1.at[n, 1 - y])
        return carry

    lax.fori_loop(0, items, drain, 0)
    left(S_X2, 0, side(z, here, first_rows))
    left(S_Y2, 0, side(z, here, last_rows))
    left(S_Y3, 0, side(z, here, first_rows))
    left(S_X3, 0, side(z, here, last_rows))
    left(S_Y4, 0, side(z, other_x, first_rows))
    left(S_X4, 0, side(z, other_y, last_rows))

    def drain_side(p, carry):
        @pl.when((p <= z) & (z + 1 < planes))
        def _():
            left(S_UP, p, gs.at[c, p])

        @pl.when((p >= z) & (z > 0))
        def _():
            left(S_DOWN, p, gs.at[c, p])

        left(S_CORE, p, gs.at[c, p])
        return carry

    lax.fori_loop(0, planes, drain_side, 0)
    left(TOTAL, 0, total_own)
    for e in range(cuts * heads):
        left(ACROSS, e, side_out.at[e])

        @pl.when(z + 1 < planes)
        def _():
            left(CHAIN, e, carry_out.at[e])

    for j in range(pieces):
        left(MIX_C, j, blend.at[j, 1 - c])
        left(MIX_Y, j, held.at[j])


def rope_tables(length, spans):
    half_dim = HEAD_DIM // 2
    rates = rope_base ** (-np.arange(half_dim, dtype=np.float64) / half_dim)
    rates = np.concatenate([rates, rates])[None, :]
    near = np.arange(length, dtype=np.float64)[:, None] * rates
    starts = (np.arange(spans, dtype=np.float64) * length)[:, None] * rates
    sign = np.concatenate([-np.ones(half_dim), np.ones(half_dim)])[None, :]
    base = np.zeros((spans, 8, HEAD_DIM))
    base[:, 0], base[:, 1] = np.cos(starts), np.sin(starts)
    base[:, 2], base[:, 3] = sign * np.sin(starts), sign * np.cos(starts)
    near_table = np.stack([np.cos(near), np.sin(near)]).astype(np.float32)
    return jnp.asarray(near_table), jnp.asarray(base.reshape(spans * 8, HEAD_DIM).astype(np.float32))


def fused_layer(
    query_rows, key_rows, value_rows, gate_rows, log_decay, head_gain, out_weight, residual, ffn_gain,
    gate_part, up_part, down_part, routes, route_weights,
):
    sp_count = lax.axis_size("sp")
    length, heads = log_decay.shape
    rows_all, width = residual.shape
    inner = query_rows.shape[1]
    near_table, base_table = rope_tables(length, sp_count)
    half = width // 2
    planes = sp_count // 2
    items = 2 * planes
    rows = rows_all // 2
    pieces = 8
    span = 2 * width // pieces
    wide_s = 128 * (3 * width // 2048)
    wide_a = (width - wide_s - 128) // 256 * 128
    wide_b = width - wide_s - wide_a
    bf16, f32 = jnp.bfloat16, jnp.float32
    whole = pl.BlockSpec(memory_space=pltpu.VMEM)
    far = pl.BlockSpec(memory_space=pltpu.HBM)
    operands = (
        log_decay.T, key_rows, near_table, base_table, value_rows, query_rows, gate_rows, head_gain[None, :],
        routes.T, route_weights.T, residual, ffn_gain[None, :], out_weight, gate_part, up_part, down_part,
    )
    square = (2 * heads, HEAD_DIM // 2, HEAD_DIM)
    return pl.pallas_call(
        functools.partial(layer_kernel, planes),
        out_shape=jax.ShapeDtypeStruct((rows_all, width), bf16),
        in_specs=[far] * len(operands),
        out_specs=whole,
        scratch_shapes=[
            *[pltpu.VMEM(operand.shape, operand.dtype) for operand in operands],
            pltpu.VMEM((2, length, HEAD_DIM), f32),
            pltpu.VMEM((length, inner), bf16),
            pltpu.VMEM((length, inner), f32),
            pltpu.VMEM((length, inner), bf16),
            pltpu.VMEM(square, f32),
            pltpu.VMEM((length, 8), f32),
            pltpu.VMEM((8, length), f32),
            pltpu.VMEM((8, HEAD_DIM), f32),
            pltpu.VMEM((8, HEAD_DIM), f32),
            pltpu.VMEM(square, bf16),
            pltpu.VMEM(square, bf16),
            pltpu.VMEM(square, bf16),
            pltpu.VMEM(square, bf16),
            pltpu.VMEM((4, rows_all, inner), bf16),
            pltpu.VMEM((pieces, 2, 2, rows, span), bf16),
            pltpu.VMEM((pieces, 2, rows, span), bf16),
            pltpu.VMEM((pieces, rows, span), bf16),
            pltpu.VMEM((pieces, rows, span), bf16),
            pltpu.VMEM((rows_all, width), f32),
            pltpu.VMEM((8, 128), f32),
            pltpu.VMEM((2, items, 4, rows, wide_a + 128), bf16),
            pltpu.VMEM((2, items, 4, rows, wide_b), bf16),
            pltpu.VMEM((2, planes, 4, rows_all, wide_s), bf16),
            pltpu.VMEM((items, 2, 4 * rows, width), bf16),
            pltpu.VMEM((items, 4 * rows, width), bf16),
            pltpu.VMEM((items, 2, 2, rows, half), bf16),
            pltpu.VMEM((items, 2, 2, rows, half), bf16),
            pltpu.VMEM((items, 2, rows, half), bf16),
            pltpu.VMEM((items, 2, rows, half), bf16),
            pltpu.VMEM((items, 2, rows, half), bf16),
            pltpu.VMEM((items, 2, rows, half), bf16),
            pltpu.VMEM((items, rows, half), bf16),
            pltpu.VMEM((items, rows, half), bf16),
            pltpu.VMEM((items, rows, half), bf16),
            pltpu.VMEM((items, rows, half), bf16),
            pltpu.VMEM((items, rows, half), bf16),
            pltpu.VMEM((items, rows, half), bf16),
            pltpu.SemaphoreType.DMA((33, max(items, 2 * heads, pieces))),
            pltpu.SemaphoreType.DMA((33, max(items, 2 * heads, pieces))),
            pltpu.SemaphoreType.DMA((len(operands),)),
        ],
        compiler_params=pltpu.CompilerParams(
            collective_id=0, has_side_effects=True, vmem_limit_bytes=63 * 1024 * 1024
        ),
    )(*operands)


def body(
    query_rows,
    key_rows,
    value_rows,
    gate_rows,
    log_decay,
    head_gain,
    out_weight,
    residual,
    ffn_gain,
    gate_weight,
    up_weight,
    down_weight,
    routes,
    route_weights,
):
    tok_count = query_rows.shape[0]
    local_heads = log_decay.shape[1]
    sp_count = lax.axis_size("sp")
    tp_count = lax.axis_size("tp")
    model_width = residual.shape[1]
    rows_own = tok_count // tp_count
    capacity = max(2, 3 * rows_own * TOPK // (2 * sp_count))
    tp_index = lax.axis_index("tp")
    if (
        tp_count == 4 and sp_count % 2 == 0 and sp_count <= 16 and local_heads <= 8
        and rows_own <= 128 and rows_own < 2 * capacity and model_width % 2048 == 0
    ):
        return fused_layer(
            query_rows, key_rows, value_rows, gate_rows, log_decay, head_gain, out_weight, residual, ffn_gain,
            gate_weight[0], up_weight[0], down_weight[0], routes, route_weights,
        )
    own_routes = lax.dynamic_slice_in_dim(routes, tp_index * rows_own, rows_own, 0)
    hidden = retention(query_rows, key_rows, value_rows, gate_rows, log_decay, head_gain)
    mixed = jnp.dot(hidden, out_weight, preferred_element_type=jnp.float32).astype(jnp.bfloat16)
    mixed_sum = lax.psum_scatter(mixed, "tp", scatter_dimension=0, tiled=True).astype(jnp.float32)
    updated = residual.astype(jnp.float32) + mixed_sum
    ffn_in = square_norm(updated, ffn_gain)
    own_experts, own_ranks = slot_ranks(own_routes, sp_count)
    home_slot = own_experts * capacity + own_ranks
    gate_part = gate_weight[0]
    up_part = up_weight[0]
    down_part = down_weight[0]
    empty_row = jnp.zeros((1, model_width), jnp.bfloat16)
    source_row = (
        jnp.full((sp_count * capacity,), rows_own, jnp.int32)
        .at[home_slot]
        .set(jnp.arange(rows_own * TOPK, dtype=jnp.int32) // TOPK)
    )
    padded = jnp.concatenate([ffn_in, empty_row], axis=0)
    outgoing = padded[source_row].reshape(sp_count, capacity, model_width)
    arrived = lax.all_to_all(outgoing, "sp", split_axis=0, concat_axis=0, tiled=True)
    fanned = lax.all_gather(arrived[None], "tp", axis=0, tiled=True)
    activity = expert_rows(fanned.reshape(-1, model_width), gate_part, up_part)
    partial_out = jnp.dot(activity, down_part, preferred_element_type=jnp.float32).reshape(
        tp_count, sp_count, capacity, model_width
    )
    summed = (
        lax.psum_scatter(partial_out.astype(jnp.bfloat16), "tp", scatter_dimension=0, tiled=True)
        .astype(jnp.float32)
        .reshape(sp_count, capacity, model_width)
    )
    returned = lax.all_to_all(
        summed.astype(jnp.bfloat16), "sp", split_axis=0, concat_axis=0, tiled=True
    )
    picked = returned.reshape(sp_count * capacity, model_width)[home_slot].reshape(
        rows_own, TOPK, model_width
    )
    expert_sum = jnp.sum(route_weights[:, :, None] * picked.astype(jnp.float32), axis=1)
    return (updated + expert_sum).astype(jnp.bfloat16)


def solution(mesh):
    return jax.shard_map(
        body,
        mesh=mesh,
        in_specs=(
            P("sp", "tp"),
            P("sp", "tp"),
            P("sp", "tp"),
            P("sp", "tp"),
            P("sp", "tp"),
            P("tp"),
            P("tp", None),
            P(("sp", "tp"), None),
            P(),
            P("sp", None, "tp"),
            P("sp", None, "tp"),
            P("sp", "tp", None),
            P("sp", None),
            P(("sp", "tp"), None),
        ),
        out_specs=P(("sp", "tp"), None),
        check_vma=False,
    )
```

```python
import functools

import jax
import jax.numpy as jnp
import numpy as np
from jax import lax
from jax.experimental import pallas as pl
from jax.experimental.pallas import tpu as pltpu
from jax.sharding import PartitionSpec as P

HEAD_DIM = 128
TOPK = 4
BLOCK = 128


highest = lax.Precision.HIGHEST
rope_base = 10000.0
group_eps = 1e-05
square_eps = 1e-06
clamp_limit = 7.0
swish_alpha = 1.702


def rotary_angles(positions, head_dim):
    half_dim = head_dim // 2
    inverse = rope_base ** (-jnp.arange(half_dim, dtype=jnp.float32) / half_dim)
    return positions[:, None] * inverse[None, :]


def square_norm(updated, gain_row):
    factor = lax.rsqrt(jnp.mean(updated * updated, axis=-1, keepdims=True) + square_eps)
    return (updated * factor * gain_row).astype(jnp.bfloat16)


def expert_rows(rows, gate_part, up_part):
    gate_pre = jnp.dot(rows, gate_part, preferred_element_type=jnp.float32)
    up_pre = jnp.dot(rows, up_part, preferred_element_type=jnp.float32)
    gate_clip = jnp.minimum(gate_pre, clamp_limit)
    up_clip = jnp.clip(up_pre, -clamp_limit, clamp_limit)
    return ((up_clip + 1.0) * (gate_clip * jax.nn.sigmoid(gate_clip * swish_alpha))).astype(
        jnp.bfloat16
    )


def slot_ranks(route_block, experts):
    flat_routes = route_block.reshape(-1)
    onehot = (flat_routes[:, None] == jnp.arange(experts, dtype=jnp.int32)[None, :]).astype(
        jnp.int32
    )
    return (flat_routes, jnp.sum(jnp.cumsum(onehot, axis=0) * onehot, axis=1) - 1)


def retention_kernel(q_ref, k_ref, v_ref, cos_ref, sin_ref, cum_ref, cum_row_ref, ret_ref, qdec_ref, state_ref):
    head = pl.program_id(0)
    length = q_ref.shape[0]
    cosine, sine = cos_ref[...], sin_ref[...]
    half = HEAD_DIM // 2

    def turned(ref):
        rows = ref[...].astype(jnp.float32)
        return rows * cosine + pltpu.roll(rows, half, 1) * sine

    lanes = lax.broadcasted_iota(jnp.int32, cum_ref.shape, 1)
    column = jnp.sum(jnp.where(lanes == head, cum_ref[...], 0.0), axis=1, keepdims=True)
    row = cum_row_ref[0]
    queries = turned(q_ref)
    keys = turned(k_ref) * HEAD_DIM ** (-0.5)
    values = v_ref[...]
    scores = lax.dot_general(
        queries.astype(jnp.bfloat16),
        keys.astype(jnp.bfloat16),
        (((1,), (1,)), ((), ())),
        preferred_element_type=jnp.float32,
    )
    causal = lax.broadcasted_iota(jnp.int32, (length, length), 0) >= lax.broadcasted_iota(
        jnp.int32, (length, length), 1
    )
    weights = jnp.where(causal, jnp.exp(jnp.minimum(column - row, 0.0)), 0.0)
    ret_ref[...] = jnp.dot(
        (scores * weights).astype(jnp.bfloat16), values, preferred_element_type=jnp.float32
    )
    qdec_ref[...] = (queries * jnp.exp(column)).astype(jnp.bfloat16)
    total = column[length - 1 :, :]
    tailed = (keys * jnp.exp(total - column)).astype(jnp.bfloat16)
    state_ref[0, :HEAD_DIM, :] = lax.dot_general(
        tailed, values, (((0,), (0,)), ((), ())), preferred_element_type=jnp.float32
    )
    state_ref[0, HEAD_DIM:, :] = jnp.broadcast_to(total, (8, HEAD_DIM))


def norm_kernel(ret_ref, qdec_ref, enter_ref, gain_ref, gate_ref, hidden_ref):
    retained = ret_ref[...] + jnp.dot(
        qdec_ref[...], enter_ref[0].astype(jnp.bfloat16), preferred_element_type=jnp.float32
    )
    centred = retained - jnp.mean(retained, axis=-1, keepdims=True)
    variance = jnp.mean(centred * centred, axis=-1, keepdims=True)
    gate = gate_ref[...].astype(jnp.float32)
    scaled = centred * lax.rsqrt(variance + group_eps) * gain_ref[...]
    hidden_ref[...] = (scaled * (gate / (1.0 + jnp.exp(-gate)))).astype(jnp.bfloat16)


def retention(query_rows, key_rows, value_rows, gate_rows, log_decay, head_gain):
    length, local_heads = log_decay.shape
    width = query_rows.shape[1]
    sp_count, mine = lax.axis_size("sp"), lax.axis_index("sp")
    positions = (mine * length + jnp.arange(length, dtype=jnp.int32)).astype(jnp.float32)
    angles = rotary_angles(positions, HEAD_DIM)
    cosine, sine = jnp.cos(angles), jnp.sin(angles)
    cosine = jnp.concatenate([cosine, cosine], axis=1)
    sine = jnp.concatenate([-sine, sine], axis=1)
    cumulative = jnp.cumsum(log_decay, axis=0)
    rows_spec = pl.BlockSpec((length, HEAD_DIM), lambda h: (0, h))
    table_spec = pl.BlockSpec((length, HEAD_DIM), lambda h: (0, 0))
    retained, qdec, state = pl.pallas_call(
        retention_kernel,
        grid=(local_heads,),
        out_shape=(
            jax.ShapeDtypeStruct((length, width), jnp.float32),
            jax.ShapeDtypeStruct((length, width), jnp.bfloat16),
            jax.ShapeDtypeStruct((local_heads, HEAD_DIM + 8, HEAD_DIM), jnp.float32),
        ),
        in_specs=[
            rows_spec,
            rows_spec,
            rows_spec,
            table_spec,
            table_spec,
            pl.BlockSpec((length, local_heads), lambda h: (0, 0)),
            pl.BlockSpec((1, 1, length), lambda h: (h, 0, 0)),
        ],
        out_specs=(
            rows_spec,
            rows_spec,
            pl.BlockSpec((1, HEAD_DIM + 8, HEAD_DIM), lambda h: (h, 0, 0)),
        ),
    )(query_rows, key_rows, value_rows, cosine, sine, cumulative, cumulative.T[:, None, :])
    pieces = lax.all_gather(state, "sp")
    totals = pieces[:, :, HEAD_DIM, 0]
    index = jnp.arange(sp_count, dtype=jnp.int32)
    between = (index[None, :] > index[:, None]) & (index[None, :] < mine)
    gap = jnp.sum(jnp.where(between[:, :, None], totals[None], 0.0), axis=1)
    factor = jnp.where((index < mine)[:, None], jnp.exp(gap), 0.0)
    entering = jnp.sum(factor[:, :, None, None] * pieces[:, :, :HEAD_DIM, :], axis=0)
    return pl.pallas_call(
        norm_kernel,
        grid=(local_heads,),
        out_shape=jax.ShapeDtypeStruct((length, width), jnp.bfloat16),
        in_specs=[
            rows_spec,
            rows_spec,
            pl.BlockSpec((1, HEAD_DIM, HEAD_DIM), lambda h: (h, 0, 0)),
            pl.BlockSpec((1, HEAD_DIM), lambda h: (0, h)),
            rows_spec,
        ],
        out_specs=rows_spec,
    )(retained, qdec, entering, head_gain[None, :], gate_rows)


(
    UP_A, UP_B, DOWN_A, DOWN_B, X_A2, Y_B2, Y_A3, Y_A4, X_B3, X_B4, C_A, C_B, C_P, Y_A, X_B, X_A, Y_B, R_UP_A, R_UP_B,
    TOTAL, CHAIN, ACROSS, MIX_C, MIX_Y, S_X2, S_Y2, S_Y3, S_X3, S_Y4, S_X4, S_UP, S_DOWN, S_CORE,
    T_UP, T_DOWN, T_Y1, T_X1, T_X2, T_Y2, R_DOWN_A, R_DOWN_B,
) = range(41)


def layer_kernel(
    planes, logs_hbm, k_hbm, near_hbm, base_hbm, v_hbm, q_hbm, gate_hbm, gain_hbm, routes_hbm, shares_hbm,
    residual_hbm, ffn_gain_hbm, wo_hbm, wg_hbm, wu_hbm, wd_hbm, out,
    logs, k_ref, near_table, base_table, v_ref, q_ref, gate_ref, head_gain, routes, route_weights,
    residual, ffn_gain, wo, wg, wu, wd, rotary, turned_k, ret, qdec, state, cum_col, cum_row, total_own, total_x, carry_in, carry_out,
    side_out, side_in, hidden, blend, from_core, held, from_y, upd,
    share_in, g0, g1, gs, pm, pr, a0, a1, r10, r11, b0, b1, r20, r21, d0, d1, low_up, low_down, high_up, high_down,
    tot, tot_up, tot_down, home, home_in, pair, pair_in,
    ssem, rsem, wsem,
):
    sp, tp = lax.axis_index("sp"), lax.axis_index("tp")
    sp_count = 2 * planes
    z, x = sp // 2, sp % 2
    y, c = tp // 2, tp % 2
    own_rows, width = out.shape
    half = a0.shape[-1]
    wide_a, wide_b = g0.shape[-1] - 128, g1.shape[-1]
    wide_ab = wide_a + wide_b
    rows = own_rows // 2
    items = 2 * planes
    lag = items - 3
    f32, bf16 = jnp.float32, jnp.bfloat16
    to_core = {"sp": sp, "tp": y * 2 + (1 - c)}
    to_y = {"sp": sp, "tp": (1 - y) * 2 + c}
    to_x = {"sp": z * 2 + (1 - x), "tp": tp}

    def half_of(n):
        return jnp.where(n == items - 1, 1, jnp.where(n == 0, 0, (n + 1) % 2))

    def plane_at(k):
        low = z < planes // 2
        mirrored = jnp.where(low, z, planes - 1 - z)
        q = jnp.where(k <= mirrored, mirrored - k, k)
        return jnp.where(low, q, planes - 1 - q)

    def plane_of(n):
        return plane_at(((n + 1) // 2) % planes)

    def item_of(n):
        return 2 * plane_of(n) + half_of(n)

    def step_of(turn):
        back = items - 3 - 2 * ((turn - 2) // 2) + turn % 2
        kept = (turn <= 1) | (turn == items - 1)
        return jnp.where(kept, turn, jnp.where(turn == items - 2, 2, back))

    def has_turn(u):
        return (u >= 0) & (u < items)

    def at_plane(p):
        return {"sp": p * 2 + x, "tp": tp}

    def to_z(i):
        return at_plane((z + planes - i) % planes)

    def move(kind, n, src, dst, device, m=None):
        return pltpu.make_async_remote_copy(
            src_ref=src, dst_ref=dst, send_sem=ssem.at[kind, n],
            recv_sem=rsem.at[kind, n if m is None else m],
            device_id=device, device_id_type=pl.DeviceIdType.MESH,
        )

    def send(kind, n, src, dst, device, m=None):
        move(kind, n, src, dst, device, m).start()

    def arrived(kind, n, dst):
        move(kind, n, dst, dst, to_core).wait_recv()

    def left(kind, n, src):
        move(kind, n, src, src, to_core).wait_send()

    loads = [
        pltpu.make_async_copy(far, near, wsem.at[i])
        for i, (far, near) in enumerate(
            [
                (logs_hbm, logs), (k_hbm, k_ref), (near_hbm, near_table), (base_hbm, base_table), (v_hbm, v_ref),
                (q_hbm, q_ref), (gate_hbm, gate_ref), (gain_hbm, head_gain), (routes_hbm, routes),
                (shares_hbm, route_weights), (residual_hbm, residual), (ffn_gain_hbm, ffn_gain),
                (wo_hbm, wo), (wg_hbm, wg), (wu_hbm, wu), (wd_hbm, wd),
            ]
        )
    ]
    for copy in loads:
        copy.start()
    barrier = pltpu.get_barrier_semaphore()
    for device in [to_core, to_y, to_x] + [to_z(i) for i in range(1, planes)]:
        pl.semaphore_signal(barrier, inc=1, device_id=device, device_id_type=pl.DeviceIdType.MESH)

    length = q_ref.shape[0]
    dim = HEAD_DIM
    heads = q_ref.shape[1] // dim
    depth = state.shape[1]
    cuts = dim // depth
    after = lax.broadcasted_iota(jnp.int32, (length, length), 0) >= lax.broadcasted_iota(
        jnp.int32, (length, length), 1
    )
    ones = jnp.where(after, 1.0, 0.0).astype(f32)
    loads[0].wait()
    log_rows = jnp.concatenate([logs[...], jnp.zeros((8 - heads, length), f32)], axis=0)
    cum_row[...] = lax.dot_general(
        log_rows, ones, (((1,), (1,)), ((), ())), precision=highest, preferred_element_type=f32
    )
    cum_col[...] = lax.dot_general(
        ones, log_rows, (((1,), (1,)), ((), ())), precision=highest, preferred_element_type=f32
    )
    total_own[...] = jnp.broadcast_to(cum_row[:, length - 1 :], (8, dim))
    pl.semaphore_wait(barrier, 2 + planes)
    send(TOTAL, 0, total_own, total_x, to_x)

    loads[2].wait()
    loads[3].wait()
    base = base_table[pl.ds(sp * 8, 8), :]
    cosine = base[0:1] * near_table[0] - base[1:2] * near_table[1]
    sine = base[2:3] * near_table[0] + base[3:4] * near_table[1]
    rotary[0] = cosine
    rotary[1] = sine

    def turned(rows_in):
        wide = rows_in.astype(f32)
        return wide * rotary[0] + pltpu.roll(wide, dim // 2, 1) * rotary[1]

    def column_of(h):
        lanes = lax.broadcasted_iota(jnp.int32, cum_col.shape, 1)
        return jnp.sum(jnp.where(lanes == h, cum_col[...], 0.0), axis=1, keepdims=True)

    left_side = x == 0

    def pass_state(e):
        h = e // cuts
        own_total, x_total = total_own[h : h + 1, :], total_x[h : h + 1, :]
        before = carry_in[e].astype(f32)

        @pl.when(z + 1 < planes)
        def _():
            fresh = jnp.where(left_side, jnp.exp(x_total), 1.0) * state[e]
            carry_out[e] = (jnp.exp(own_total + x_total) * before + fresh).astype(bf16)
            send(CHAIN, e, carry_out.at[e], carry_in.at[e], at_plane(z + 1))

        side_out[e] = jnp.where(left_side, jnp.exp(own_total) * before + state[e], before).astype(bf16)
        send(ACROSS, e, side_out.at[e], side_in.at[e], to_x)

    @pl.when(z == 0)
    def _():
        carry_in[...] = jnp.zeros_like(carry_in)
        for r in range(2):
            for ref in (tot_up, low_up, high_up):
                ref[r] = jnp.zeros_like(ref[r])

    @pl.when(z == planes - 1)
    def _():
        for r in range(2):
            for ref in (tot_down, low_down, high_down):
                ref[2 * planes - 2 + r] = jnp.zeros_like(ref[r])

    loads[1].wait()
    loads[4].wait()
    for h in range(heads):
        lanes = pl.ds(h * dim, dim)
        keys = turned(k_ref[:, lanes]) * dim ** (-0.5)
        turned_k[:, lanes] = keys.astype(bf16)
        column = column_of(h)
        tailed = (keys * jnp.exp(column[length - 1 :, :] - column)).astype(bf16)
        state[cuts * h : cuts * (h + 1)] = lax.dot_general(
            tailed, v_ref[:, lanes], (((0,), (0,)), ((), ())), preferred_element_type=f32
        ).reshape(cuts, depth, dim)

        @pl.when(z == 0)
        def _():
            if h == 0:
                arrived(TOTAL, 0, total_x)
            for e in range(cuts * h, cuts * (h + 1)):
                pass_state(e)

    def attend(h, carry):
        lanes = pl.ds(pl.multiple_of(h * dim, dim), dim)
        queries = turned(q_ref[:, lanes])
        column = column_of(h)
        scores = lax.dot_general(
            queries.astype(bf16), turned_k[:, lanes], (((1,), (1,)), ((), ())), preferred_element_type=f32
        )
        gap = jnp.minimum(column - cum_row[pl.ds(h, 1), :], 0.0)
        decays = jnp.where(after, jnp.exp(gap), 0.0)
        ret[:, lanes] = jnp.dot((scores * decays).astype(bf16), v_ref[:, lanes], preferred_element_type=f32)
        qdec[:, lanes] = (queries * jnp.exp(column)).astype(bf16)
        return carry

    early = jnp.where(z >= planes // 2, heads, 0)
    loads[5].wait()
    lax.fori_loop(0, early, attend, 0)

    @pl.when(z > 0)
    def _():
        arrived(TOTAL, 0, total_x)

    for e in range(cuts * heads):

        @pl.when(z > 0)
        def _():
            arrived(CHAIN, e, carry_in.at[e])
            pass_state(e)

    lax.fori_loop(early, heads, attend, 0)

    for h in range(heads):
        lanes = pl.ds(h * dim, dim)
        if h == 0:
            loads[6].wait()
            loads[7].wait()
        blocks = slice(cuts * h, cuts * (h + 1))
        for e in range(cuts * h, cuts * (h + 1)):
            arrived(ACROSS, e, side_in.at[e])
        factor = jnp.where(left_side, 1.0, jnp.exp(total_x[h : h + 1, :]))
        before = carry_in[blocks].reshape(dim, dim).astype(f32)
        entering = (factor * before + side_in[blocks].reshape(dim, dim).astype(f32)).astype(bf16)
        retained = ret[:, lanes] + jnp.dot(qdec[:, lanes], entering, preferred_element_type=f32)
        centred = retained - jnp.mean(retained, axis=-1, keepdims=True)
        variance = jnp.mean(centred * centred, axis=-1, keepdims=True)
        gate_in = gate_ref[:, lanes].astype(f32)
        scaled = centred * lax.rsqrt(variance + group_eps) * head_gain[:, lanes]
        made = (scaled * (gate_in / (1.0 + jnp.exp(-gate_in)))).astype(bf16)
        hidden[:, :, lanes] = made.reshape(4, own_rows, dim)

    loads[12].wait()
    pieces = blend.shape[0]
    spans = pieces // 2
    span = width // spans

    def cross(j):
        arrived(MIX_C, j, from_core.at[j])
        held[j] = (blend[j, c, 1 - y].astype(f32) + from_core[j, 1 - y].astype(f32)).astype(bf16)
        send(MIX_Y, j, held.at[j], from_y.at[j], to_y)

    for j in range(pieces):
        picked = hidden[:, j // spans * rows : (j // spans + 1) * rows, :].reshape(4 * rows, heads * dim)
        mixed = jnp.dot(picked, wo[:, pl.ds(j % spans * span, span)], preferred_element_type=f32).astype(bf16)
        for q in range(4):
            blend[j, q % 2, q // 2] = mixed[q * rows : (q + 1) * rows, :]
        send(MIX_C, j, blend.at[j, 1 - c], from_core.at[j], to_core)
        if j > 0:
            cross(j - 1)
    cross(pieces - 1)

    here = x * 2 + y
    other_x = (1 - x) * 2 + y
    other_y = x * 2 + (1 - y)
    other_xy = (1 - x) * 2 + (1 - y)
    for copy in loads[8:12]:
        copy.wait()
    count = routes.shape[0]
    share_in[...] = jnp.zeros_like(share_in)
    share_in[:count, :own_rows] = route_weights[...]
    all_routes = jnp.concatenate([routes[...]] * (8 // count), axis=0)
    own_routes = jnp.zeros((8, 128), jnp.int32)
    for q in range(4):
        turned_routes = pltpu.roll(all_routes, (length - q * own_rows) % length, 1)
        own_routes = own_routes + jnp.where(tp == q, turned_routes[:, :128], 0)
    expert = lax.broadcasted_iota(jnp.int32, (128, 128), 0)
    shares = jnp.zeros((128, 128), f32)
    for k in range(count):
        shares = shares + jnp.where(own_routes[k : k + 1, :] == expert, share_in[k : k + 1, :], 0.0)
    share = jnp.transpose(shares)[:own_rows, :]
    coarse = share.astype(bf16).astype(f32)
    tail_rows = (coarse + pltpu.roll(share - coarse, sp_count, 1)).astype(bf16)
    first_rows, last_rows = pl.ds(0, rows), pl.ds(rows, rows)
    def side(p, chip, part):
        return gs.at[c, p, chip, part]

    def pass_side(kind, n, chip, part, device):
        send(kind, n, side(z, chip, part), side(z, chip, part), device)

    def spread_side(r):
        if r == 0:
            pass_side(S_X2, 0, here, first_rows, to_x)
            pass_side(S_Y3, 0, here, first_rows, to_y)
        else:
            pass_side(S_Y2, 0, here, last_rows, to_y)
            pass_side(S_X3, 0, here, last_rows, to_x)

    def relay_side():
        arrived(S_X2, 0, side(z, other_x, first_rows))
        pass_side(S_Y4, 0, other_x, first_rows, to_y)
        arrived(S_Y2, 0, side(z, other_y, last_rows))
        pass_side(S_X4, 0, other_y, last_rows, to_x)

    def side_up(p):
        @pl.when(z + 1 < planes)
        def _():
            send(S_UP, p, gs.at[c, p], gs.at[c, p], at_plane(z + 1))

    def side_down(p):
        @pl.when(z > 0)
        def _():
            send(S_DOWN, p, gs.at[c, p], gs.at[c, p], at_plane(z - 1))

    def side_core(p):
        send(S_CORE, p, gs.at[c, p], gs.at[c, p], to_core)

    def close_side():
        arrived(S_Y3, 0, side(z, other_y, first_rows))
        arrived(S_Y4, 0, side(z, other_xy, first_rows))
        arrived(S_X3, 0, side(z, other_x, last_rows))
        arrived(S_X4, 0, side(z, other_xy, last_rows))
        side_up(z)
        side_down(z)
        side_core(z)

    def spread(n):
        send(X_A2, n, g0.at[c, n, here], g0.at[c, n, here], to_x)
        send(Y_B2, n, g1.at[c, n, here], g1.at[c, n, here], to_y)
        send(Y_A3, n, g0.at[c, n, here], g0.at[c, n, here], to_y)
        send(X_B3, n, g1.at[c, n, here], g1.at[c, n, here], to_x)

    def raise_up(n):
        @pl.when(z + 1 < planes)
        def _():
            send(UP_A, n, g0.at[c, n, here], g0.at[c, n, here], at_plane(z + 1))
            send(UP_B, n, g1.at[c, n, here], g1.at[c, n, here], at_plane(z + 1))

    def hand_down(n):
        @pl.when(z > 0)
        def _():
            send(DOWN_A, n, g0.at[c, n, here], g0.at[c, n, here], at_plane(z - 1))
            send(DOWN_B, n, g1.at[c, n, here], g1.at[c, n, here], at_plane(z - 1))

    for r in range(2):
        mine, n = slice(r * rows, (r + 1) * rows), 2 * z + r
        square = jnp.zeros((rows, 1), f32)
        for j in range(r * spans, (r + 1) * spans):
            cols = pl.ds(j % spans * span, span)
            near = residual[mine, cols].astype(f32) + blend[j, c, y].astype(f32) + from_core[j, y].astype(f32)
            arrived(MIX_Y, j, from_y.at[j])
            total = near + from_y[j].astype(f32)
            upd[mine, cols] = total
            square = square + jnp.sum(total * total, axis=-1, keepdims=True)
        scale = lax.rsqrt(square * (1.0 / width) + square_eps)
        ready = (upd[mine, :] * scale * ffn_gain[...]).astype(bf16)
        g0[c, n, here, :, :wide_a] = ready[:, :wide_a]
        g0[c, n, here, :, wide_a:] = tail_rows[mine]
        g1[c, n, here] = ready[:, wide_a:wide_ab]
        gs[c, z, here, mine, :] = ready[:, wide_ab:]
        raise_up(n)
        hand_down(n)
        spread_side(r)
        if r == 0:
            spread(n)

    last_chains = [(T_UP, T_DOWN, tot, tot_up, tot_down)]
    main_chains = [(R_UP_A, R_DOWN_A, d0, low_up, low_down), (R_UP_B, R_DOWN_B, d1, high_up, high_down)]

    def start_chain(n, chains):
        @pl.when((n // 2 > z) & (z == 0))
        def _():
            for up, _, acc, got_up, _ in chains:
                send(up, n, acc.at[n], got_up.at[n], at_plane(z + 1))

        @pl.when((n // 2 < z) & (z == planes - 1))
        def _():
            for _, down, acc, _, got_down in chains:
                send(down, n, acc.at[n], got_down.at[n], at_plane(z - 1))

    def go_on(turn, chains):
        n = item_of(step_of(turn))

        @pl.when((n // 2 > z) & (z > 0))
        def _():
            for up, _, acc, got_up, _ in chains:
                arrived(up, n, got_up.at[n])
                acc[n] = (acc[n].astype(f32) + got_up[n].astype(f32)).astype(bf16)
                send(up, n, acc.at[n], got_up.at[n], at_plane(z + 1))

        @pl.when((n // 2 < z) & (z < planes - 1))
        def _():
            for _, down, acc, _, got_down in chains:
                arrived(down, n, got_down.at[n])
                acc[n] = (acc[n].astype(f32) + got_down[n].astype(f32)).astype(bf16)
                send(down, n, acc.at[n], got_down.at[n], at_plane(z - 1))

    def tick(t, carry):
        def relay():
            n = item_of(t)
            arrived(X_A2, n, g0.at[c, n, other_x])
            send(Y_A4, n, g0.at[c, n, other_x], g0.at[c, n, other_x], to_y)
            arrived(Y_B2, n, g1.at[c, n, other_y])
            send(X_B4, n, g1.at[c, n, other_y], g1.at[c, n, other_y], to_x)

        pl.when(t == 0)(relay_side)
        pl.when(t == 0)(relay)
        pl.when(t == 1)(close_side)

        @pl.when(t + 1 < items)
        def _():
            k, r = (t + 2) // 2, t % 2

            @pl.when((t + 1 < items - 1) & (z - k >= 0))
            def _():
                n = 2 * (z - k) + r
                arrived(UP_A, n, g0.at[c, n, here])
                arrived(UP_B, n, g1.at[c, n, here])
                raise_up(n)

            @pl.when((t + 1 < items - 1) & (z + k < planes))
            def _():
                n = 2 * (z + k) + r
                arrived(DOWN_A, n, g0.at[c, n, here])
                arrived(DOWN_B, n, g1.at[c, n, here])
                hand_down(n)

            spread(item_of(t + 1))

        pl.when((t > 0) & (t < items))(relay)

        @pl.when((t >= 2) & (t < items) & (t % 2 == 0))
        def _():
            below, above = z - t // 2, z + t // 2

            @pl.when(below >= 0)
            def _():
                arrived(S_UP, below, gs.at[c, below])
                side_up(below)
                side_core(below)

            @pl.when(above < planes)
            def _():
                arrived(S_DOWN, above, gs.at[c, above])
                side_down(above)
                side_core(above)

        @pl.when(t == 2)
        def _():
            for copy in loads[13:]:
                copy.wait()

        @pl.when((t >= 2) & (t < items + 2))
        def _():
            n = item_of(t - 2)
            arrived(C_A, n, g0.at[1 - c, n])
            arrived(C_B, n, g1.at[1 - c, n])
            p, r = plane_of(t - 2), half_of(t - 2)

            @pl.when(r == 0)
            def _():
                arrived(S_CORE, p, gs.at[1 - c, p])

            lead = g0[:, n].reshape(8 * rows, wide_a + 128)
            tail = lead[:, wide_a:].astype(f32)
            rest = g1[:, n].reshape(8 * rows, wide_b)
            last = gs[:, p, :, pl.ds(pl.multiple_of(r * rows, rows), rows), :].reshape(8 * rows, width - wide_ab)
            rows_in = jnp.concatenate([lead[:, :wide_a], rest, last], axis=1)
            lane = lax.broadcasted_iota(jnp.int32, tail.shape, 1)
            weight = jnp.sum(
                jnp.where((lane == sp) | (lane == sp + sp_count), tail, 0.0), axis=1, keepdims=True
            )

            def product(w):
                return jnp.dot(rows_in, w[...], preferred_element_type=f32)

            gate = jnp.minimum(product(wg), clamp_limit)
            up = jnp.clip(product(wu), -clamp_limit, clamp_limit)
            act = ((up + 1.0) * (gate / (1.0 + jnp.exp(-swish_alpha * gate)))).astype(bf16)
            made = (jnp.dot(act, wd[...], preferred_element_type=f32) * weight).astype(bf16)
            pm[n] = made.reshape(2, 4 * rows, width)
            send(C_P, n, pm.at[n, 1 - c], pr.at[n], to_core)

        @pl.when((t >= 1) & (t < items + 1))
        def _():
            n = item_of(t - 1)
            arrived(Y_A3, n, g0.at[c, n, other_y])
            arrived(Y_A4, n, g0.at[c, n, other_xy])
            arrived(X_B3, n, g1.at[c, n, other_x])
            arrived(X_B4, n, g1.at[c, n, other_xy])
            send(C_A, n, g0.at[c, n], g0.at[c, n], to_core)
            send(C_B, n, g1.at[c, n], g1.at[c, n], to_core)

        @pl.when(has_turn(t - lag))
        def _():
            n = item_of(step_of(t - lag))
            arrived(C_P, n, pr.at[n])
            for q in range(4):
                part = pl.ds(q * rows, rows)
                total = (pm[n, c, part, :].astype(f32) + pr[n, part, :].astype(f32)).astype(bf16)
                a0[n, q % 2, q // 2] = total[:, :half]
                a1[n, q // 2, q % 2] = total[:, half : 2 * half]
                tot[n, q] = total[:, 2 * half :]
            send(Y_A, n, a0.at[n, 1 - y], r10.at[n], to_y)
            send(X_B, n, a1.at[n, 1 - x], r11.at[n], to_x)
            start_chain(n, last_chains)

        @pl.when(has_turn(t - lag - 1))
        def _():
            n = item_of(step_of(t - lag - 1))
            arrived(Y_A, n, r10.at[n])
            b0[n] = (a0[n, y].astype(f32) + r10[n].astype(f32)).astype(bf16)
            send(X_A, n, b0.at[n, 1 - x], r20.at[n], to_x)
            arrived(X_B, n, r11.at[n])
            b1[n] = (a1[n, x].astype(f32) + r11[n].astype(f32)).astype(bf16)
            send(Y_B, n, b1.at[n, 1 - y], r21.at[n], to_y)

        @pl.when(has_turn(t - lag - 2))
        def _():
            n = item_of(step_of(t - lag - 2))
            arrived(X_A, n, r20.at[n])
            d0[n] = (b0[n, x].astype(f32) + r20[n].astype(f32)).astype(bf16)
            arrived(Y_B, n, r21.at[n])
            d1[n] = (b1[n, y].astype(f32) + r21[n].astype(f32)).astype(bf16)
            start_chain(n, main_chains)

        u = t - lag

        @pl.when((u >= 3) & (u <= items - 2))
        def _():
            go_on(u - 1, last_chains)

        @pl.when(u == items - 2)
        def _():
            go_on(1, last_chains)
            go_on(items - 2, last_chains)

        @pl.when((u >= 5) & (u <= items))
        def _():
            go_on(u - 3, main_chains)

        @pl.when(u == items)
        def _():
            go_on(1, main_chains)
            go_on(items - 2, main_chains)

        @pl.when(u == items - 1)
        def _():
            for r in range(2):
                n = 2 * z + r

                @pl.when(z > 0)
                def _():
                    arrived(T_UP, n, tot_up.at[n])

                @pl.when(z < planes - 1)
                def _():
                    arrived(T_DOWN, n, tot_down.at[n])

                for q in range(4):
                    total = tot[n, q].astype(f32) + tot_up[n, q].astype(f32) + tot_down[n, q].astype(f32)
                    place = (q % 2, q // 2) if r == 0 else (q // 2, q % 2)
                    home[r, place[0], place[1]] = total.astype(bf16)
            send(T_Y1, 0, home.at[0, 1 - y], home_in.at[0], to_y)
            send(T_X1, 0, home.at[1, 1 - x], home_in.at[1], to_x)

        @pl.when(u == items)
        def _():
            arrived(T_Y1, 0, home_in.at[0])
            pair[0] = (home[0, y].astype(f32) + home_in[0].astype(f32)).astype(bf16)
            send(T_X2, 0, pair.at[0, 1 - x], pair_in.at[0], to_x)
            arrived(T_X1, 0, home_in.at[1])
            pair[1] = (home[1, x].astype(f32) + home_in[1].astype(f32)).astype(bf16)
            send(T_Y2, 0, pair.at[1, 1 - y], pair_in.at[1], to_y)

        return carry

    lax.fori_loop(0, items + lag + 2, tick, 0)
    arrived(T_X2, 0, pair_in.at[0])
    arrived(T_Y2, 0, pair_in.at[1])
    for r in range(2):
        n, part = 2 * z + r, pl.ds(r * rows, rows)
        low = upd[part, :half] + d0[n].astype(f32)
        high = upd[part, half : 2 * half] + d1[n].astype(f32)

        @pl.when(z > 0)
        def _():
            arrived(R_UP_A, n, low_up.at[n])
            arrived(R_UP_B, n, high_up.at[n])

        @pl.when(z < planes - 1)
        def _():
            arrived(R_DOWN_A, n, low_down.at[n])
            arrived(R_DOWN_B, n, high_down.at[n])

        low = low + low_up[n].astype(f32) + low_down[n].astype(f32)
        high = high + high_up[n].astype(f32) + high_down[n].astype(f32)
        out[part, :half] = low.astype(bf16)
        out[part, half : 2 * half] = high.astype(bf16)
        kept = pair[0, x] if r == 0 else pair[1, y]
        out[part, 2 * half :] = (
            upd[part, 2 * half :] + kept.astype(f32) + pair_in[r].astype(f32)
        ).astype(bf16)

    left(T_Y1, 0, home.at[0, 1 - y])
    left(T_X1, 0, home.at[1, 1 - x])
    left(T_X2, 0, pair.at[0, 1 - x])
    left(T_Y2, 0, pair.at[1, 1 - y])

    def drain(n, carry):
        p = n // 2

        @pl.when(p > z)
        def _():
            for up, _, acc, _, _ in last_chains + main_chains:
                left(up, n, acc.at[n])

        @pl.when(p < z)
        def _():
            for _, down, acc, _, _ in last_chains + main_chains:
                left(down, n, acc.at[n])

        @pl.when((p <= z) & (z + 1 < planes))
        def _():
            left(UP_A, n, g0.at[c, n, here])
            left(UP_B, n, g1.at[c, n, here])

        @pl.when((p >= z) & (z > 0))
        def _():
            left(DOWN_A, n, g0.at[c, n, here])
            left(DOWN_B, n, g1.at[c, n, here])

        left(X_A2, n, g0.at[c, n, here])
        left(Y_B2, n, g1.at[c, n, here])
        left(Y_A3, n, g0.at[c, n, here])
        left(X_B3, n, g1.at[c, n, here])
        left(Y_A4, n, g0.at[c, n, other_x])
        left(X_B4, n, g1.at[c, n, other_y])
        left(C_A, n, g0.at[c, n])
        left(C_B, n, g1.at[c, n])
        left(C_P, n, pm.at[n, 1 - c])
        left(Y_A, n, a0.at[n, 1 - y])
        left(X_B, n, a1.at[n, 1 - x])
        left(X_A, n, b0.at[n, 1 - x])
        left(Y_B, n, b1.at[n, 1 - y])
        return carry

    lax.fori_loop(0, items, drain, 0)
    left(S_X2, 0, side(z, here, first_rows))
    left(S_Y2, 0, side(z, here, last_rows))
    left(S_Y3, 0, side(z, here, first_rows))
    left(S_X3, 0, side(z, here, last_rows))
    left(S_Y4, 0, side(z, other_x, first_rows))
    left(S_X4, 0, side(z, other_y, last_rows))

    def drain_side(p, carry):
        @pl.when((p <= z) & (z + 1 < planes))
        def _():
            left(S_UP, p, gs.at[c, p])

        @pl.when((p >= z) & (z > 0))
        def _():
            left(S_DOWN, p, gs.at[c, p])

        left(S_CORE, p, gs.at[c, p])
        return carry

    lax.fori_loop(0, planes, drain_side, 0)
    left(TOTAL, 0, total_own)
    for e in range(cuts * heads):
        left(ACROSS, e, side_out.at[e])

        @pl.when(z + 1 < planes)
        def _():
            left(CHAIN, e, carry_out.at[e])

    for j in range(pieces):
        left(MIX_C, j, blend.at[j, 1 - c])
        left(MIX_Y, j, held.at[j])


def rope_tables(length, spans):
    half_dim = HEAD_DIM // 2
    rates = rope_base ** (-np.arange(half_dim, dtype=np.float64) / half_dim)
    rates = np.concatenate([rates, rates])[None, :]
    near = np.arange(length, dtype=np.float64)[:, None] * rates
    starts = (np.arange(spans, dtype=np.float64) * length)[:, None] * rates
    sign = np.concatenate([-np.ones(half_dim), np.ones(half_dim)])[None, :]
    base = np.zeros((spans, 8, HEAD_DIM))
    base[:, 0], base[:, 1] = np.cos(starts), np.sin(starts)
    base[:, 2], base[:, 3] = sign * np.sin(starts), sign * np.cos(starts)
    near_table = np.stack([np.cos(near), np.sin(near)]).astype(np.float32)
    return jnp.asarray(near_table), jnp.asarray(base.reshape(spans * 8, HEAD_DIM).astype(np.float32))


def fused_layer(
    query_rows, key_rows, value_rows, gate_rows, log_decay, head_gain, out_weight, residual, ffn_gain,
    gate_part, up_part, down_part, routes, route_weights,
):
    sp_count = lax.axis_size("sp")
    length, heads = log_decay.shape
    rows_all, width = residual.shape
    inner = query_rows.shape[1]
    near_table, base_table = rope_tables(length, sp_count)
    wide_t = 128 * (width // 1024)
    half = (width - wide_t) // 2
    planes = sp_count // 2
    items = 2 * planes
    rows = rows_all // 2
    pieces = 8
    span = 2 * width // pieces
    wide_s = 128 * (3 * width // 2048)
    wide_a = (width - wide_s - 128) // 256 * 128
    wide_b = width - wide_s - wide_a
    bf16, f32 = jnp.bfloat16, jnp.float32
    whole = pl.BlockSpec(memory_space=pltpu.VMEM)
    far = pl.BlockSpec(memory_space=pltpu.HBM)
    operands = (
        log_decay.T, key_rows, near_table, base_table, value_rows, query_rows, gate_rows, head_gain[None, :],
        routes.T, route_weights.T, residual, ffn_gain[None, :], out_weight, gate_part, up_part, down_part,
    )
    square = (2 * heads, HEAD_DIM // 2, HEAD_DIM)
    return pl.pallas_call(
        functools.partial(layer_kernel, planes),
        out_shape=jax.ShapeDtypeStruct((rows_all, width), bf16),
        in_specs=[far] * len(operands),
        out_specs=whole,
        scratch_shapes=[
            *[pltpu.VMEM(operand.shape, operand.dtype) for operand in operands],
            pltpu.VMEM((2, length, HEAD_DIM), f32),
            pltpu.VMEM((length, inner), bf16),
            pltpu.VMEM((length, inner), f32),
            pltpu.VMEM((length, inner), bf16),
            pltpu.VMEM(square, f32),
            pltpu.VMEM((length, 8), f32),
            pltpu.VMEM((8, length), f32),
            pltpu.VMEM((8, HEAD_DIM), f32),
            pltpu.VMEM((8, HEAD_DIM), f32),
            pltpu.VMEM(square, bf16),
            pltpu.VMEM(square, bf16),
            pltpu.VMEM(square, bf16),
            pltpu.VMEM(square, bf16),
            pltpu.VMEM((4, rows_all, inner), bf16),
            pltpu.VMEM((pieces, 2, 2, rows, span), bf16),
            pltpu.VMEM((pieces, 2, rows, span), bf16),
            pltpu.VMEM((pieces, rows, span), bf16),
            pltpu.VMEM((pieces, rows, span), bf16),
            pltpu.VMEM((rows_all, width), f32),
            pltpu.VMEM((8, 128), f32),
            pltpu.VMEM((2, items, 4, rows, wide_a + 128), bf16),
            pltpu.VMEM((2, items, 4, rows, wide_b), bf16),
            pltpu.VMEM((2, planes, 4, rows_all, wide_s), bf16),
            pltpu.VMEM((items, 2, 4 * rows, width), bf16),
            pltpu.VMEM((items, 4 * rows, width), bf16),
            pltpu.VMEM((items, 2, 2, rows, half), bf16),
            pltpu.VMEM((items, 2, 2, rows, half), bf16),
            pltpu.VMEM((items, 2, rows, half), bf16),
            pltpu.VMEM((items, 2, rows, half), bf16),
            pltpu.VMEM((items, 2, rows, half), bf16),
            pltpu.VMEM((items, 2, rows, half), bf16),
            pltpu.VMEM((items, rows, half), bf16),
            pltpu.VMEM((items, rows, half), bf16),
            pltpu.VMEM((items, rows, half), bf16),
            pltpu.VMEM((items, rows, half), bf16),
            pltpu.VMEM((items, rows, half), bf16),
            pltpu.VMEM((items, rows, half), bf16),
            pltpu.VMEM((items, rows, half), bf16),
            pltpu.VMEM((items, rows, half), bf16),
            pltpu.VMEM((items, 4, rows, wide_t), bf16),
            pltpu.VMEM((items, 4, rows, wide_t), bf16),
            pltpu.VMEM((items, 4, rows, wide_t), bf16),
            pltpu.VMEM((2, 2, 2, rows, wide_t), bf16),
            pltpu.VMEM((2, 2, rows, wide_t), bf16),
            pltpu.VMEM((2, 2, rows, wide_t), bf16),
            pltpu.VMEM((2, rows, wide_t), bf16),
            pltpu.SemaphoreType.DMA((41, max(items, 2 * heads, pieces))),
            pltpu.SemaphoreType.DMA((41, max(items, 2 * heads, pieces))),
            pltpu.SemaphoreType.DMA((len(operands),)),
        ],
        compiler_params=pltpu.CompilerParams(
            collective_id=0, has_side_effects=True, vmem_limit_bytes=63 * 1024 * 1024
        ),
    )(*operands)


def body(
    query_rows,
    key_rows,
    value_rows,
    gate_rows,
    log_decay,
    head_gain,
    out_weight,
    residual,
    ffn_gain,
    gate_weight,
    up_weight,
    down_weight,
    routes,
    route_weights,
):
    tok_count = query_rows.shape[0]
    local_heads = log_decay.shape[1]
    sp_count = lax.axis_size("sp")
    tp_count = lax.axis_size("tp")
    model_width = residual.shape[1]
    rows_own = tok_count // tp_count
    capacity = max(2, 3 * rows_own * TOPK // (2 * sp_count))
    tp_index = lax.axis_index("tp")
    if (
        tp_count == 4 and sp_count % 2 == 0 and sp_count <= 16 and local_heads <= 8
        and rows_own <= 128 and rows_own < 2 * capacity and model_width % 2048 == 0
    ):
        return fused_layer(
            query_rows, key_rows, value_rows, gate_rows, log_decay, head_gain, out_weight, residual, ffn_gain,
            gate_weight[0], up_weight[0], down_weight[0], routes, route_weights,
        )
    own_routes = lax.dynamic_slice_in_dim(routes, tp_index * rows_own, rows_own, 0)
    hidden = retention(query_rows, key_rows, value_rows, gate_rows, log_decay, head_gain)
    mixed = jnp.dot(hidden, out_weight, preferred_element_type=jnp.float32).astype(jnp.bfloat16)
    mixed_sum = lax.psum_scatter(mixed, "tp", scatter_dimension=0, tiled=True).astype(jnp.float32)
    updated = residual.astype(jnp.float32) + mixed_sum
    ffn_in = square_norm(updated, ffn_gain)
    own_experts, own_ranks = slot_ranks(own_routes, sp_count)
    home_slot = own_experts * capacity + own_ranks
    gate_part = gate_weight[0]
    up_part = up_weight[0]
    down_part = down_weight[0]
    empty_row = jnp.zeros((1, model_width), jnp.bfloat16)
    source_row = (
        jnp.full((sp_count * capacity,), rows_own, jnp.int32)
        .at[home_slot]
        .set(jnp.arange(rows_own * TOPK, dtype=jnp.int32) // TOPK)
    )
    padded = jnp.concatenate([ffn_in, empty_row], axis=0)
    outgoing = padded[source_row].reshape(sp_count, capacity, model_width)
    arrived = lax.all_to_all(outgoing, "sp", split_axis=0, concat_axis=0, tiled=True)
    fanned = lax.all_gather(arrived[None], "tp", axis=0, tiled=True)
    activity = expert_rows(fanned.reshape(-1, model_width), gate_part, up_part)
    partial_out = jnp.dot(activity, down_part, preferred_element_type=jnp.float32).reshape(
        tp_count, sp_count, capacity, model_width
    )
    summed = (
        lax.psum_scatter(partial_out.astype(jnp.bfloat16), "tp", scatter_dimension=0, tiled=True)
        .astype(jnp.float32)
        .reshape(sp_count, capacity, model_width)
    )
    returned = lax.all_to_all(
        summed.astype(jnp.bfloat16), "sp", split_axis=0, concat_axis=0, tiled=True
    )
    picked = returned.reshape(sp_count * capacity, model_width)[home_slot].reshape(
        rows_own, TOPK, model_width
    )
    expert_sum = jnp.sum(route_weights[:, :, None] * picked.astype(jnp.float32), axis=1)
    return (updated + expert_sum).astype(jnp.bfloat16)


def solution(mesh):
    return jax.shard_map(
        body,
        mesh=mesh,
        in_specs=(
            P("sp", "tp"),
            P("sp", "tp"),
            P("sp", "tp"),
            P("sp", "tp"),
            P("sp", "tp"),
            P("tp"),
            P("tp", None),
            P(("sp", "tp"), None),
            P(),
            P("sp", None, "tp"),
            P("sp", None, "tp"),
            P("sp", "tp", None),
            P("sp", None),
            P(("sp", "tp"), None),
        ),
        out_specs=P(("sp", "tp"), None),
        check_vma=False,
    )
```

```python
import functools

import jax
import jax.numpy as jnp
import numpy as np
from jax import lax
from jax.experimental import pallas as pl
from jax.experimental.pallas import tpu as pltpu
from jax.sharding import PartitionSpec as P

HEAD_DIM = 128
TOPK = 4
BLOCK = 128


highest = lax.Precision.HIGHEST
rope_base = 10000.0
group_eps = 1e-05
square_eps = 1e-06
clamp_limit = 7.0
swish_alpha = 1.702


def rotary_angles(positions, head_dim):
    half_dim = head_dim // 2
    inverse = rope_base ** (-jnp.arange(half_dim, dtype=jnp.float32) / half_dim)
    return positions[:, None] * inverse[None, :]


def square_norm(updated, gain_row):
    factor = lax.rsqrt(jnp.mean(updated * updated, axis=-1, keepdims=True) + square_eps)
    return (updated * factor * gain_row).astype(jnp.bfloat16)


def expert_rows(rows, gate_part, up_part):
    gate_pre = jnp.dot(rows, gate_part, preferred_element_type=jnp.float32)
    up_pre = jnp.dot(rows, up_part, preferred_element_type=jnp.float32)
    gate_clip = jnp.minimum(gate_pre, clamp_limit)
    up_clip = jnp.clip(up_pre, -clamp_limit, clamp_limit)
    return ((up_clip + 1.0) * (gate_clip * jax.nn.sigmoid(gate_clip * swish_alpha))).astype(
        jnp.bfloat16
    )


def slot_ranks(route_block, experts):
    flat_routes = route_block.reshape(-1)
    onehot = (flat_routes[:, None] == jnp.arange(experts, dtype=jnp.int32)[None, :]).astype(
        jnp.int32
    )
    return (flat_routes, jnp.sum(jnp.cumsum(onehot, axis=0) * onehot, axis=1) - 1)


def retention_kernel(q_ref, k_ref, v_ref, cos_ref, sin_ref, cum_ref, cum_row_ref, ret_ref, qdec_ref, state_ref):
    head = pl.program_id(0)
    length = q_ref.shape[0]
    cosine, sine = cos_ref[...], sin_ref[...]
    half = HEAD_DIM // 2

    def turned(ref):
        rows = ref[...].astype(jnp.float32)
        return rows * cosine + pltpu.roll(rows, half, 1) * sine

    lanes = lax.broadcasted_iota(jnp.int32, cum_ref.shape, 1)
    column = jnp.sum(jnp.where(lanes == head, cum_ref[...], 0.0), axis=1, keepdims=True)
    row = cum_row_ref[0]
    queries = turned(q_ref)
    keys = turned(k_ref) * HEAD_DIM ** (-0.5)
    values = v_ref[...]
    scores = lax.dot_general(
        queries.astype(jnp.bfloat16),
        keys.astype(jnp.bfloat16),
        (((1,), (1,)), ((), ())),
        preferred_element_type=jnp.float32,
    )
    causal = lax.broadcasted_iota(jnp.int32, (length, length), 0) >= lax.broadcasted_iota(
        jnp.int32, (length, length), 1
    )
    weights = jnp.where(causal, jnp.exp(jnp.minimum(column - row, 0.0)), 0.0)
    ret_ref[...] = jnp.dot(
        (scores * weights).astype(jnp.bfloat16), values, preferred_element_type=jnp.float32
    )
    qdec_ref[...] = (queries * jnp.exp(column)).astype(jnp.bfloat16)
    total = column[length - 1 :, :]
    tailed = (keys * jnp.exp(total - column)).astype(jnp.bfloat16)
    state_ref[0, :HEAD_DIM, :] = lax.dot_general(
        tailed, values, (((0,), (0,)), ((), ())), preferred_element_type=jnp.float32
    )
    state_ref[0, HEAD_DIM:, :] = jnp.broadcast_to(total, (8, HEAD_DIM))


def norm_kernel(ret_ref, qdec_ref, enter_ref, gain_ref, gate_ref, hidden_ref):
    retained = ret_ref[...] + jnp.dot(
        qdec_ref[...], enter_ref[0].astype(jnp.bfloat16), preferred_element_type=jnp.float32
    )
    centred = retained - jnp.mean(retained, axis=-1, keepdims=True)
    variance = jnp.mean(centred * centred, axis=-1, keepdims=True)
    gate = gate_ref[...].astype(jnp.float32)
    scaled = centred * lax.rsqrt(variance + group_eps) * gain_ref[...]
    hidden_ref[...] = (scaled * (gate / (1.0 + jnp.exp(-gate)))).astype(jnp.bfloat16)


def retention(query_rows, key_rows, value_rows, gate_rows, log_decay, head_gain):
    length, local_heads = log_decay.shape
    width = query_rows.shape[1]
    sp_count, mine = lax.axis_size("sp"), lax.axis_index("sp")
    positions = (mine * length + jnp.arange(length, dtype=jnp.int32)).astype(jnp.float32)
    angles = rotary_angles(positions, HEAD_DIM)
    cosine, sine = jnp.cos(angles), jnp.sin(angles)
    cosine = jnp.concatenate([cosine, cosine], axis=1)
    sine = jnp.concatenate([-sine, sine], axis=1)
    cumulative = jnp.cumsum(log_decay, axis=0)
    rows_spec = pl.BlockSpec((length, HEAD_DIM), lambda h: (0, h))
    table_spec = pl.BlockSpec((length, HEAD_DIM), lambda h: (0, 0))
    retained, qdec, state = pl.pallas_call(
        retention_kernel,
        grid=(local_heads,),
        out_shape=(
            jax.ShapeDtypeStruct((length, width), jnp.float32),
            jax.ShapeDtypeStruct((length, width), jnp.bfloat16),
            jax.ShapeDtypeStruct((local_heads, HEAD_DIM + 8, HEAD_DIM), jnp.float32),
        ),
        in_specs=[
            rows_spec,
            rows_spec,
            rows_spec,
            table_spec,
            table_spec,
            pl.BlockSpec((length, local_heads), lambda h: (0, 0)),
            pl.BlockSpec((1, 1, length), lambda h: (h, 0, 0)),
        ],
        out_specs=(
            rows_spec,
            rows_spec,
            pl.BlockSpec((1, HEAD_DIM + 8, HEAD_DIM), lambda h: (h, 0, 0)),
        ),
    )(query_rows, key_rows, value_rows, cosine, sine, cumulative, cumulative.T[:, None, :])
    pieces = lax.all_gather(state, "sp")
    totals = pieces[:, :, HEAD_DIM, 0]
    index = jnp.arange(sp_count, dtype=jnp.int32)
    between = (index[None, :] > index[:, None]) & (index[None, :] < mine)
    gap = jnp.sum(jnp.where(between[:, :, None], totals[None], 0.0), axis=1)
    factor = jnp.where((index < mine)[:, None], jnp.exp(gap), 0.0)
    entering = jnp.sum(factor[:, :, None, None] * pieces[:, :, :HEAD_DIM, :], axis=0)
    return pl.pallas_call(
        norm_kernel,
        grid=(local_heads,),
        out_shape=jax.ShapeDtypeStruct((length, width), jnp.bfloat16),
        in_specs=[
            rows_spec,
            rows_spec,
            pl.BlockSpec((1, HEAD_DIM, HEAD_DIM), lambda h: (h, 0, 0)),
            pl.BlockSpec((1, HEAD_DIM), lambda h: (0, h)),
            rows_spec,
        ],
        out_specs=rows_spec,
    )(retained, qdec, entering, head_gain[None, :], gate_rows)


(
    UP_A, UP_B, DOWN_A, DOWN_B, X_A2, Y_B2, Y_A3, Y_A4, X_B3, X_B4, C_A, C_B, C_P, Y_A, X_B, X_A, Y_B, R_UP_A, R_UP_B,
    TOTAL, CHAIN, ACROSS, MIX_C, MIX_Y, S_X2, S_Y2, S_Y3, S_X3, S_Y4, S_X4, S_UP, S_DOWN, S_CORE,
    T_UP, T_DOWN, T_Y1, T_X1, T_X2, T_Y2, R_DOWN_A, R_DOWN_B, TOTAL_ON,
) = range(42)


def layer_kernel(
    planes, logs_hbm, k_hbm, near_hbm, base_hbm, v_hbm, q_hbm, gate_hbm, gain_hbm, routes_hbm, shares_hbm,
    residual_hbm, ffn_gain_hbm, wo_hbm, wg_hbm, wu_hbm, wd_hbm, out_hbm,
    logs, k_ref, near_table, base_table, v_ref, q_ref, gate_ref, head_gain, routes, route_weights,
    residual, ffn_gain, wo, wg, wu, wd, rotary, turned_k, ret, qdec, state, cum_col, cum_row, total_own, total_x, carry_in, carry_out,
    side_out, side_in, hidden, blend, from_core, held, from_y, upd,
    share_in, g0, g1, gs, pm, pr, a0, a1, r10, r11, b0, b1, r20, r21, d0, d1, low_up, low_down, high_up, high_down,
    tot, tot_up, tot_down, home, home_in, pair, pair_in, total_prev, out,
    ssem, rsem, wsem,
):
    sp, tp = lax.axis_index("sp"), lax.axis_index("tp")
    sp_count = 2 * planes
    z, x = sp // 2, sp % 2
    y, c = tp // 2, tp % 2
    own_rows, width = out.shape
    half = a0.shape[-1]
    wide_a, wide_b = g0.shape[-1] - 128, g1.shape[-1]
    wide_ab = wide_a + wide_b
    rows = own_rows // 2
    items = 2 * planes
    lag = items - 3
    f32, bf16 = jnp.float32, jnp.bfloat16
    to_core = {"sp": sp, "tp": y * 2 + (1 - c)}
    to_y = {"sp": sp, "tp": (1 - y) * 2 + c}
    to_x = {"sp": z * 2 + (1 - x), "tp": tp}

    def half_of(n):
        return jnp.where(n == items - 1, 1, jnp.where(n == 0, 0, (n + 1) % 2))

    def plane_at(k):
        low = z < planes // 2
        mirrored = jnp.where(low, z, planes - 1 - z)
        q = jnp.where(k <= mirrored, mirrored - k, k)
        return jnp.where(low, q, planes - 1 - q)

    def plane_of(n):
        return plane_at(((n + 1) // 2) % planes)

    def item_of(n):
        return 2 * plane_of(n) + half_of(n)

    def step_of(turn):
        back = items - 3 - 2 * ((turn - 2) // 2) + turn % 2
        kept = (turn <= 1) | (turn == items - 1)
        return jnp.where(kept, turn, jnp.where(turn == items - 2, 2, back))

    def has_turn(u):
        return (u >= 0) & (u < items)

    def at_plane(p):
        return {"sp": p * 2 + x, "tp": tp}

    def to_z(i):
        return at_plane((z + planes - i) % planes)

    def move(kind, n, src, dst, device, m=None):
        return pltpu.make_async_remote_copy(
            src_ref=src, dst_ref=dst, send_sem=ssem.at[kind, n],
            recv_sem=rsem.at[kind, n if m is None else m],
            device_id=device, device_id_type=pl.DeviceIdType.MESH,
        )

    def send(kind, n, src, dst, device, m=None):
        move(kind, n, src, dst, device, m).start()

    def arrived(kind, n, dst):
        move(kind, n, dst, dst, to_core).wait_recv()

    def left(kind, n, src):
        move(kind, n, src, src, to_core).wait_send()

    takes = (x == 0) & (z > 0)
    loads = [
        pltpu.make_async_copy(far, near, wsem.at[i])
        for i, (far, near) in enumerate(
            [
                (logs_hbm, logs), (k_hbm, k_ref), (near_hbm, near_table), (base_hbm, base_table), (v_hbm, v_ref),
                (q_hbm, q_ref), (gate_hbm, gate_ref), (gain_hbm, head_gain), (routes_hbm, routes),
                (shares_hbm, route_weights), (residual_hbm, residual), (ffn_gain_hbm, ffn_gain),
                (wo_hbm, wo), (wg_hbm, wg), (wu_hbm, wu), (wd_hbm, wd),
            ]
        )
    ]
    for copy in loads:
        copy.start()
    barrier = pltpu.get_barrier_semaphore()
    for device in [to_core, to_y, to_x] + [to_z(i) for i in range(1, planes)]:
        pl.semaphore_signal(barrier, inc=1, device_id=device, device_id_type=pl.DeviceIdType.MESH)


    @pl.when(takes)
    def _():
        pl.semaphore_signal(
            barrier, inc=1, device_id={"sp": z * 2 - 1, "tp": tp}, device_id_type=pl.DeviceIdType.MESH
        )

    length = q_ref.shape[0]
    dim = HEAD_DIM
    heads = q_ref.shape[1] // dim
    depth = state.shape[1]
    cuts = dim // depth
    after = lax.broadcasted_iota(jnp.int32, (length, length), 0) >= lax.broadcasted_iota(
        jnp.int32, (length, length), 1
    )
    ones = jnp.where(after, 1.0, 0.0).astype(f32)
    loads[0].wait()
    log_rows = jnp.concatenate([logs[...], jnp.zeros((8 - heads, length), f32)], axis=0)
    cum_row[...] = lax.dot_general(
        log_rows, ones, (((1,), (1,)), ((), ())), precision=highest, preferred_element_type=f32
    )
    cum_col[...] = lax.dot_general(
        ones, log_rows, (((1,), (1,)), ((), ())), precision=highest, preferred_element_type=f32
    )
    total_own[...] = jnp.broadcast_to(cum_row[:, length - 1 :], (8, dim))
    gives = (x == 1) & (z + 1 < planes)
    pl.semaphore_wait(barrier, 2 + planes + jnp.where(gives, 1, 0))
    send(TOTAL, 0, total_own, total_x, to_x)

    @pl.when(gives)
    def _():
        send(TOTAL_ON, 0, total_own, total_prev, {"sp": (z + 1) * 2, "tp": tp})


    loads[2].wait()
    loads[3].wait()
    base = base_table[pl.ds(sp * 8, 8), :]
    cosine = base[0:1] * near_table[0] - base[1:2] * near_table[1]
    sine = base[2:3] * near_table[0] + base[3:4] * near_table[1]
    rotary[0] = cosine
    rotary[1] = sine

    def turned(rows_in):
        wide = rows_in.astype(f32)
        return wide * rotary[0] + pltpu.roll(wide, dim // 2, 1) * rotary[1]

    def column_of(h):
        lanes = lax.broadcasted_iota(jnp.int32, cum_col.shape, 1)
        return jnp.sum(jnp.where(lanes == h, cum_col[...], 0.0), axis=1, keepdims=True)

    left_side = x == 0

    def incoming(e):
        return jnp.where(takes, jnp.exp(total_prev[e // cuts : e // cuts + 1, :]), 1.0) * carry_in[e].astype(f32)

    def pass_state(e, first):
        h = e // cuts
        if first:
            grown = state[e].astype(bf16)
            before = jnp.zeros((depth, dim), bf16)
        else:
            near = incoming(e)
            span = total_own[h : h + 1, :] + jnp.where(left_side, 0.0, total_x[h : h + 1, :])
            grown = (jnp.exp(span) * near + state[e]).astype(bf16)
            before = near.astype(bf16)
        carry_out[e] = grown
        side_out[e] = jnp.where(left_side, grown, before)

        @pl.when(z + 1 < planes)
        def _():
            send(CHAIN, e, carry_out.at[e], carry_in.at[e], at_plane(z + 1))

        send(ACROSS, e, side_out.at[e], side_in.at[e], to_x)

    @pl.when(jnp.logical_not(takes))
    def _():
        total_prev[...] = jnp.zeros_like(total_prev)

    @pl.when(z == 0)
    def _():
        carry_in[...] = jnp.zeros_like(carry_in)
        for r in range(2):
            for ref in (tot_up, low_up, high_up):
                ref[r] = jnp.zeros_like(ref[r])

    @pl.when(z == planes - 1)
    def _():
        for r in range(2):
            for ref in (tot_down, low_down, high_down):
                ref[2 * planes - 2 + r] = jnp.zeros_like(ref[r])

    loads[1].wait()
    loads[4].wait()
    for h in range(heads):
        lanes = pl.ds(h * dim, dim)
        keys = turned(k_ref[:, lanes]) * dim ** (-0.5)
        turned_k[:, lanes] = keys.astype(bf16)
        column = column_of(h)
        tailed = (keys * jnp.exp(column[length - 1 :, :] - column)).astype(bf16)
        state[cuts * h : cuts * (h + 1)] = lax.dot_general(
            tailed, v_ref[:, lanes], (((0,), (0,)), ((), ())), preferred_element_type=f32
        ).reshape(cuts, depth, dim)

        @pl.when(z == 0)
        def _():
            for e in range(cuts * h, cuts * (h + 1)):
                pass_state(e, True)

    def attend(h, carry):
        lanes = pl.ds(pl.multiple_of(h * dim, dim), dim)
        queries = turned(q_ref[:, lanes])
        column = column_of(h)
        scores = lax.dot_general(
            queries.astype(bf16), turned_k[:, lanes], (((1,), (1,)), ((), ())), preferred_element_type=f32
        )
        gap = jnp.minimum(column - cum_row[pl.ds(h, 1), :], 0.0)
        decays = jnp.where(after, jnp.exp(gap), 0.0)
        ret[:, lanes] = jnp.dot((scores * decays).astype(bf16), v_ref[:, lanes], preferred_element_type=f32)
        qdec[:, lanes] = (queries * jnp.exp(column)).astype(bf16)
        return carry

    early = jnp.where(z >= planes // 2, heads, 0)
    loads[5].wait()
    lax.fori_loop(0, early, attend, 0)

    arrived(TOTAL, 0, total_x)

    @pl.when(takes)
    def _():
        arrived(TOTAL_ON, 0, total_prev)

    for e in range(cuts * heads):

        @pl.when(z > 0)
        def _():
            arrived(CHAIN, e, carry_in.at[e])
            pass_state(e, False)

    lax.fori_loop(early, heads, attend, 0)

    for h in range(heads):
        lanes = pl.ds(h * dim, dim)
        if h == 0:
            loads[6].wait()
            loads[7].wait()
        blocks = slice(cuts * h, cuts * (h + 1))
        for e in range(cuts * h, cuts * (h + 1)):
            arrived(ACROSS, e, side_in.at[e])
        factor = jnp.where(left_side, 1.0, jnp.exp(total_x[h : h + 1, :]))
        factor = factor * jnp.where(takes, jnp.exp(total_prev[h : h + 1, :]), 1.0)
        before = carry_in[blocks].reshape(dim, dim).astype(f32)
        entering = (factor * before + side_in[blocks].reshape(dim, dim).astype(f32)).astype(bf16)
        retained = ret[:, lanes] + jnp.dot(qdec[:, lanes], entering, preferred_element_type=f32)
        centred = retained - jnp.mean(retained, axis=-1, keepdims=True)
        variance = jnp.mean(centred * centred, axis=-1, keepdims=True)
        gate_in = gate_ref[:, lanes].astype(f32)
        scaled = centred * lax.rsqrt(variance + group_eps) * head_gain[:, lanes]
        made = (scaled * (gate_in / (1.0 + jnp.exp(-gate_in)))).astype(bf16)
        hidden[:, :, lanes] = made.reshape(4, own_rows, dim)

    loads[12].wait()
    pieces = blend.shape[0]
    spans = pieces // 2
    span = width // spans

    def cross(j):
        arrived(MIX_C, j, from_core.at[j])
        held[j] = (blend[j, c, 1 - y].astype(f32) + from_core[j, 1 - y].astype(f32)).astype(bf16)
        send(MIX_Y, j, held.at[j], from_y.at[j], to_y)

    for j in range(pieces):
        picked = hidden[:, j // spans * rows : (j // spans + 1) * rows, :].reshape(4 * rows, heads * dim)
        mixed = jnp.dot(picked, wo[:, pl.ds(j % spans * span, span)], preferred_element_type=f32).astype(bf16)
        for q in range(4):
            blend[j, q % 2, q // 2] = mixed[q * rows : (q + 1) * rows, :]
        send(MIX_C, j, blend.at[j, 1 - c], from_core.at[j], to_core)
        if j > 0:
            cross(j - 1)
    cross(pieces - 1)

    here = x * 2 + y
    other_x = (1 - x) * 2 + y
    other_y = x * 2 + (1 - y)
    other_xy = (1 - x) * 2 + (1 - y)
    for copy in loads[8:12]:
        copy.wait()
    count = routes.shape[0]
    share_in[...] = jnp.zeros_like(share_in)
    share_in[:count, :own_rows] = route_weights[...]
    all_routes = jnp.concatenate([routes[...]] * (8 // count), axis=0)
    own_routes = jnp.zeros((8, 128), jnp.int32)
    for q in range(4):
        turned_routes = pltpu.roll(all_routes, (length - q * own_rows) % length, 1)
        own_routes = own_routes + jnp.where(tp == q, turned_routes[:, :128], 0)
    expert = lax.broadcasted_iota(jnp.int32, (128, 128), 0)
    shares = jnp.zeros((128, 128), f32)
    for k in range(count):
        shares = shares + jnp.where(own_routes[k : k + 1, :] == expert, share_in[k : k + 1, :], 0.0)
    share = jnp.transpose(shares)[:own_rows, :]
    coarse = share.astype(bf16).astype(f32)
    tail_rows = (coarse + pltpu.roll(share - coarse, sp_count, 1)).astype(bf16)
    first_rows, last_rows = pl.ds(0, rows), pl.ds(rows, rows)
    def side(p, chip, part):
        return gs.at[c, p, chip, part]

    def pass_side(kind, n, chip, part, device):
        send(kind, n, side(z, chip, part), side(z, chip, part), device)

    def spread_side(r):
        if r == 0:
            pass_side(S_X2, 0, here, first_rows, to_x)
            pass_side(S_Y3, 0, here, first_rows, to_y)
        else:
            pass_side(S_Y2, 0, here, last_rows, to_y)
            pass_side(S_X3, 0, here, last_rows, to_x)

    def relay_side():
        arrived(S_X2, 0, side(z, other_x, first_rows))
        pass_side(S_Y4, 0, other_x, first_rows, to_y)
        arrived(S_Y2, 0, side(z, other_y, last_rows))
        pass_side(S_X4, 0, other_y, last_rows, to_x)

    def side_up(p):
        @pl.when(z + 1 < planes)
        def _():
            send(S_UP, p, gs.at[c, p], gs.at[c, p], at_plane(z + 1))

    def side_down(p):
        @pl.when(z > 0)
        def _():
            send(S_DOWN, p, gs.at[c, p], gs.at[c, p], at_plane(z - 1))

    def side_core(p):
        send(S_CORE, p, gs.at[c, p], gs.at[c, p], to_core)

    def close_side():
        arrived(S_Y3, 0, side(z, other_y, first_rows))
        arrived(S_Y4, 0, side(z, other_xy, first_rows))
        arrived(S_X3, 0, side(z, other_x, last_rows))
        arrived(S_X4, 0, side(z, other_xy, last_rows))
        side_up(z)
        side_down(z)
        side_core(z)

    def spread(n):
        send(X_A2, n, g0.at[c, n, here], g0.at[c, n, here], to_x)
        send(Y_B2, n, g1.at[c, n, here], g1.at[c, n, here], to_y)
        send(Y_A3, n, g0.at[c, n, here], g0.at[c, n, here], to_y)
        send(X_B3, n, g1.at[c, n, here], g1.at[c, n, here], to_x)

    def raise_up(n):
        @pl.when(z + 1 < planes)
        def _():
            send(UP_A, n, g0.at[c, n, here], g0.at[c, n, here], at_plane(z + 1))
            send(UP_B, n, g1.at[c, n, here], g1.at[c, n, here], at_plane(z + 1))

    def hand_down(n):
        @pl.when(z > 0)
        def _():
            send(DOWN_A, n, g0.at[c, n, here], g0.at[c, n, here], at_plane(z - 1))
            send(DOWN_B, n, g1.at[c, n, here], g1.at[c, n, here], at_plane(z - 1))

    for r in range(2):
        mine, n = slice(r * rows, (r + 1) * rows), 2 * z + r
        square = jnp.zeros((rows, 1), f32)
        for j in range(r * spans, (r + 1) * spans):
            cols = pl.ds(j % spans * span, span)
            near = residual[mine, cols].astype(f32) + blend[j, c, y].astype(f32) + from_core[j, y].astype(f32)
            arrived(MIX_Y, j, from_y.at[j])
            total = near + from_y[j].astype(f32)
            upd[mine, cols] = total
            square = square + jnp.sum(total * total, axis=-1, keepdims=True)
        scale = lax.rsqrt(square * (1.0 / width) + square_eps)
        ready = (upd[mine, :] * scale * ffn_gain[...]).astype(bf16)
        g0[c, n, here, :, :wide_a] = ready[:, :wide_a]
        g0[c, n, here, :, wide_a:] = tail_rows[mine]
        g1[c, n, here] = ready[:, wide_a:wide_ab]
        gs[c, z, here, mine, :] = ready[:, wide_ab:]
        raise_up(n)
        hand_down(n)
        spread_side(r)
        if r == 0:
            spread(n)

    last_chains = [(T_UP, T_DOWN, tot, tot_up, tot_down)]
    main_chains = [(R_UP_A, R_DOWN_A, d0, low_up, low_down), (R_UP_B, R_DOWN_B, d1, high_up, high_down)]

    def start_chain(n, chains):
        @pl.when((n // 2 > z) & (z == 0))
        def _():
            for up, _, acc, got_up, _ in chains:
                send(up, n, acc.at[n], got_up.at[n], at_plane(z + 1))

        @pl.when((n // 2 < z) & (z == planes - 1))
        def _():
            for _, down, acc, _, got_down in chains:
                send(down, n, acc.at[n], got_down.at[n], at_plane(z - 1))

    def go_on(turn, chains):
        n = item_of(step_of(turn))

        @pl.when((n // 2 > z) & (z > 0))
        def _():
            for up, _, acc, got_up, _ in chains:
                arrived(up, n, got_up.at[n])
                acc[n] = (acc[n].astype(f32) + got_up[n].astype(f32)).astype(bf16)
                send(up, n, acc.at[n], got_up.at[n], at_plane(z + 1))

        @pl.when((n // 2 < z) & (z < planes - 1))
        def _():
            for _, down, acc, _, got_down in chains:
                arrived(down, n, got_down.at[n])
                acc[n] = (acc[n].astype(f32) + got_down[n].astype(f32)).astype(bf16)
                send(down, n, acc.at[n], got_down.at[n], at_plane(z - 1))

    def tick(t, carry):
        def relay():
            n = item_of(t)
            arrived(X_A2, n, g0.at[c, n, other_x])
            send(Y_A4, n, g0.at[c, n, other_x], g0.at[c, n, other_x], to_y)
            arrived(Y_B2, n, g1.at[c, n, other_y])
            send(X_B4, n, g1.at[c, n, other_y], g1.at[c, n, other_y], to_x)

        pl.when(t == 0)(relay_side)
        pl.when(t == 0)(relay)
        pl.when(t == 1)(close_side)

        @pl.when(t + 1 < items)
        def _():
            k, r = (t + 2) // 2, t % 2

            @pl.when((t + 1 < items - 1) & (z - k >= 0))
            def _():
                n = 2 * (z - k) + r
                arrived(UP_A, n, g0.at[c, n, here])
                arrived(UP_B, n, g1.at[c, n, here])
                raise_up(n)

            @pl.when((t + 1 < items - 1) & (z + k < planes))
            def _():
                n = 2 * (z + k) + r
                arrived(DOWN_A, n, g0.at[c, n, here])
                arrived(DOWN_B, n, g1.at[c, n, here])
                hand_down(n)

            spread(item_of(t + 1))

        pl.when((t > 0) & (t < items))(relay)

        @pl.when((t >= 2) & (t < items) & (t % 2 == 0))
        def _():
            below, above = z - t // 2, z + t // 2

            @pl.when(below >= 0)
            def _():
                arrived(S_UP, below, gs.at[c, below])
                side_up(below)
                side_core(below)

            @pl.when(above < planes)
            def _():
                arrived(S_DOWN, above, gs.at[c, above])
                side_down(above)
                side_core(above)

        @pl.when(t == 2)
        def _():
            for copy in loads[13:]:
                copy.wait()

        @pl.when((t >= 2) & (t < items + 2))
        def _():
            n = item_of(t - 2)
            arrived(C_A, n, g0.at[1 - c, n])
            arrived(C_B, n, g1.at[1 - c, n])
            p, r = plane_of(t - 2), half_of(t - 2)

            @pl.when(r == 0)
            def _():
                arrived(S_CORE, p, gs.at[1 - c, p])

            lead = g0[:, n].reshape(8 * rows, wide_a + 128)
            tail = lead[:, wide_a:].astype(f32)
            rest = g1[:, n].reshape(8 * rows, wide_b)
            last = gs[:, p, :, pl.ds(pl.multiple_of(r * rows, rows), rows), :].reshape(8 * rows, width - wide_ab)
            rows_in = jnp.concatenate([lead[:, :wide_a], rest, last], axis=1)
            lane = lax.broadcasted_iota(jnp.int32, tail.shape, 1)
            weight = jnp.sum(
                jnp.where((lane == sp) | (lane == sp + sp_count), tail, 0.0), axis=1, keepdims=True
            )

            def product(w):
                return jnp.dot(rows_in, w[...], preferred_element_type=f32)

            gate = jnp.minimum(product(wg), clamp_limit)
            up = jnp.clip(product(wu), -clamp_limit, clamp_limit)
            act = ((up + 1.0) * (gate / (1.0 + jnp.exp(-swish_alpha * gate)))).astype(bf16)
            made = (jnp.dot(act, wd[...], preferred_element_type=f32) * weight).astype(bf16)
            pm[n] = made.reshape(2, 4 * rows, width)
            send(C_P, n, pm.at[n, 1 - c], pr.at[n], to_core)

        @pl.when((t >= 1) & (t < items + 1))
        def _():
            n = item_of(t - 1)
            arrived(Y_A3, n, g0.at[c, n, other_y])
            arrived(Y_A4, n, g0.at[c, n, other_xy])
            arrived(X_B3, n, g1.at[c, n, other_x])
            arrived(X_B4, n, g1.at[c, n, other_xy])
            send(C_A, n, g0.at[c, n], g0.at[c, n], to_core)
            send(C_B, n, g1.at[c, n], g1.at[c, n], to_core)

        @pl.when(has_turn(t - lag))
        def _():
            n = item_of(step_of(t - lag))
            arrived(C_P, n, pr.at[n])
            for q in range(4):
                part = pl.ds(q * rows, rows)
                total = (pm[n, c, part, :].astype(f32) + pr[n, part, :].astype(f32)).astype(bf16)
                a0[n, q % 2, q // 2] = total[:, :half]
                a1[n, q // 2, q % 2] = total[:, half : 2 * half]
                tot[n, q] = total[:, 2 * half :]
            send(Y_A, n, a0.at[n, 1 - y], r10.at[n], to_y)
            send(X_B, n, a1.at[n, 1 - x], r11.at[n], to_x)
            start_chain(n, last_chains)

        @pl.when(has_turn(t - lag - 1))
        def _():
            n = item_of(step_of(t - lag - 1))
            arrived(Y_A, n, r10.at[n])
            b0[n] = (a0[n, y].astype(f32) + r10[n].astype(f32)).astype(bf16)
            send(X_A, n, b0.at[n, 1 - x], r20.at[n], to_x)
            arrived(X_B, n, r11.at[n])
            b1[n] = (a1[n, x].astype(f32) + r11[n].astype(f32)).astype(bf16)
            send(Y_B, n, b1.at[n, 1 - y], r21.at[n], to_y)

        @pl.when(has_turn(t - lag - 2))
        def _():
            n = item_of(step_of(t - lag - 2))
            arrived(X_A, n, r20.at[n])
            d0[n] = (b0[n, x].astype(f32) + r20[n].astype(f32)).astype(bf16)
            arrived(Y_B, n, r21.at[n])
            d1[n] = (b1[n, y].astype(f32) + r21[n].astype(f32)).astype(bf16)
            start_chain(n, main_chains)

        u = t - lag

        @pl.when((u >= 3) & (u <= items - 2))
        def _():
            go_on(u - 1, last_chains)

        @pl.when(u == items - 2)
        def _():
            go_on(1, last_chains)
            go_on(items - 2, last_chains)

        @pl.when((u >= 5) & (u <= items))
        def _():
            go_on(u - 3, main_chains)

        @pl.when(u == items)
        def _():
            go_on(1, main_chains)
            go_on(items - 2, main_chains)

        @pl.when(u == items - 1)
        def _():
            for r in range(2):
                n = 2 * z + r

                @pl.when(z > 0)
                def _():
                    arrived(T_UP, n, tot_up.at[n])

                @pl.when(z < planes - 1)
                def _():
                    arrived(T_DOWN, n, tot_down.at[n])

                for q in range(4):
                    total = tot[n, q].astype(f32) + tot_up[n, q].astype(f32) + tot_down[n, q].astype(f32)
                    place = (q % 2, q // 2) if r == 0 else (q // 2, q % 2)
                    home[r, place[0], place[1]] = total.astype(bf16)
            send(T_Y1, 0, home.at[0, 1 - y], home_in.at[0], to_y)
            send(T_X1, 0, home.at[1, 1 - x], home_in.at[1], to_x)

        @pl.when(u == items)
        def _():
            arrived(T_Y1, 0, home_in.at[0])
            pair[0] = (home[0, y].astype(f32) + home_in[0].astype(f32)).astype(bf16)
            send(T_X2, 0, pair.at[0, 1 - x], pair_in.at[0], to_x)
            arrived(T_X1, 0, home_in.at[1])
            pair[1] = (home[1, x].astype(f32) + home_in[1].astype(f32)).astype(bf16)
            send(T_Y2, 0, pair.at[1, 1 - y], pair_in.at[1], to_y)

        return carry

    lax.fori_loop(0, items + lag + 2, tick, 0)
    arrived(T_X2, 0, pair_in.at[0])
    arrived(T_Y2, 0, pair_in.at[1])
    writes = []
    for r in range(2):
        n, part = 2 * z + r, pl.ds(r * rows, rows)
        low = upd[part, :half] + d0[n].astype(f32)
        high = upd[part, half : 2 * half] + d1[n].astype(f32)

        @pl.when(z > 0)
        def _():
            arrived(R_UP_A, n, low_up.at[n])
            arrived(R_UP_B, n, high_up.at[n])

        @pl.when(z < planes - 1)
        def _():
            arrived(R_DOWN_A, n, low_down.at[n])
            arrived(R_DOWN_B, n, high_down.at[n])

        low = low + low_up[n].astype(f32) + low_down[n].astype(f32)
        high = high + high_up[n].astype(f32) + high_down[n].astype(f32)
        out[part, :half] = low.astype(bf16)
        out[part, half : 2 * half] = high.astype(bf16)
        kept = pair[0, x] if r == 0 else pair[1, y]
        out[part, 2 * half :] = (
            upd[part, 2 * half :] + kept.astype(f32) + pair_in[r].astype(f32)
        ).astype(bf16)
        write = pltpu.make_async_copy(out.at[part], out_hbm.at[part], wsem.at[len(loads) + r])
        write.start()
        writes.append(write)

    left(T_Y1, 0, home.at[0, 1 - y])
    left(T_X1, 0, home.at[1, 1 - x])
    left(T_X2, 0, pair.at[0, 1 - x])
    left(T_Y2, 0, pair.at[1, 1 - y])

    def drain(n, carry):
        p = n // 2

        @pl.when(p > z)
        def _():
            for up, _, acc, _, _ in last_chains + main_chains:
                left(up, n, acc.at[n])

        @pl.when(p < z)
        def _():
            for _, down, acc, _, _ in last_chains + main_chains:
                left(down, n, acc.at[n])

        @pl.when((p <= z) & (z + 1 < planes))
        def _():
            left(UP_A, n, g0.at[c, n, here])
            left(UP_B, n, g1.at[c, n, here])

        @pl.when((p >= z) & (z > 0))
        def _():
            left(DOWN_A, n, g0.at[c, n, here])
            left(DOWN_B, n, g1.at[c, n, here])

        left(X_A2, n, g0.at[c, n, here])
        left(Y_B2, n, g1.at[c, n, here])
        left(Y_A3, n, g0.at[c, n, here])
        left(X_B3, n, g1.at[c, n, here])
        left(Y_A4, n, g0.at[c, n, other_x])
        left(X_B4, n, g1.at[c, n, other_y])
        left(C_A, n, g0.at[c, n])
        left(C_B, n, g1.at[c, n])
        left(C_P, n, pm.at[n, 1 - c])
        left(Y_A, n, a0.at[n, 1 - y])
        left(X_B, n, a1.at[n, 1 - x])
        left(X_A, n, b0.at[n, 1 - x])
        left(Y_B, n, b1.at[n, 1 - y])
        return carry

    lax.fori_loop(0, items, drain, 0)
    left(S_X2, 0, side(z, here, first_rows))
    left(S_Y2, 0, side(z, here, last_rows))
    left(S_Y3, 0, side(z, here, first_rows))
    left(S_X3, 0, side(z, here, last_rows))
    left(S_Y4, 0, side(z, other_x, first_rows))
    left(S_X4, 0, side(z, other_y, last_rows))

    def drain_side(p, carry):
        @pl.when((p <= z) & (z + 1 < planes))
        def _():
            left(S_UP, p, gs.at[c, p])

        @pl.when((p >= z) & (z > 0))
        def _():
            left(S_DOWN, p, gs.at[c, p])

        left(S_CORE, p, gs.at[c, p])
        return carry

    lax.fori_loop(0, planes, drain_side, 0)
    left(TOTAL, 0, total_own)

    @pl.when(gives)
    def _():
        left(TOTAL_ON, 0, total_own)

    for e in range(cuts * heads):
        left(ACROSS, e, side_out.at[e])

        @pl.when(z + 1 < planes)
        def _():
            left(CHAIN, e, carry_out.at[e])

    for j in range(pieces):
        left(MIX_C, j, blend.at[j, 1 - c])
        left(MIX_Y, j, held.at[j])
    for write in writes:
        write.wait()


def rope_tables(length, spans):
    half_dim = HEAD_DIM // 2
    rates = rope_base ** (-np.arange(half_dim, dtype=np.float64) / half_dim)
    rates = np.concatenate([rates, rates])[None, :]
    near = np.arange(length, dtype=np.float64)[:, None] * rates
    starts = (np.arange(spans, dtype=np.float64) * length)[:, None] * rates
    sign = np.concatenate([-np.ones(half_dim), np.ones(half_dim)])[None, :]
    base = np.zeros((spans, 8, HEAD_DIM))
    base[:, 0], base[:, 1] = np.cos(starts), np.sin(starts)
    base[:, 2], base[:, 3] = sign * np.sin(starts), sign * np.cos(starts)
    near_table = np.stack([np.cos(near), np.sin(near)]).astype(np.float32)
    return jnp.asarray(near_table), jnp.asarray(base.reshape(spans * 8, HEAD_DIM).astype(np.float32))


def fused_layer(
    query_rows, key_rows, value_rows, gate_rows, log_decay, head_gain, out_weight, residual, ffn_gain,
    gate_part, up_part, down_part, routes, route_weights,
):
    sp_count = lax.axis_size("sp")
    length, heads = log_decay.shape
    rows_all, width = residual.shape
    inner = query_rows.shape[1]
    near_table, base_table = rope_tables(length, sp_count)
    wide_t = 128 * (width // 1024)
    half = (width - wide_t) // 2
    planes = sp_count // 2
    items = 2 * planes
    rows = rows_all // 2
    pieces = 8
    span = 2 * width // pieces
    wide_s = 128 * (3 * width // 2048)
    wide_a = (width - wide_s - 128) // 256 * 128
    wide_b = width - wide_s - wide_a
    bf16, f32 = jnp.bfloat16, jnp.float32
    whole = pl.BlockSpec(memory_space=pltpu.VMEM)
    far = pl.BlockSpec(memory_space=pltpu.HBM)
    operands = (
        log_decay.T, key_rows, near_table, base_table, value_rows, query_rows, gate_rows, head_gain[None, :],
        routes.T, route_weights.T, residual, ffn_gain[None, :], out_weight, gate_part, up_part, down_part,
    )
    square = (2 * heads, HEAD_DIM // 2, HEAD_DIM)
    return pl.pallas_call(
        functools.partial(layer_kernel, planes),
        out_shape=jax.ShapeDtypeStruct((rows_all, width), bf16),
        in_specs=[far] * len(operands),
        out_specs=far,
        scratch_shapes=[
            *[pltpu.VMEM(operand.shape, operand.dtype) for operand in operands],
            pltpu.VMEM((2, length, HEAD_DIM), f32),
            pltpu.VMEM((length, inner), bf16),
            pltpu.VMEM((length, inner), f32),
            pltpu.VMEM((length, inner), bf16),
            pltpu.VMEM(square, f32),
            pltpu.VMEM((length, 8), f32),
            pltpu.VMEM((8, length), f32),
            pltpu.VMEM((8, HEAD_DIM), f32),
            pltpu.VMEM((8, HEAD_DIM), f32),
            pltpu.VMEM(square, bf16),
            pltpu.VMEM(square, bf16),
            pltpu.VMEM(square, bf16),
            pltpu.VMEM(square, bf16),
            pltpu.VMEM((4, rows_all, inner), bf16),
            pltpu.VMEM((pieces, 2, 2, rows, span), bf16),
            pltpu.VMEM((pieces, 2, rows, span), bf16),
            pltpu.VMEM((pieces, rows, span), bf16),
            pltpu.VMEM((pieces, rows, span), bf16),
            pltpu.VMEM((rows_all, width), f32),
            pltpu.VMEM((8, 128), f32),
            pltpu.VMEM((2, items, 4, rows, wide_a + 128), bf16),
            pltpu.VMEM((2, items, 4, rows, wide_b), bf16),
            pltpu.VMEM((2, planes, 4, rows_all, wide_s), bf16),
            pltpu.VMEM((items, 2, 4 * rows, width), bf16),
            pltpu.VMEM((items, 4 * rows, width), bf16),
            pltpu.VMEM((items, 2, 2, rows, half), bf16),
            pltpu.VMEM((items, 2, 2, rows, half), bf16),
            pltpu.VMEM((items, 2, rows, half), bf16),
            pltpu.VMEM((items, 2, rows, half), bf16),
            pltpu.VMEM((items, 2, rows, half), bf16),
            pltpu.VMEM((items, 2, rows, half), bf16),
            pltpu.VMEM((items, rows, half), bf16),
            pltpu.VMEM((items, rows, half), bf16),
            pltpu.VMEM((items, rows, half), bf16),
            pltpu.VMEM((items, rows, half), bf16),
            pltpu.VMEM((items, rows, half), bf16),
            pltpu.VMEM((items, rows, half), bf16),
            pltpu.VMEM((items, rows, half), bf16),
            pltpu.VMEM((items, rows, half), bf16),
            pltpu.VMEM((items, 4, rows, wide_t), bf16),
            pltpu.VMEM((items, 4, rows, wide_t), bf16),
            pltpu.VMEM((items, 4, rows, wide_t), bf16),
            pltpu.VMEM((2, 2, 2, rows, wide_t), bf16),
            pltpu.VMEM((2, 2, rows, wide_t), bf16),
            pltpu.VMEM((2, 2, rows, wide_t), bf16),
            pltpu.VMEM((2, rows, wide_t), bf16),
            pltpu.VMEM((8, HEAD_DIM), f32),
            pltpu.VMEM((rows_all, width), bf16),
            pltpu.SemaphoreType.DMA((42, max(items, 2 * heads, pieces))),
            pltpu.SemaphoreType.DMA((42, max(items, 2 * heads, pieces))),
            pltpu.SemaphoreType.DMA((len(operands) + 2,)),
        ],
        compiler_params=pltpu.CompilerParams(
            collective_id=0, has_side_effects=True, vmem_limit_bytes=63 * 1024 * 1024
        ),
    )(*operands)


def body(
    query_rows,
    key_rows,
    value_rows,
    gate_rows,
    log_decay,
    head_gain,
    out_weight,
    residual,
    ffn_gain,
    gate_weight,
    up_weight,
    down_weight,
    routes,
    route_weights,
):
    tok_count = query_rows.shape[0]
    local_heads = log_decay.shape[1]
    sp_count = lax.axis_size("sp")
    tp_count = lax.axis_size("tp")
    model_width = residual.shape[1]
    rows_own = tok_count // tp_count
    capacity = max(2, 3 * rows_own * TOPK // (2 * sp_count))
    tp_index = lax.axis_index("tp")
    if (
        tp_count == 4 and sp_count % 2 == 0 and sp_count <= 16 and local_heads <= 8
        and rows_own <= 128 and rows_own < 2 * capacity and model_width % 2048 == 0
    ):
        return fused_layer(
            query_rows, key_rows, value_rows, gate_rows, log_decay, head_gain, out_weight, residual, ffn_gain,
            gate_weight[0], up_weight[0], down_weight[0], routes, route_weights,
        )
    own_routes = lax.dynamic_slice_in_dim(routes, tp_index * rows_own, rows_own, 0)
    hidden = retention(query_rows, key_rows, value_rows, gate_rows, log_decay, head_gain)
    mixed = jnp.dot(hidden, out_weight, preferred_element_type=jnp.float32).astype(jnp.bfloat16)
    mixed_sum = lax.psum_scatter(mixed, "tp", scatter_dimension=0, tiled=True).astype(jnp.float32)
    updated = residual.astype(jnp.float32) + mixed_sum
    ffn_in = square_norm(updated, ffn_gain)
    own_experts, own_ranks = slot_ranks(own_routes, sp_count)
    home_slot = own_experts * capacity + own_ranks
    gate_part = gate_weight[0]
    up_part = up_weight[0]
    down_part = down_weight[0]
    empty_row = jnp.zeros((1, model_width), jnp.bfloat16)
    source_row = (
        jnp.full((sp_count * capacity,), rows_own, jnp.int32)
        .at[home_slot]
        .set(jnp.arange(rows_own * TOPK, dtype=jnp.int32) // TOPK)
    )
    padded = jnp.concatenate([ffn_in, empty_row], axis=0)
    outgoing = padded[source_row].reshape(sp_count, capacity, model_width)
    arrived = lax.all_to_all(outgoing, "sp", split_axis=0, concat_axis=0, tiled=True)
    fanned = lax.all_gather(arrived[None], "tp", axis=0, tiled=True)
    activity = expert_rows(fanned.reshape(-1, model_width), gate_part, up_part)
    partial_out = jnp.dot(activity, down_part, preferred_element_type=jnp.float32).reshape(
        tp_count, sp_count, capacity, model_width
    )
    summed = (
        lax.psum_scatter(partial_out.astype(jnp.bfloat16), "tp", scatter_dimension=0, tiled=True)
        .astype(jnp.float32)
        .reshape(sp_count, capacity, model_width)
    )
    returned = lax.all_to_all(
        summed.astype(jnp.bfloat16), "sp", split_axis=0, concat_axis=0, tiled=True
    )
    picked = returned.reshape(sp_count * capacity, model_width)[home_slot].reshape(
        rows_own, TOPK, model_width
    )
    expert_sum = jnp.sum(route_weights[:, :, None] * picked.astype(jnp.float32), axis=1)
    return (updated + expert_sum).astype(jnp.bfloat16)


def solution(mesh):
    return jax.shard_map(
        body,
        mesh=mesh,
        in_specs=(
            P("sp", "tp"),
            P("sp", "tp"),
            P("sp", "tp"),
            P("sp", "tp"),
            P("sp", "tp"),
            P("tp"),
            P("tp", None),
            P(("sp", "tp"), None),
            P(),
            P("sp", None, "tp"),
            P("sp", None, "tp"),
            P("sp", "tp", None),
            P("sp", None),
            P(("sp", "tp"), None),
        ),
        out_specs=P(("sp", "tp"), None),
        check_vma=False,
    )
```

```python
import functools

import jax
import jax.numpy as jnp
import numpy as np
from jax import lax
from jax.experimental import pallas as pl
from jax.experimental.pallas import tpu as pltpu
from jax.sharding import PartitionSpec as P

HEAD_DIM = 128
TOPK = 4
BLOCK = 128


highest = lax.Precision.HIGHEST
rope_base = 10000.0
group_eps = 1e-05
square_eps = 1e-06
clamp_limit = 7.0
swish_alpha = 1.702


def rotary_angles(positions, head_dim):
    half_dim = head_dim // 2
    inverse = rope_base ** (-jnp.arange(half_dim, dtype=jnp.float32) / half_dim)
    return positions[:, None] * inverse[None, :]


def square_norm(updated, gain_row):
    factor = lax.rsqrt(jnp.mean(updated * updated, axis=-1, keepdims=True) + square_eps)
    return (updated * factor * gain_row).astype(jnp.bfloat16)


def expert_rows(rows, gate_part, up_part):
    gate_pre = jnp.dot(rows, gate_part, preferred_element_type=jnp.float32)
    up_pre = jnp.dot(rows, up_part, preferred_element_type=jnp.float32)
    gate_clip = jnp.minimum(gate_pre, clamp_limit)
    up_clip = jnp.clip(up_pre, -clamp_limit, clamp_limit)
    return ((up_clip + 1.0) * (gate_clip * jax.nn.sigmoid(gate_clip * swish_alpha))).astype(
        jnp.bfloat16
    )


def slot_ranks(route_block, experts):
    flat_routes = route_block.reshape(-1)
    onehot = (flat_routes[:, None] == jnp.arange(experts, dtype=jnp.int32)[None, :]).astype(
        jnp.int32
    )
    return (flat_routes, jnp.sum(jnp.cumsum(onehot, axis=0) * onehot, axis=1) - 1)


def retention_kernel(q_ref, k_ref, v_ref, cos_ref, sin_ref, cum_ref, cum_row_ref, ret_ref, qdec_ref, state_ref):
    head = pl.program_id(0)
    length = q_ref.shape[0]
    cosine, sine = cos_ref[...], sin_ref[...]
    half = HEAD_DIM // 2

    def turned(ref):
        rows = ref[...].astype(jnp.float32)
        return rows * cosine + pltpu.roll(rows, half, 1) * sine

    lanes = lax.broadcasted_iota(jnp.int32, cum_ref.shape, 1)
    column = jnp.sum(jnp.where(lanes == head, cum_ref[...], 0.0), axis=1, keepdims=True)
    row = cum_row_ref[0]
    queries = turned(q_ref)
    keys = turned(k_ref) * HEAD_DIM ** (-0.5)
    values = v_ref[...]
    scores = lax.dot_general(
        queries.astype(jnp.bfloat16),
        keys.astype(jnp.bfloat16),
        (((1,), (1,)), ((), ())),
        preferred_element_type=jnp.float32,
    )
    causal = lax.broadcasted_iota(jnp.int32, (length, length), 0) >= lax.broadcasted_iota(
        jnp.int32, (length, length), 1
    )
    weights = jnp.where(causal, jnp.exp(jnp.minimum(column - row, 0.0)), 0.0)
    ret_ref[...] = jnp.dot(
        (scores * weights).astype(jnp.bfloat16), values, preferred_element_type=jnp.float32
    )
    qdec_ref[...] = (queries * jnp.exp(column)).astype(jnp.bfloat16)
    total = column[length - 1 :, :]
    tailed = (keys * jnp.exp(total - column)).astype(jnp.bfloat16)
    state_ref[0, :HEAD_DIM, :] = lax.dot_general(
        tailed, values, (((0,), (0,)), ((), ())), preferred_element_type=jnp.float32
    )
    state_ref[0, HEAD_DIM:, :] = jnp.broadcast_to(total, (8, HEAD_DIM))


def norm_kernel(ret_ref, qdec_ref, enter_ref, gain_ref, gate_ref, hidden_ref):
    retained = ret_ref[...] + jnp.dot(
        qdec_ref[...], enter_ref[0].astype(jnp.bfloat16), preferred_element_type=jnp.float32
    )
    centred = retained - jnp.mean(retained, axis=-1, keepdims=True)
    variance = jnp.mean(centred * centred, axis=-1, keepdims=True)
    gate = gate_ref[...].astype(jnp.float32)
    scaled = centred * lax.rsqrt(variance + group_eps) * gain_ref[...]
    hidden_ref[...] = (scaled * (gate / (1.0 + jnp.exp(-gate)))).astype(jnp.bfloat16)


def retention(query_rows, key_rows, value_rows, gate_rows, log_decay, head_gain):
    length, local_heads = log_decay.shape
    width = query_rows.shape[1]
    sp_count, mine = lax.axis_size("sp"), lax.axis_index("sp")
    positions = (mine * length + jnp.arange(length, dtype=jnp.int32)).astype(jnp.float32)
    angles = rotary_angles(positions, HEAD_DIM)
    cosine, sine = jnp.cos(angles), jnp.sin(angles)
    cosine = jnp.concatenate([cosine, cosine], axis=1)
    sine = jnp.concatenate([-sine, sine], axis=1)
    cumulative = jnp.cumsum(log_decay, axis=0)
    rows_spec = pl.BlockSpec((length, HEAD_DIM), lambda h: (0, h))
    table_spec = pl.BlockSpec((length, HEAD_DIM), lambda h: (0, 0))
    retained, qdec, state = pl.pallas_call(
        retention_kernel,
        grid=(local_heads,),
        out_shape=(
            jax.ShapeDtypeStruct((length, width), jnp.float32),
            jax.ShapeDtypeStruct((length, width), jnp.bfloat16),
            jax.ShapeDtypeStruct((local_heads, HEAD_DIM + 8, HEAD_DIM), jnp.float32),
        ),
        in_specs=[
            rows_spec,
            rows_spec,
            rows_spec,
            table_spec,
            table_spec,
            pl.BlockSpec((length, local_heads), lambda h: (0, 0)),
            pl.BlockSpec((1, 1, length), lambda h: (h, 0, 0)),
        ],
        out_specs=(
            rows_spec,
            rows_spec,
            pl.BlockSpec((1, HEAD_DIM + 8, HEAD_DIM), lambda h: (h, 0, 0)),
        ),
    )(query_rows, key_rows, value_rows, cosine, sine, cumulative, cumulative.T[:, None, :])
    pieces = lax.all_gather(state, "sp")
    totals = pieces[:, :, HEAD_DIM, 0]
    index = jnp.arange(sp_count, dtype=jnp.int32)
    between = (index[None, :] > index[:, None]) & (index[None, :] < mine)
    gap = jnp.sum(jnp.where(between[:, :, None], totals[None], 0.0), axis=1)
    factor = jnp.where((index < mine)[:, None], jnp.exp(gap), 0.0)
    entering = jnp.sum(factor[:, :, None, None] * pieces[:, :, :HEAD_DIM, :], axis=0)
    return pl.pallas_call(
        norm_kernel,
        grid=(local_heads,),
        out_shape=jax.ShapeDtypeStruct((length, width), jnp.bfloat16),
        in_specs=[
            rows_spec,
            rows_spec,
            pl.BlockSpec((1, HEAD_DIM, HEAD_DIM), lambda h: (h, 0, 0)),
            pl.BlockSpec((1, HEAD_DIM), lambda h: (0, h)),
            rows_spec,
        ],
        out_specs=rows_spec,
    )(retained, qdec, entering, head_gain[None, :], gate_rows)


(
    UP_A, UP_B, DOWN_A, DOWN_B, X_A2, Y_B2, Y_A3, Y_A4, X_B3, X_B4, C_A, C_B, C_P, Y_A, X_B, X_A, Y_B, R_UP_A, R_UP_B,
    TOTAL, CHAIN, ACROSS, MIX_C, MIX_Y, S_X2, S_Y2, S_Y3, S_X3, S_Y4, S_X4, S_UP, S_DOWN, S_CORE,
    T_UP, T_DOWN, T_Y1, T_X1, T_X2, T_Y2, R_DOWN_A, R_DOWN_B, TOTAL_ON,
) = range(42)


def layer_kernel(
    planes, logs_hbm, k_hbm, near_hbm, base_hbm, v_hbm, q_hbm, gate_hbm, gain_hbm, routes_hbm, shares_hbm,
    residual_hbm, ffn_gain_hbm, wo_hbm, wg_hbm, wu_hbm, wd_hbm, out_hbm,
    logs, k_ref, near_table, base_table, v_ref, q_ref, gate_ref, head_gain, routes, route_weights,
    residual, ffn_gain, wo, wg, wu, wd, rotary, turned_k, ret, qdec, state, cum_col, cum_row, total_own, total_x, carry_in, carry_out,
    side_out, side_in, hidden, blend, from_core, held, from_y, upd,
    share_in, g0, g1, gs, pm, pr, a0, a1, r10, r11, b0, b1, r20, r21, d0, d1, low_up, low_down, high_up, high_down,
    tot, tot_up, tot_down, home, home_in, pair, pair_in, total_prev, out,
    ssem, rsem, wsem,
):
    sp, tp = lax.axis_index("sp"), lax.axis_index("tp")
    sp_count = 2 * planes
    z, x = sp // 2, sp % 2
    y, c = tp // 2, tp % 2
    own_rows, width = out.shape
    half = a0.shape[-1]
    wide_a, wide_b = g0.shape[-1] - 128, g1.shape[-1]
    wide_ab = wide_a + wide_b
    rows = own_rows // 2
    items = 2 * planes
    lag = items - 3
    f32, bf16 = jnp.float32, jnp.bfloat16
    to_core = {"sp": sp, "tp": y * 2 + (1 - c)}
    to_y = {"sp": sp, "tp": (1 - y) * 2 + c}
    to_x = {"sp": z * 2 + (1 - x), "tp": tp}

    def half_of(n):
        return jnp.where(n == items - 1, 1, jnp.where(n == 0, 0, (n + 1) % 2))

    def plane_at(k):
        low = z < planes // 2
        mirrored = jnp.where(low, z, planes - 1 - z)
        q = jnp.where(k <= mirrored, mirrored - k, k)
        return jnp.where(low, q, planes - 1 - q)

    def plane_of(n):
        return plane_at(((n + 1) // 2) % planes)

    def item_of(n):
        return 2 * plane_of(n) + half_of(n)

    def step_of(turn):
        back = items - 3 - 2 * ((turn - 2) // 2) + turn % 2
        kept = (turn <= 1) | (turn == items - 1)
        return jnp.where(kept, turn, jnp.where(turn == items - 2, 2, back))

    def has_turn(u):
        return (u >= 0) & (u < items)

    def at_plane(p):
        return {"sp": p * 2 + x, "tp": tp}

    def to_z(i):
        return at_plane((z + planes - i) % planes)

    def move(kind, n, src, dst, device, m=None):
        return pltpu.make_async_remote_copy(
            src_ref=src, dst_ref=dst, send_sem=ssem.at[kind, n],
            recv_sem=rsem.at[kind, n if m is None else m],
            device_id=device, device_id_type=pl.DeviceIdType.MESH,
        )

    def send(kind, n, src, dst, device, m=None):
        move(kind, n, src, dst, device, m).start()

    def arrived(kind, n, dst):
        move(kind, n, dst, dst, to_core).wait_recv()

    def left(kind, n, src):
        move(kind, n, src, src, to_core).wait_send()

    takes = (x == 0) & (z > 0)
    loads = [
        pltpu.make_async_copy(far, near, wsem.at[i])
        for i, (far, near) in enumerate(
            [
                (logs_hbm, logs), (k_hbm, k_ref), (near_hbm, near_table), (base_hbm, base_table), (v_hbm, v_ref),
                (q_hbm, q_ref), (gate_hbm, gate_ref), (gain_hbm, head_gain), (routes_hbm, routes),
                (shares_hbm, route_weights), (residual_hbm, residual), (ffn_gain_hbm, ffn_gain),
                (wo_hbm, wo), (wg_hbm, wg), (wu_hbm, wu), (wd_hbm, wd),
            ]
        )
    ]
    for copy in loads:
        copy.start()
    barrier = pltpu.get_barrier_semaphore()
    for device in [to_core, to_y, to_x] + [to_z(i) for i in range(1, planes)]:
        pl.semaphore_signal(barrier, inc=1, device_id=device, device_id_type=pl.DeviceIdType.MESH)


    @pl.when(takes)
    def _():
        pl.semaphore_signal(
            barrier, inc=1, device_id={"sp": z * 2 - 1, "tp": tp}, device_id_type=pl.DeviceIdType.MESH
        )

    length = q_ref.shape[0]
    dim = HEAD_DIM
    heads = q_ref.shape[1] // dim
    depth = state.shape[1]
    cuts = dim // depth
    after = lax.broadcasted_iota(jnp.int32, (length, length), 0) >= lax.broadcasted_iota(
        jnp.int32, (length, length), 1
    )
    ones = jnp.where(after, 1.0, 0.0).astype(f32)
    loads[0].wait()
    log_rows = jnp.concatenate([logs[...], jnp.zeros((8 - heads, length), f32)], axis=0)
    cum_row[...] = lax.dot_general(
        log_rows, ones, (((1,), (1,)), ((), ())), precision=highest, preferred_element_type=f32
    )
    cum_col[...] = lax.dot_general(
        ones, log_rows, (((1,), (1,)), ((), ())), precision=highest, preferred_element_type=f32
    )
    total_own[...] = jnp.broadcast_to(cum_row[:, length - 1 :], (8, dim))
    loads[2].wait()
    loads[3].wait()
    base = base_table[pl.ds(sp * 8, 8), :]
    cosine = base[0:1] * near_table[0] - base[1:2] * near_table[1]
    sine = base[2:3] * near_table[0] + base[3:4] * near_table[1]
    rotary[0] = cosine
    rotary[1] = sine

    def turned(rows_in):
        wide = rows_in.astype(f32)
        return wide * rotary[0] + pltpu.roll(wide, dim // 2, 1) * rotary[1]

    def column_of(h):
        lanes = lax.broadcasted_iota(jnp.int32, cum_col.shape, 1)
        return jnp.sum(jnp.where(lanes == h, cum_col[...], 0.0), axis=1, keepdims=True)

    left_side = x == 0

    def incoming(e):
        return jnp.where(takes, jnp.exp(total_prev[e // cuts : e // cuts + 1, :]), 1.0) * carry_in[e].astype(f32)

    def pass_state(e, first):
        h = e // cuts
        if first:
            grown = state[e].astype(bf16)
            before = jnp.zeros((depth, dim), bf16)
        else:
            near = incoming(e)
            span = total_own[h : h + 1, :] + jnp.where(left_side, 0.0, total_x[h : h + 1, :])
            grown = (jnp.exp(span) * near + state[e]).astype(bf16)
            before = near.astype(bf16)
        carry_out[e] = grown
        side_out[e] = jnp.where(left_side, grown, before)

        @pl.when(z + 1 < planes)
        def _():
            send(CHAIN, e, carry_out.at[e], carry_in.at[e], at_plane(z + 1))

        send(ACROSS, e, side_out.at[e], side_in.at[e], to_x)

    @pl.when(jnp.logical_not(takes))
    def _():
        total_prev[...] = jnp.zeros_like(total_prev)

    @pl.when(z == 0)
    def _():
        carry_in[...] = jnp.zeros_like(carry_in)
        for r in range(2):
            for ref in (tot_up, low_up, high_up):
                ref[r] = jnp.zeros_like(ref[r])

    @pl.when(z == planes - 1)
    def _():
        for r in range(2):
            for ref in (tot_down, low_down, high_down):
                ref[2 * planes - 2 + r] = jnp.zeros_like(ref[r])

    loads[1].wait()
    loads[4].wait()
    for h in range(heads):
        lanes = pl.ds(h * dim, dim)
        keys = turned(k_ref[:, lanes]) * dim ** (-0.5)
        turned_k[:, lanes] = keys.astype(bf16)
        column = column_of(h)
        tailed = (keys * jnp.exp(column[length - 1 :, :] - column)).astype(bf16)
        state[cuts * h : cuts * (h + 1)] = lax.dot_general(
            tailed, v_ref[:, lanes], (((0,), (0,)), ((), ())), preferred_element_type=f32
        ).reshape(cuts, depth, dim)

        if h == 0:
            gives = (x == 1) & (z + 1 < planes)
            pl.semaphore_wait(barrier, 2 + planes + jnp.where(gives, 1, 0))
            send(TOTAL, 0, total_own, total_x, to_x)

            @pl.when(gives)
            def _():
                send(TOTAL_ON, 0, total_own, total_prev, {"sp": (z + 1) * 2, "tp": tp})


        @pl.when(z == 0)
        def _():
            for e in range(cuts * h, cuts * (h + 1)):
                pass_state(e, True)

    def attend(h, carry):
        lanes = pl.ds(pl.multiple_of(h * dim, dim), dim)
        queries = turned(q_ref[:, lanes])
        column = column_of(h)
        scores = lax.dot_general(
            queries.astype(bf16), turned_k[:, lanes], (((1,), (1,)), ((), ())), preferred_element_type=f32
        )
        gap = jnp.minimum(column - cum_row[pl.ds(h, 1), :], 0.0)
        decays = jnp.where(after, jnp.exp(gap), 0.0)
        ret[:, lanes] = jnp.dot((scores * decays).astype(bf16), v_ref[:, lanes], preferred_element_type=f32)
        qdec[:, lanes] = (queries * jnp.exp(column)).astype(bf16)
        return carry

    early = jnp.where(z >= planes // 2, heads, 0)
    loads[5].wait()
    lax.fori_loop(0, early, attend, 0)

    arrived(TOTAL, 0, total_x)

    @pl.when(takes)
    def _():
        arrived(TOTAL_ON, 0, total_prev)

    for e in range(cuts * heads):

        @pl.when(z > 0)
        def _():
            arrived(CHAIN, e, carry_in.at[e])
            pass_state(e, False)

    lax.fori_loop(early, heads, attend, 0)

    for h in range(heads):
        lanes = pl.ds(h * dim, dim)
        if h == 0:
            loads[6].wait()
            loads[7].wait()
        blocks = slice(cuts * h, cuts * (h + 1))
        for e in range(cuts * h, cuts * (h + 1)):
            arrived(ACROSS, e, side_in.at[e])
        factor = jnp.where(left_side, 1.0, jnp.exp(total_x[h : h + 1, :]))
        factor = factor * jnp.where(takes, jnp.exp(total_prev[h : h + 1, :]), 1.0)
        before = carry_in[blocks].reshape(dim, dim).astype(f32)
        entering = (factor * before + side_in[blocks].reshape(dim, dim).astype(f32)).astype(bf16)
        retained = ret[:, lanes] + jnp.dot(qdec[:, lanes], entering, preferred_element_type=f32)
        centred = retained - jnp.mean(retained, axis=-1, keepdims=True)
        variance = jnp.mean(centred * centred, axis=-1, keepdims=True)
        gate_in = gate_ref[:, lanes].astype(f32)
        scaled = centred * lax.rsqrt(variance + group_eps) * head_gain[:, lanes]
        made = (scaled * (gate_in / (1.0 + jnp.exp(-gate_in)))).astype(bf16)
        hidden[:, :, lanes] = made.reshape(4, own_rows, dim)

    loads[12].wait()
    pieces = blend.shape[0]
    spans = pieces // 2
    span = width // spans

    def cross(j):
        arrived(MIX_C, j, from_core.at[j])
        held[j] = (blend[j, c, 1 - y].astype(f32) + from_core[j, 1 - y].astype(f32)).astype(bf16)
        send(MIX_Y, j, held.at[j], from_y.at[j], to_y)

    for j in range(pieces):
        picked = hidden[:, j // spans * rows : (j // spans + 1) * rows, :].reshape(4 * rows, heads * dim)
        mixed = jnp.dot(picked, wo[:, pl.ds(j % spans * span, span)], preferred_element_type=f32).astype(bf16)
        for q in range(4):
            blend[j, q % 2, q // 2] = mixed[q * rows : (q + 1) * rows, :]
        send(MIX_C, j, blend.at[j, 1 - c], from_core.at[j], to_core)
        if j > 0:
            cross(j - 1)
    cross(pieces - 1)

    here = x * 2 + y
    other_x = (1 - x) * 2 + y
    other_y = x * 2 + (1 - y)
    other_xy = (1 - x) * 2 + (1 - y)
    for copy in loads[8:12]:
        copy.wait()
    count = routes.shape[0]
    share_in[...] = jnp.zeros_like(share_in)
    share_in[:count, :own_rows] = route_weights[...]
    all_routes = jnp.concatenate([routes[...]] * (8 // count), axis=0)
    own_routes = jnp.zeros((8, 128), jnp.int32)
    for q in range(4):
        turned_routes = pltpu.roll(all_routes, (length - q * own_rows) % length, 1)
        own_routes = own_routes + jnp.where(tp == q, turned_routes[:, :128], 0)
    expert = lax.broadcasted_iota(jnp.int32, (128, 128), 0)
    shares = jnp.zeros((128, 128), f32)
    for k in range(count):
        shares = shares + jnp.where(own_routes[k : k + 1, :] == expert, share_in[k : k + 1, :], 0.0)
    share = jnp.transpose(shares)[:own_rows, :]
    coarse = share.astype(bf16).astype(f32)
    tail_rows = (coarse + pltpu.roll(share - coarse, sp_count, 1)).astype(bf16)
    first_rows, last_rows = pl.ds(0, rows), pl.ds(rows, rows)
    def side(p, chip, part):
        return gs.at[c, p, chip, part]

    def pass_side(kind, n, chip, part, device):
        send(kind, n, side(z, chip, part), side(z, chip, part), device)

    def spread_side(r):
        if r == 0:
            pass_side(S_X2, 0, here, first_rows, to_x)
            pass_side(S_Y3, 0, here, first_rows, to_y)
        else:
            pass_side(S_Y2, 0, here, last_rows, to_y)
            pass_side(S_X3, 0, here, last_rows, to_x)

    def relay_side():
        arrived(S_X2, 0, side(z, other_x, first_rows))
        pass_side(S_Y4, 0, other_x, first_rows, to_y)
        arrived(S_Y2, 0, side(z, other_y, last_rows))
        pass_side(S_X4, 0, other_y, last_rows, to_x)

    def side_up(p):
        @pl.when(z + 1 < planes)
        def _():
            send(S_UP, p, gs.at[c, p], gs.at[c, p], at_plane(z + 1))

    def side_down(p):
        @pl.when(z > 0)
        def _():
            send(S_DOWN, p, gs.at[c, p], gs.at[c, p], at_plane(z - 1))

    def side_core(p):
        send(S_CORE, p, gs.at[c, p], gs.at[c, p], to_core)

    def close_side():
        arrived(S_Y3, 0, side(z, other_y, first_rows))
        arrived(S_Y4, 0, side(z, other_xy, first_rows))
        arrived(S_X3, 0, side(z, other_x, last_rows))
        arrived(S_X4, 0, side(z, other_xy, last_rows))
        side_up(z)
        side_down(z)
        side_core(z)

    def spread(n):
        send(X_A2, n, g0.at[c, n, here], g0.at[c, n, here], to_x)
        send(Y_B2, n, g1.at[c, n, here], g1.at[c, n, here], to_y)
        send(Y_A3, n, g0.at[c, n, here], g0.at[c, n, here], to_y)
        send(X_B3, n, g1.at[c, n, here], g1.at[c, n, here], to_x)

    def raise_up(n):
        @pl.when(z + 1 < planes)
        def _():
            send(UP_A, n, g0.at[c, n, here], g0.at[c, n, here], at_plane(z + 1))
            send(UP_B, n, g1.at[c, n, here], g1.at[c, n, here], at_plane(z + 1))

    def hand_down(n):
        @pl.when(z > 0)
        def _():
            send(DOWN_A, n, g0.at[c, n, here], g0.at[c, n, here], at_plane(z - 1))
            send(DOWN_B, n, g1.at[c, n, here], g1.at[c, n, here], at_plane(z - 1))

    for r in range(2):
        mine, n = slice(r * rows, (r + 1) * rows), 2 * z + r
        square = jnp.zeros((rows, 1), f32)
        for j in range(r * spans, (r + 1) * spans):
            cols = pl.ds(j % spans * span, span)
            near = residual[mine, cols].astype(f32) + blend[j, c, y].astype(f32) + from_core[j, y].astype(f32)
            arrived(MIX_Y, j, from_y.at[j])
            total = near + from_y[j].astype(f32)
            upd[mine, cols] = total
            square = square + jnp.sum(total * total, axis=-1, keepdims=True)
        scale = lax.rsqrt(square * (1.0 / width) + square_eps)
        ready = (upd[mine, :] * scale * ffn_gain[...]).astype(bf16)
        g0[c, n, here, :, :wide_a] = ready[:, :wide_a]
        g0[c, n, here, :, wide_a:] = tail_rows[mine]
        g1[c, n, here] = ready[:, wide_a:wide_ab]
        gs[c, z, here, mine, :] = ready[:, wide_ab:]
        raise_up(n)
        hand_down(n)
        spread_side(r)
        if r == 0:
            spread(n)

    last_chains = [(T_UP, T_DOWN, tot, tot_up, tot_down)]
    main_chains = [(R_UP_A, R_DOWN_A, d0, low_up, low_down), (R_UP_B, R_DOWN_B, d1, high_up, high_down)]

    def start_chain(n, chains):
        @pl.when((n // 2 > z) & (z == 0))
        def _():
            for up, _, acc, got_up, _ in chains:
                send(up, n, acc.at[n], got_up.at[n], at_plane(z + 1))

        @pl.when((n // 2 < z) & (z == planes - 1))
        def _():
            for _, down, acc, _, got_down in chains:
                send(down, n, acc.at[n], got_down.at[n], at_plane(z - 1))

    def go_on(turn, chains):
        n = item_of(step_of(turn))

        @pl.when((n // 2 > z) & (z > 0))
        def _():
            for up, _, acc, got_up, _ in chains:
                arrived(up, n, got_up.at[n])
                acc[n] = acc[n] + got_up[n]
                send(up, n, acc.at[n], got_up.at[n], at_plane(z + 1))

        @pl.when((n // 2 < z) & (z < planes - 1))
        def _():
            for _, down, acc, _, got_down in chains:
                arrived(down, n, got_down.at[n])
                acc[n] = acc[n] + got_down[n]
                send(down, n, acc.at[n], got_down.at[n], at_plane(z - 1))

    def tick(t, carry):
        def relay():
            n = item_of(t)
            arrived(X_A2, n, g0.at[c, n, other_x])
            send(Y_A4, n, g0.at[c, n, other_x], g0.at[c, n, other_x], to_y)
            arrived(Y_B2, n, g1.at[c, n, other_y])
            send(X_B4, n, g1.at[c, n, other_y], g1.at[c, n, other_y], to_x)

        pl.when(t == 0)(relay_side)
        pl.when(t == 0)(relay)
        pl.when(t == 1)(close_side)

        @pl.when(t + 1 < items)
        def _():
            k, r = (t + 2) // 2, t % 2

            @pl.when((t + 1 < items - 1) & (z - k >= 0))
            def _():
                n = 2 * (z - k) + r
                arrived(UP_A, n, g0.at[c, n, here])
                arrived(UP_B, n, g1.at[c, n, here])
                raise_up(n)

            @pl.when((t + 1 < items - 1) & (z + k < planes))
            def _():
                n = 2 * (z + k) + r
                arrived(DOWN_A, n, g0.at[c, n, here])
                arrived(DOWN_B, n, g1.at[c, n, here])
                hand_down(n)

            spread(item_of(t + 1))

        pl.when((t > 0) & (t < items))(relay)

        @pl.when((t >= 2) & (t < items) & (t % 2 == 0))
        def _():
            below, above = z - t // 2, z + t // 2

            @pl.when(below >= 0)
            def _():
                arrived(S_UP, below, gs.at[c, below])
                side_up(below)
                side_core(below)

            @pl.when(above < planes)
            def _():
                arrived(S_DOWN, above, gs.at[c, above])
                side_down(above)
                side_core(above)

        @pl.when(t == 2)
        def _():
            for copy in loads[13:]:
                copy.wait()

        @pl.when((t >= 2) & (t < items + 2))
        def _():
            n = item_of(t - 2)
            arrived(C_A, n, g0.at[1 - c, n])
            arrived(C_B, n, g1.at[1 - c, n])
            p, r = plane_of(t - 2), half_of(t - 2)

            @pl.when(r == 0)
            def _():
                arrived(S_CORE, p, gs.at[1 - c, p])

            lead = g0[:, n].reshape(8 * rows, wide_a + 128)
            tail = lead[:, wide_a:].astype(f32)
            rest = g1[:, n].reshape(8 * rows, wide_b)
            last = gs[:, p, :, pl.ds(pl.multiple_of(r * rows, rows), rows), :].reshape(8 * rows, width - wide_ab)
            rows_in = jnp.concatenate([lead[:, :wide_a], rest, last], axis=1)
            lane = lax.broadcasted_iota(jnp.int32, tail.shape, 1)
            weight = jnp.sum(
                jnp.where((lane == sp) | (lane == sp + sp_count), tail, 0.0), axis=1, keepdims=True
            )

            def product(w):
                return jnp.dot(rows_in, w[...], preferred_element_type=f32)

            gate = jnp.minimum(product(wg), clamp_limit)
            up = jnp.clip(product(wu), -clamp_limit, clamp_limit)
            act = ((up + 1.0) * (gate / (1.0 + jnp.exp(-swish_alpha * gate)))).astype(bf16)
            made = (jnp.dot(act, wd[...], preferred_element_type=f32) * weight).astype(bf16)
            pm[n] = made.reshape(2, 4 * rows, width)
            send(C_P, n, pm.at[n, 1 - c], pr.at[n], to_core)

        @pl.when((t >= 1) & (t < items + 1))
        def _():
            n = item_of(t - 1)
            arrived(Y_A3, n, g0.at[c, n, other_y])
            arrived(Y_A4, n, g0.at[c, n, other_xy])
            arrived(X_B3, n, g1.at[c, n, other_x])
            arrived(X_B4, n, g1.at[c, n, other_xy])
            send(C_A, n, g0.at[c, n], g0.at[c, n], to_core)
            send(C_B, n, g1.at[c, n], g1.at[c, n], to_core)

        @pl.when(has_turn(t - lag))
        def _():
            n = item_of(step_of(t - lag))
            arrived(C_P, n, pr.at[n])
            for q in range(4):
                part = pl.ds(q * rows, rows)
                total = pm[n, c, part, :] + pr[n, part, :]
                a0[n, q % 2, q // 2] = total[:, :half]
                a1[n, q // 2, q % 2] = total[:, half : 2 * half]
                tot[n, q] = total[:, 2 * half :]
            send(Y_A, n, a0.at[n, 1 - y], r10.at[n], to_y)
            send(X_B, n, a1.at[n, 1 - x], r11.at[n], to_x)
            start_chain(n, last_chains)

        @pl.when(has_turn(t - lag - 1))
        def _():
            n = item_of(step_of(t - lag - 1))
            arrived(Y_A, n, r10.at[n])
            b0[n] = a0[n, y] + r10[n]
            send(X_A, n, b0.at[n, 1 - x], r20.at[n], to_x)
            arrived(X_B, n, r11.at[n])
            b1[n] = a1[n, x] + r11[n]
            send(Y_B, n, b1.at[n, 1 - y], r21.at[n], to_y)

        @pl.when(has_turn(t - lag - 2))
        def _():
            n = item_of(step_of(t - lag - 2))
            arrived(X_A, n, r20.at[n])
            d0[n] = b0[n, x] + r20[n]
            arrived(Y_B, n, r21.at[n])
            d1[n] = b1[n, y] + r21[n]
            start_chain(n, main_chains)

        u = t - lag

        @pl.when((u >= 3) & (u <= items - 2))
        def _():
            go_on(u - 1, last_chains)

        @pl.when(u == items - 2)
        def _():
            go_on(1, last_chains)
            go_on(items - 2, last_chains)

        @pl.when((u >= 5) & (u <= items))
        def _():
            go_on(u - 3, main_chains)

        @pl.when(u == items)
        def _():
            go_on(1, main_chains)
            go_on(items - 2, main_chains)

        @pl.when(u == items - 1)
        def _():
            for r in range(2):
                n = 2 * z + r

                @pl.when(z > 0)
                def _():
                    arrived(T_UP, n, tot_up.at[n])

                @pl.when(z < planes - 1)
                def _():
                    arrived(T_DOWN, n, tot_down.at[n])

                for q in range(4):
                    total = tot[n, q].astype(f32) + tot_up[n, q].astype(f32) + tot_down[n, q].astype(f32)
                    place = (q % 2, q // 2) if r == 0 else (q // 2, q % 2)
                    home[r, place[0], place[1]] = total.astype(bf16)
            send(T_Y1, 0, home.at[0, 1 - y], home_in.at[0], to_y)
            send(T_X1, 0, home.at[1, 1 - x], home_in.at[1], to_x)

        @pl.when(u == items)
        def _():
            arrived(T_Y1, 0, home_in.at[0])
            pair[0] = (home[0, y].astype(f32) + home_in[0].astype(f32)).astype(bf16)
            send(T_X2, 0, pair.at[0, 1 - x], pair_in.at[0], to_x)
            arrived(T_X1, 0, home_in.at[1])
            pair[1] = (home[1, x].astype(f32) + home_in[1].astype(f32)).astype(bf16)
            send(T_Y2, 0, pair.at[1, 1 - y], pair_in.at[1], to_y)

        return carry

    lax.fori_loop(0, items + lag + 2, tick, 0)
    arrived(T_X2, 0, pair_in.at[0])
    arrived(T_Y2, 0, pair_in.at[1])
    writes = []
    for r in range(2):
        n, part = 2 * z + r, pl.ds(r * rows, rows)
        low = upd[part, :half] + d0[n].astype(f32)
        high = upd[part, half : 2 * half] + d1[n].astype(f32)

        @pl.when(z > 0)
        def _():
            arrived(R_UP_A, n, low_up.at[n])
            arrived(R_UP_B, n, high_up.at[n])

        @pl.when(z < planes - 1)
        def _():
            arrived(R_DOWN_A, n, low_down.at[n])
            arrived(R_DOWN_B, n, high_down.at[n])

        low = low + low_up[n].astype(f32) + low_down[n].astype(f32)
        high = high + high_up[n].astype(f32) + high_down[n].astype(f32)
        out[part, :half] = low.astype(bf16)
        out[part, half : 2 * half] = high.astype(bf16)
        kept = pair[0, x] if r == 0 else pair[1, y]
        out[part, 2 * half :] = (
            upd[part, 2 * half :] + kept.astype(f32) + pair_in[r].astype(f32)
        ).astype(bf16)
        write = pltpu.make_async_copy(out.at[part], out_hbm.at[part], wsem.at[len(loads) + r])
        write.start()
        writes.append(write)

    left(T_Y1, 0, home.at[0, 1 - y])
    left(T_X1, 0, home.at[1, 1 - x])
    left(T_X2, 0, pair.at[0, 1 - x])
    left(T_Y2, 0, pair.at[1, 1 - y])

    def drain(n, carry):
        p = n // 2

        @pl.when(p > z)
        def _():
            for up, _, acc, _, _ in last_chains + main_chains:
                left(up, n, acc.at[n])

        @pl.when(p < z)
        def _():
            for _, down, acc, _, _ in last_chains + main_chains:
                left(down, n, acc.at[n])

        @pl.when((p <= z) & (z + 1 < planes))
        def _():
            left(UP_A, n, g0.at[c, n, here])
            left(UP_B, n, g1.at[c, n, here])

        @pl.when((p >= z) & (z > 0))
        def _():
            left(DOWN_A, n, g0.at[c, n, here])
            left(DOWN_B, n, g1.at[c, n, here])

        left(X_A2, n, g0.at[c, n, here])
        left(Y_B2, n, g1.at[c, n, here])
        left(Y_A3, n, g0.at[c, n, here])
        left(X_B3, n, g1.at[c, n, here])
        left(Y_A4, n, g0.at[c, n, other_x])
        left(X_B4, n, g1.at[c, n, other_y])
        left(C_A, n, g0.at[c, n])
        left(C_B, n, g1.at[c, n])
        left(C_P, n, pm.at[n, 1 - c])
        left(Y_A, n, a0.at[n, 1 - y])
        left(X_B, n, a1.at[n, 1 - x])
        left(X_A, n, b0.at[n, 1 - x])
        left(Y_B, n, b1.at[n, 1 - y])
        return carry

    lax.fori_loop(0, items, drain, 0)
    left(S_X2, 0, side(z, here, first_rows))
    left(S_Y2, 0, side(z, here, last_rows))
    left(S_Y3, 0, side(z, here, first_rows))
    left(S_X3, 0, side(z, here, last_rows))
    left(S_Y4, 0, side(z, other_x, first_rows))
    left(S_X4, 0, side(z, other_y, last_rows))

    def drain_side(p, carry):
        @pl.when((p <= z) & (z + 1 < planes))
        def _():
            left(S_UP, p, gs.at[c, p])

        @pl.when((p >= z) & (z > 0))
        def _():
            left(S_DOWN, p, gs.at[c, p])

        left(S_CORE, p, gs.at[c, p])
        return carry

    lax.fori_loop(0, planes, drain_side, 0)
    left(TOTAL, 0, total_own)

    @pl.when(gives)
    def _():
        left(TOTAL_ON, 0, total_own)

    for e in range(cuts * heads):
        left(ACROSS, e, side_out.at[e])

        @pl.when(z + 1 < planes)
        def _():
            left(CHAIN, e, carry_out.at[e])

    for j in range(pieces):
        left(MIX_C, j, blend.at[j, 1 - c])
        left(MIX_Y, j, held.at[j])
    for write in writes:
        write.wait()


def rope_tables(length, spans):
    half_dim = HEAD_DIM // 2
    rates = rope_base ** (-np.arange(half_dim, dtype=np.float64) / half_dim)
    rates = np.concatenate([rates, rates])[None, :]
    near = np.arange(length, dtype=np.float64)[:, None] * rates
    starts = (np.arange(spans, dtype=np.float64) * length)[:, None] * rates
    sign = np.concatenate([-np.ones(half_dim), np.ones(half_dim)])[None, :]
    base = np.zeros((spans, 8, HEAD_DIM))
    base[:, 0], base[:, 1] = np.cos(starts), np.sin(starts)
    base[:, 2], base[:, 3] = sign * np.sin(starts), sign * np.cos(starts)
    near_table = np.stack([np.cos(near), np.sin(near)]).astype(np.float32)
    return jnp.asarray(near_table), jnp.asarray(base.reshape(spans * 8, HEAD_DIM).astype(np.float32))


def fused_layer(
    query_rows, key_rows, value_rows, gate_rows, log_decay, head_gain, out_weight, residual, ffn_gain,
    gate_part, up_part, down_part, routes, route_weights,
):
    sp_count = lax.axis_size("sp")
    length, heads = log_decay.shape
    rows_all, width = residual.shape
    inner = query_rows.shape[1]
    near_table, base_table = rope_tables(length, sp_count)
    wide_t = 128 * (width // 1024)
    half = (width - wide_t) // 2
    planes = sp_count // 2
    items = 2 * planes
    rows = rows_all // 2
    pieces = 8
    span = 2 * width // pieces
    wide_s = 128 * (3 * width // 2048)
    wide_a = (width - wide_s - 128) // 256 * 128
    wide_b = width - wide_s - wide_a
    bf16, f32 = jnp.bfloat16, jnp.float32
    whole = pl.BlockSpec(memory_space=pltpu.VMEM)
    far = pl.BlockSpec(memory_space=pltpu.HBM)
    operands = (
        log_decay.T, key_rows, near_table, base_table, value_rows, query_rows, gate_rows, head_gain[None, :],
        routes.T, route_weights.T, residual, ffn_gain[None, :], out_weight, gate_part, up_part, down_part,
    )
    square = (2 * heads, HEAD_DIM // 2, HEAD_DIM)
    return pl.pallas_call(
        functools.partial(layer_kernel, planes),
        out_shape=jax.ShapeDtypeStruct((rows_all, width), bf16),
        in_specs=[far] * len(operands),
        out_specs=far,
        scratch_shapes=[
            *[pltpu.VMEM(operand.shape, operand.dtype) for operand in operands],
            pltpu.VMEM((2, length, HEAD_DIM), f32),
            pltpu.VMEM((length, inner), bf16),
            pltpu.VMEM((length, inner), f32),
            pltpu.VMEM((length, inner), bf16),
            pltpu.VMEM(square, f32),
            pltpu.VMEM((length, 8), f32),
            pltpu.VMEM((8, length), f32),
            pltpu.VMEM((8, HEAD_DIM), f32),
            pltpu.VMEM((8, HEAD_DIM), f32),
            pltpu.VMEM(square, bf16),
            pltpu.VMEM(square, bf16),
            pltpu.VMEM(square, bf16),
            pltpu.VMEM(square, bf16),
            pltpu.VMEM((4, rows_all, inner), bf16),
            pltpu.VMEM((pieces, 2, 2, rows, span), bf16),
            pltpu.VMEM((pieces, 2, rows, span), bf16),
            pltpu.VMEM((pieces, rows, span), bf16),
            pltpu.VMEM((pieces, rows, span), bf16),
            pltpu.VMEM((rows_all, width), f32),
            pltpu.VMEM((8, 128), f32),
            pltpu.VMEM((2, items, 4, rows, wide_a + 128), bf16),
            pltpu.VMEM((2, items, 4, rows, wide_b), bf16),
            pltpu.VMEM((2, planes, 4, rows_all, wide_s), bf16),
            pltpu.VMEM((items, 2, 4 * rows, width), bf16),
            pltpu.VMEM((items, 4 * rows, width), bf16),
            pltpu.VMEM((items, 2, 2, rows, half), bf16),
            pltpu.VMEM((items, 2, 2, rows, half), bf16),
            pltpu.VMEM((items, 2, rows, half), bf16),
            pltpu.VMEM((items, 2, rows, half), bf16),
            pltpu.VMEM((items, 2, rows, half), bf16),
            pltpu.VMEM((items, 2, rows, half), bf16),
            pltpu.VMEM((items, rows, half), bf16),
            pltpu.VMEM((items, rows, half), bf16),
            pltpu.VMEM((items, rows, half), bf16),
            pltpu.VMEM((items, rows, half), bf16),
            pltpu.VMEM((items, rows, half), bf16),
            pltpu.VMEM((items, rows, half), bf16),
            pltpu.VMEM((items, rows, half), bf16),
            pltpu.VMEM((items, rows, half), bf16),
            pltpu.VMEM((items, 4, rows, wide_t), bf16),
            pltpu.VMEM((items, 4, rows, wide_t), bf16),
            pltpu.VMEM((items, 4, rows, wide_t), bf16),
            pltpu.VMEM((2, 2, 2, rows, wide_t), bf16),
            pltpu.VMEM((2, 2, rows, wide_t), bf16),
            pltpu.VMEM((2, 2, rows, wide_t), bf16),
            pltpu.VMEM((2, rows, wide_t), bf16),
            pltpu.VMEM((8, HEAD_DIM), f32),
            pltpu.VMEM((rows_all, width), bf16),
            pltpu.SemaphoreType.DMA((42, max(items, 2 * heads, pieces))),
            pltpu.SemaphoreType.DMA((42, max(items, 2 * heads, pieces))),
            pltpu.SemaphoreType.DMA((len(operands) + 2,)),
        ],
        compiler_params=pltpu.CompilerParams(
            collective_id=0, has_side_effects=True, vmem_limit_bytes=63 * 1024 * 1024
        ),
    )(*operands)


def body(
    query_rows,
    key_rows,
    value_rows,
    gate_rows,
    log_decay,
    head_gain,
    out_weight,
    residual,
    ffn_gain,
    gate_weight,
    up_weight,
    down_weight,
    routes,
    route_weights,
):
    tok_count = query_rows.shape[0]
    local_heads = log_decay.shape[1]
    sp_count = lax.axis_size("sp")
    tp_count = lax.axis_size("tp")
    model_width = residual.shape[1]
    rows_own = tok_count // tp_count
    capacity = max(2, 3 * rows_own * TOPK // (2 * sp_count))
    tp_index = lax.axis_index("tp")
    if (
        tp_count == 4 and sp_count % 2 == 0 and sp_count <= 16 and local_heads <= 8
        and rows_own <= 128 and rows_own < 2 * capacity and model_width % 2048 == 0
    ):
        return fused_layer(
            query_rows, key_rows, value_rows, gate_rows, log_decay, head_gain, out_weight, residual, ffn_gain,
            gate_weight[0], up_weight[0], down_weight[0], routes, route_weights,
        )
    own_routes = lax.dynamic_slice_in_dim(routes, tp_index * rows_own, rows_own, 0)
    hidden = retention(query_rows, key_rows, value_rows, gate_rows, log_decay, head_gain)
    mixed = jnp.dot(hidden, out_weight, preferred_element_type=jnp.float32).astype(jnp.bfloat16)
    mixed_sum = lax.psum_scatter(mixed, "tp", scatter_dimension=0, tiled=True).astype(jnp.float32)
    updated = residual.astype(jnp.float32) + mixed_sum
    ffn_in = square_norm(updated, ffn_gain)
    own_experts, own_ranks = slot_ranks(own_routes, sp_count)
    home_slot = own_experts * capacity + own_ranks
    gate_part = gate_weight[0]
    up_part = up_weight[0]
    down_part = down_weight[0]
    empty_row = jnp.zeros((1, model_width), jnp.bfloat16)
    source_row = (
        jnp.full((sp_count * capacity,), rows_own, jnp.int32)
        .at[home_slot]
        .set(jnp.arange(rows_own * TOPK, dtype=jnp.int32) // TOPK)
    )
    padded = jnp.concatenate([ffn_in, empty_row], axis=0)
    outgoing = padded[source_row].reshape(sp_count, capacity, model_width)
    arrived = lax.all_to_all(outgoing, "sp", split_axis=0, concat_axis=0, tiled=True)
    fanned = lax.all_gather(arrived[None], "tp", axis=0, tiled=True)
    activity = expert_rows(fanned.reshape(-1, model_width), gate_part, up_part)
    partial_out = jnp.dot(activity, down_part, preferred_element_type=jnp.float32).reshape(
        tp_count, sp_count, capacity, model_width
    )
    summed = (
        lax.psum_scatter(partial_out.astype(jnp.bfloat16), "tp", scatter_dimension=0, tiled=True)
        .astype(jnp.float32)
        .reshape(sp_count, capacity, model_width)
    )
    returned = lax.all_to_all(
        summed.astype(jnp.bfloat16), "sp", split_axis=0, concat_axis=0, tiled=True
    )
    picked = returned.reshape(sp_count * capacity, model_width)[home_slot].reshape(
        rows_own, TOPK, model_width
    )
    expert_sum = jnp.sum(route_weights[:, :, None] * picked.astype(jnp.float32), axis=1)
    return (updated + expert_sum).astype(jnp.bfloat16)


def solution(mesh):
    return jax.shard_map(
        body,
        mesh=mesh,
        in_specs=(
            P("sp", "tp"),
            P("sp", "tp"),
            P("sp", "tp"),
            P("sp", "tp"),
            P("sp", "tp"),
            P("tp"),
            P("tp", None),
            P(("sp", "tp"), None),
            P(),
            P("sp", None, "tp"),
            P("sp", None, "tp"),
            P("sp", "tp", None),
            P("sp", None),
            P(("sp", "tp"), None),
        ),
        out_specs=P(("sp", "tp"), None),
        check_vma=False,
    )
```
